32 devices in a mesh: ep: 4 (over y, x), tp: 8 (over z, core).
Axes of the slice: x: 2, y: 2, z: 4, core: 2. Of those that a mesh axis runs over, the one named last changes fastest.
Arguments:
- hidden: bfloat16 [160, 4096], P('ep', 'tp'), may hold values from -6 to 6
- positions: int32 [160], P('ep'), may hold values from 0 to 16383
- ret_state: float32 [160, 16, 128, 128], P('ep', 'tp'), may hold values from -1.5 to 1.5
- query_weight: bfloat16 [4096, 2048], P('ep', 'tp'), may hold values from -0.09375 to 0.09375
- key_weight: bfloat16 [4096, 2048], P('ep', 'tp'), may hold values from -0.09375 to 0.09375
- value_weight: bfloat16 [4096, 2048], P('ep', 'tp'), may hold values from -0.09375 to 0.09375
- gate_weight: bfloat16 [4096, 2048], P('ep', 'tp'), may hold values from -0.09375 to 0.09375
- head_gain: float32 [2048], P('tp'), may hold values from 0.1 to 1.9
- out_weight: bfloat16 [2048, 4096], P(None, 'tp'), may hold values from -0.125 to 0.125
- mix_gain: float32 [4096], replicated, may hold values from 0.1 to 1.9
- ffn_gain: float32 [4096], replicated, may hold values from 0.1 to 1.9
- expert_gate: bfloat16 [8, 4096, 2048], P('ep', None, 'tp'), may hold values from -0.09375 to 0.09375
- expert_up: bfloat16 [8, 4096, 2048], P('ep', None, 'tp'), may hold values from -0.09375 to 0.09375
- expert_down: bfloat16 [8, 2048, 4096], P('ep', None, 'tp'), may hold values from -0.125 to 0.125
- route_ids: int32 [160, 2], P('ep'), may hold values from 0 to 7, as said below
- route_weight: float32 [160, 2], P('ep'), may hold values from 0.25 to 1
Outputs:
- updated: bfloat16 [160, 4096], P('ep', 'tp')
- next_state: float32 [160, 16, 128, 128], P('ep', 'tp')
The draws below stay inside these ranges and needn't reach their ends.
Inputs may be any that keep to these rules, and one draw needn't show every extreme that they name: `route_ids`: each row names two different experts of one group, the group being the numbers g * 2 to g * 2 + 1; in the rows of one device (aligned blocks of 40 rows) no expert is named more than 10 times, and some expert is named exactly 10 times.
All inputs are finite; a program needn't handle non-finite values.
Results may differ from the reference program's by a relative error of at most 0.014.
Values may be sent and summed in bfloat16 or wider, within the bound.
No kernel may reach another device: no remote copies, remote signals or barrier semaphores. Data moves between devices by JAX's collectives and lax.ppermute only.
A program may use at most 64 MiB of HBM per device.

```python
import jax
import jax.numpy as jnp
from jax import lax

D = 4096
HEADS = 16
HEAD = 128
RD = 2048
FF = 2048
GROUPS = 4
EXPERTS = 8
TOP = 2
B_DEV = 40
BATCH = 160
CAP = 10
MAXPOS = 16384
N_EP = 4


def draw_route_ids(key, part):
    blocks = BATCH // B_DEV
    group_size = EXPERTS // GROUPS
    order_key, shift_key = jax.random.split(key)
    orders = jax.vmap(lambda item: jax.random.permutation(item, B_DEV))(jax.random.split(order_key, blocks))
    shifts = jax.random.randint(shift_key, (blocks, GROUPS), 0, group_size)
    group = orders % GROUPS
    within = orders // GROUPS
    offset = jnp.take_along_axis(shifts, group, axis=1)
    first = (within + offset) % group_size
    second = (first + 1) % group_size
    pairs = jnp.stack([group * group_size + first, group * group_size + second], axis=-1)
    return pairs.reshape(BATCH, TOP).astype(jnp.int32)


def place_ends(values, key, least, largest):
    spot = [jax.random.randint(jax.random.fold_in(key, axis), (), 0, length) for axis, length in enumerate(values.shape)]
    longest = values.shape.index(max(values.shape))
    beside = spot[:longest] + [(spot[longest] + 1) % values.shape[longest]] + spot[longest + 1:]
    return values.at[tuple(spot)].set(least).at[tuple(beside)].set(largest)


def block_levels(own_key, extent, shards, low, largest):
    def one(axis_at, blocks):
        draws = jax.random.uniform(jax.random.fold_in(jax.random.fold_in(own_key, 6), axis_at), (blocks,), jnp.float32, low / len(shards), largest / len(shards))
        return jnp.repeat(jnp.exp(draws), extent[axis_at] // blocks).reshape((-1,) + (1,) * (len(extent) - axis_at - 1))

    level = one(*shards[0])
    for cut in shards[1:]:
        level = level * one(*cut)
    return level


def scatter_about(rng, dims, scale, bound, cuts=(), held_as=jnp.bfloat16):
    values = scale * jax.random.normal(rng, dims, jnp.float32)
    if cuts:
        values = values * block_levels(rng, dims, cuts, -0.22, 0.18)
    return jnp.clip(values, -bound, bound).astype(held_as)


def setup_inputs(seed: int = 0) -> dict:
    keys = jax.random.split(jax.random.key(seed), 17)
    hidden = scatter_about(keys[0], (BATCH, D), 1.0, 6.0, ((0, 4), (1, 8)))
    positions = place_ends(jax.random.randint(keys[1], (BATCH,), 0, MAXPOS), jax.random.fold_in(keys[1], 1), 0, MAXPOS - 1).astype(jnp.int32)
    ret_state = scatter_about(keys[2], (BATCH, HEADS, HEAD, HEAD), 0.25, 1.5, ((0, 4), (1, 8)), jnp.float32)
    query_weight = scatter_about(keys[3], (D, RD), D ** -0.5, 0.09375, ((0, 4), (1, 8)))
    key_weight = scatter_about(keys[4], (D, RD), D ** -0.5, 0.09375, ((0, 4), (1, 8)))
    value_weight = scatter_about(keys[5], (D, RD), D ** -0.5, 0.09375, ((0, 4), (1, 8)))
    gate_weight = scatter_about(keys[6], (D, RD), D ** -0.5, 0.09375, ((0, 4), (1, 8)))
    head_gain = jnp.clip(1.0 + 0.18 * jax.random.normal(keys[7], (RD,), jnp.float32), 0.1, 1.9)
    out_weight = scatter_about(keys[8], (RD, D), RD ** -0.5, 0.125, ((1, 8),))
    mix_gain = jnp.clip(1.0 + 0.18 * jax.random.normal(keys[9], (D,), jnp.float32), 0.1, 1.9)
    ffn_gain = jnp.clip(1.0 + 0.18 * jax.random.normal(keys[10], (D,), jnp.float32), 0.1, 1.9)
    expert_gate = scatter_about(keys[11], (EXPERTS, D, FF), D ** -0.5, 0.09375, ((0, 4), (2, 8)))
    expert_up = scatter_about(keys[12], (EXPERTS, D, FF), D ** -0.5, 0.09375, ((0, 4), (2, 8)))
    expert_down = scatter_about(keys[13], (EXPERTS, FF, D), FF ** -0.5, 0.125, ((0, 4), (2, 8)))
    route_ids = draw_route_ids(jax.random.fold_in(keys[16], 71), 0)
    route_weight = jnp.clip(0.25 + 0.75 * jax.random.uniform(keys[15], (BATCH, TOP), jnp.float32) ** block_levels(keys[15], (BATCH, TOP), ((0, 4),), -0.2, 0.2), 0.25, 1.0)
    return dict(hidden=hidden, positions=positions, ret_state=ret_state, query_weight=query_weight, key_weight=key_weight, value_weight=value_weight, gate_weight=gate_weight, head_gain=head_gain, out_weight=out_weight, mix_gain=mix_gain, ffn_gain=ffn_gain, expert_gate=expert_gate, expert_up=expert_up, expert_down=expert_down, route_ids=route_ids, route_weight=route_weight)


epsilon = 1e-06
rope_base = 10000.0

def rms_scale(rows, gain):
    values = rows.astype(jnp.float32)
    factor = lax.rsqrt(lax.optimization_barrier(jnp.mean(values * values, axis=-1, keepdims=True)) + epsilon)
    return (values * factor * gain).astype(jnp.bfloat16)

def log_decay(head_ids):
    return jnp.log(1.0 - 2.0 ** (-5.0 - 5.0 * head_ids.astype(jnp.float32) / (HEADS - 1)))

def rotate(values, positions):
    width = values.shape[-1]
    inverse = 1.0 / rope_base ** (jnp.arange(0, width, 2, dtype=jnp.float32) / width)
    angle = positions.astype(jnp.float32)[:, None, None] * inverse[None, None, :]
    cosine = jnp.cos(angle)
    sine = jnp.sin(angle)
    first = values[..., :width // 2]
    second = values[..., width // 2:]
    return jnp.concatenate([first * cosine - second * sine, first * sine + second * cosine], axis=-1)

def retain(query, key_rows, value_rows, gate_rows, ret_state, positions, head_ids, head_gain):
    batch = query.shape[0]
    heads = head_ids.shape[0]

    def split(array):
        return array.astype(jnp.float32).reshape(batch, heads, HEAD)
    rotated_query = rotate(split(query), positions)
    rotated_key = rotate(split(key_rows), positions) * HEAD ** (-0.5)
    value_heads = split(value_rows)
    decay = jnp.exp(log_decay(head_ids))
    next_state = decay[None, :, None, None] * ret_state + rotated_key[..., :, None] * value_heads[..., None, :]
    read = jnp.einsum('bhd,bhde->bhe', rotated_query, next_state, precision=lax.Precision.HIGHEST)
    centered = read - lax.optimization_barrier(jnp.mean(read, axis=-1, keepdims=True))
    normal = centered * lax.rsqrt(lax.optimization_barrier(jnp.mean(centered * centered, axis=-1, keepdims=True)) + epsilon)
    mixed = normal.reshape(batch, heads * HEAD) * head_gain * jax.nn.silu(gate_rows.astype(jnp.float32))
    return (mixed.astype(jnp.bfloat16), next_state)

def reference(hidden, positions, ret_state, query_weight, key_weight, value_weight, gate_weight, head_gain, out_weight, mix_gain, ffn_gain, expert_gate, expert_up, expert_down, route_ids, route_weight):
    normed = rms_scale(hidden, mix_gain)

    def project(weight):
        return jnp.dot(normed, weight, preferred_element_type=jnp.float32).astype(jnp.bfloat16)
    mixed, next_state = retain(project(query_weight), project(key_weight), project(value_weight), project(gate_weight), ret_state, positions, jnp.arange(HEADS, dtype=jnp.int32), head_gain)
    after = (hidden.astype(jnp.float32) + jnp.dot(mixed, out_weight, preferred_element_type=jnp.float32)).astype(jnp.bfloat16)
    inner = rms_scale(after, ffn_gain)
    pair_count = BATCH * TOP
    chosen = route_ids.reshape(pair_count).astype(jnp.int32)
    pair_rows = jnp.repeat(inner, TOP, axis=0)
    onehot = (chosen[:, None] == jnp.arange(EXPERTS, dtype=jnp.int32)[None, :]).astype(jnp.int32)
    ranks = lax.optimization_barrier(jnp.sum((jnp.cumsum(onehot, axis=0).astype(jnp.int32) - 1) * onehot, axis=1)).astype(jnp.int32)
    slots = jnp.arange(N_EP * CAP, dtype=jnp.int32)

    def one_expert(carry, index):
        select = ((chosen[None, :] == index) & (ranks[None, :] == slots[:, None])).astype(jnp.bfloat16)
        rows = jnp.dot(select, pair_rows, preferred_element_type=jnp.float32).astype(jnp.bfloat16)
        gate = jnp.dot(rows, expert_gate[index], preferred_element_type=jnp.float32)
        lifted = jnp.dot(rows, expert_up[index], preferred_element_type=jnp.float32)
        activated = (jax.nn.silu(gate) * lifted).astype(jnp.bfloat16)
        result = jnp.dot(activated, expert_down[index], preferred_element_type=jnp.float32).astype(jnp.bfloat16)
        return (carry + jnp.dot(select.T, result, preferred_element_type=jnp.float32), None)
    pair_out, unused = lax.scan(one_expert, jnp.zeros((pair_count, D), jnp.float32), jnp.arange(EXPERTS, dtype=jnp.int32))
    weighted = lax.optimization_barrier(jnp.sum(pair_out.reshape(BATCH, TOP, D) * route_weight[:, :, None], axis=1))
    updated = (after.astype(jnp.float32) + weighted).astype(jnp.bfloat16)
    return (updated, next_state)
```

```python
import functools

import jax
import jax.numpy as jnp
from jax import lax
from jax.experimental import pallas as pl
from jax.experimental.pallas import tpu as pltpu
from jax.sharding import PartitionSpec as P

HEADS = 16
HEAD = 128
GROUPS = 4
TOP = 2
CORES = 2


epsilon = 1e-06
rope_base = 10000.0
f32 = jnp.float32
bf16 = jnp.bfloat16


def log_decay(head_ids):
    return jnp.log(1.0 - 2.0 ** (-5.0 - 5.0 * head_ids.astype(f32) / (HEADS - 1)))


def swap_cores(array):
    size = lax.axis_size("tp")
    return lax.ppermute(array, "tp", [(i, i ^ 1) for i in range(size)])


def along_z(array):
    size = lax.axis_size("tp")
    steps = range(1, size // CORES)
    return [array] + [
        lax.ppermute(array, "tp", [(i, i ^ (CORES * k)) for i in range(size)]) for k in steps
    ]


def to_peer(array, step):
    size = lax.axis_size("ep")
    return lax.ppermute(array, "ep", [(i, i ^ step) for i in range(size)])


def pick(pieces, index):
    chosen = pieces[0]
    for number in range(1, len(pieces)):
        chosen = jnp.where(index == number, pieces[number], chosen)
    return chosen


def whole(shape):
    rank = len(shape)
    return pl.BlockSpec(shape, lambda *_: (0,) * rank)


def scalars():
    return pl.BlockSpec(memory_space=pltpu.SMEM)


def project_kernel(count, peers, rows, *refs):
    place_ref, gain_ref = refs[0], refs[1]
    parts = refs[2 : 2 + count]
    weights = refs[2 + count : 6 + count]
    outs = refs[6 + count :]
    width = weights[0].shape[1]
    totals = [None] * 4
    for number in range(count):
        part = parts[number]
        span = part.shape[1]
        start = pl.multiple_of(place_ref[number], 128)
        gain = gain_ref[:, pl.ds(start, span)]
        scaled = (part[...].astype(f32) * gain).astype(bf16)
        for which in range(4):
            block = weights[which][pl.ds(start, span), :]
            product = jnp.dot(scaled, block, preferred_element_type=f32)
            totals[which] = product if totals[which] is None else totals[which] + product
    for peer in range(peers):
        for which in range(4):
            rows_here = totals[which][peer * rows : (peer + 1) * rows, :]
            outs[peer][:, which * width : (which + 1) * width] = rows_here.astype(outs[peer].dtype)


def project(parts, places, gain, weights, peers, rows):
    width = weights[0].shape[1]
    out_shape = [jax.ShapeDtypeStruct((rows, 4 * width), f32)]
    out_shape += [jax.ShapeDtypeStruct((rows, 4 * width), bf16)] * (peers - 1)
    return pl.pallas_call(
        functools.partial(project_kernel, len(parts), peers, rows),
        out_shape=out_shape,
        in_specs=[scalars(), whole(gain.shape)]
        + [whole(part.shape) for part in parts]
        + [whole(weight.shape) for weight in weights],
        out_specs=[whole((rows, 4 * width))] * peers,
        name="project",
    )(places, gain, *parts, *weights)


def retain_kernel(peers, heads, width_model, *refs):
    decay_ref, squares_ref, cos_ref, sin_ref, gain_ref = refs[:5]
    parts = refs[5 : 5 + peers]
    state_ref = refs[5 + peers]
    mixed_ref, next_ref = refs[6 + peers : 8 + peers]
    query_ref, key_ref, value_ref, gate_ref, read_ref = refs[8 + peers :]
    block = state_ref.shape[0]
    width = heads * HEAD

    @pl.when(pl.program_id(0) == 0)
    def first():
        factor = lax.rsqrt(squares_ref[...] * (1.0 / width_model) + epsilon)

        def total(which):
            cut = slice(which * width, (which + 1) * width)
            summed = parts[0][:, cut]
            for part in parts[1:]:
                summed = summed + part[:, cut].astype(f32)
            return (summed * factor).astype(bf16).astype(f32)

        query, key = total(0), total(1)
        for head in range(heads):
            cut = slice(head * HEAD, (head + 1) * HEAD)
            one = query[:, cut]
            query_ref[:, cut] = one * cos_ref[...] + pltpu.roll(one, HEAD // 2, 1) * sin_ref[...]
            two = key[:, cut]
            turned = two * cos_ref[...] + pltpu.roll(two, HEAD // 2, 1) * sin_ref[...]
            key_ref[:, cut] = turned * HEAD ** (-0.5)
        value_ref[...] = total(2)
        gate = total(3)
        gate_ref[...] = gate * jax.nn.sigmoid(gate) * gain_ref[...]

    start = pl.multiple_of(pl.program_id(0) * block, block)
    for head in range(heads):
        cut = slice(head * HEAD, (head + 1) * HEAD)
        query_columns = query_ref[pl.ds(start, block), cut].T
        key_columns = key_ref[pl.ds(start, block), cut].T
        value_rows = value_ref[pl.ds(start, block), cut]
        decay = decay_ref[head]
        for row in range(block):
            updated = (
                decay * state_ref[row, head]
                + key_columns[:, row : row + 1] * value_rows[row : row + 1, :]
            )
            next_ref[row, head] = updated
            read_ref[row : row + 1, :] = jnp.sum(
                query_columns[:, row : row + 1] * updated, axis=0, keepdims=True
            )
        read = read_ref[...]
        centered = read - jnp.mean(read, axis=-1, keepdims=True)
        spread = jnp.mean(centered * centered, axis=-1, keepdims=True)
        normal = centered * lax.rsqrt(spread + epsilon)
        mixed_ref[:, cut] = (normal * gate_ref[pl.ds(start, block), cut]).astype(bf16)


def retain(parts, squares, decay, cosine, sine, head_gain, ret_state, width_model):
    rows, heads = ret_state.shape[:2]
    width = heads * HEAD
    block = 8
    state_spec = pl.BlockSpec((block, heads, HEAD, HEAD), lambda i: (i, 0, 0, 0))
    return pl.pallas_call(
        functools.partial(retain_kernel, len(parts), heads, width_model),
        grid=(rows // block,),
        out_shape=[
            jax.ShapeDtypeStruct((rows, width), bf16),
            jax.ShapeDtypeStruct(ret_state.shape, f32),
        ],
        in_specs=[
            scalars(),
            whole(squares.shape),
            whole(cosine.shape),
            whole(sine.shape),
            whole(head_gain.shape),
        ]
        + [whole(part.shape) for part in parts]
        + [state_spec],
        out_specs=[pl.BlockSpec((block, width), lambda i: (i, 0)), state_spec],
        scratch_shapes=[pltpu.VMEM((rows, width), f32)] * 4 + [pltpu.VMEM((block, HEAD), f32)],
        name="retain",
    )(decay, squares, cosine, sine, head_gain, *parts, ret_state)


def out_kernel(count, peers, *refs):
    place_ref = refs[0]
    pieces = refs[1 : 1 + count]
    weight_ref, hidden_ref = refs[1 + count : 3 + count]
    placing = refs[3 + count : 3 + count + peers]
    after_ref = refs[3 + count + peers]
    outs = refs[4 + count + peers : 4 + count + 2 * peers]
    rows_ref, total_ref = refs[4 + count + 2 * peers :]
    step = pl.program_id(0)

    @pl.when(step == 0)
    def first():
        for number in range(count):
            width = pieces[number].shape[1]
            rows_ref[:, pl.ds(pl.multiple_of(place_ref[number], 128), width)] = pieces[number][...]
        total_ref[...] = hidden_ref[...].astype(f32)

    span = weight_ref.shape[0]
    part = rows_ref[:, pl.ds(pl.multiple_of(step * span, 128), span)]
    total_ref[...] += jnp.dot(part, weight_ref[...], preferred_element_type=f32)

    @pl.when(step == pl.num_programs(0) - 1)
    def last():
        after = total_ref[...].astype(bf16)
        after_ref[...] = after
        for peer in range(peers):
            sent = jnp.dot(placing[peer][...], after, preferred_element_type=f32)
            outs[peer][...] = sent.astype(bf16)


def out_project(pieces, places, weight, hidden, placing, steps):
    rows, width = hidden.shape
    depth = weight.shape[0]
    slots = placing[0].shape[0]
    peers = len(placing)
    return pl.pallas_call(
        functools.partial(out_kernel, len(pieces), peers),
        grid=(steps,),
        out_shape=[jax.ShapeDtypeStruct((rows, width), bf16)]
        + [jax.ShapeDtypeStruct((slots, width), bf16)] * peers,
        in_specs=[scalars()]
        + [whole(piece.shape) for piece in pieces]
        + [pl.BlockSpec((depth // steps, width), lambda i: (i, 0)), whole(hidden.shape)]
        + [whole(place.shape) for place in placing],
        out_specs=[whole((rows, width))] + [whole((slots, width))] * peers,
        scratch_shapes=[pltpu.VMEM((rows, depth), bf16), pltpu.VMEM((rows, width), f32)],
        name="out_project",
    )(places, *pieces, weight, hidden, *placing)


def lift_kernel(count, depth, *refs):
    place_ref = refs[0]
    pieces = refs[1 : 1 + count]
    gain_ref, gate_ref, up_ref, active_ref, rows_ref, sum_gate, sum_up = refs[1 + count :]
    step = pl.program_id(1)

    @pl.when((step == 0) & (pl.program_id(0) == 0))
    def first():
        squares = None
        for piece in pieces:
            values = piece[...].astype(f32)
            here = jnp.sum(values * values, axis=-1, keepdims=True)
            squares = here if squares is None else squares + here
        factor = lax.rsqrt(squares * (1.0 / depth) + epsilon)
        for number in range(count):
            width = pieces[number].shape[1]
            start = pl.multiple_of(place_ref[number], 128)
            gain = gain_ref[:, pl.ds(start, width)]
            scaled = pieces[number][...].astype(f32) * factor * gain
            rows_ref[:, pl.ds(start, width)] = scaled.astype(bf16)

    @pl.when(step == 0)
    def clear():
        sum_gate[...] = jnp.zeros_like(sum_gate)
        sum_up[...] = jnp.zeros_like(sum_up)

    span = gate_ref.shape[1]
    part = rows_ref[:, pl.ds(pl.multiple_of(step * span, 128), span)]
    sum_gate[...] += jnp.dot(part, gate_ref[0], preferred_element_type=f32)
    sum_up[...] += jnp.dot(part, up_ref[0], preferred_element_type=f32)

    @pl.when(step == pl.num_programs(1) - 1)
    def last():
        gate = sum_gate[...]
        active_ref[0] = (gate * jax.nn.sigmoid(gate) * sum_up[...]).astype(bf16)


def lift(pieces, places, gain, expert_gate, expert_up, steps):
    experts, depth, width = expert_gate.shape
    rows = pieces[0].shape[0]
    weight_spec = pl.BlockSpec((1, depth // steps, width), lambda e, i: (e, i, 0))
    return pl.pallas_call(
        functools.partial(lift_kernel, len(pieces), depth),
        grid=(experts, steps),
        out_shape=jax.ShapeDtypeStruct((experts, rows, width), bf16),
        in_specs=[scalars()]
        + [whole(piece.shape) for piece in pieces]
        + [whole(gain.shape), weight_spec, weight_spec],
        out_specs=pl.BlockSpec((1, rows, width), lambda e, i: (e, 0, 0)),
        scratch_shapes=[
            pltpu.VMEM((rows, depth), bf16),
            pltpu.VMEM((rows, width), f32),
            pltpu.VMEM((rows, width), f32),
        ],
        name="lift",
    )(places, *pieces, gain, expert_gate, expert_up)


def lower_kernel(count, peers, slots, *refs):
    place_ref = refs[0]
    pieces = refs[1 : 1 + count]
    down_ref, shares_ref = refs[1 + count : 3 + count]
    outs = refs[3 + count : 3 + count + peers]
    rows_ref, total_ref, mean_ref = refs[3 + count + peers :]
    expert, step = pl.program_id(0), pl.program_id(1)
    experts = pieces[0].shape[0]

    @pl.when((step == 0) & (expert == 0))
    def first():
        for number in range(count):
            width = pieces[number].shape[2]
            start = pl.multiple_of(place_ref[number], 128)
            rows_ref[:, :, pl.ds(start, width)] = pieces[number][...]
        mean_ref[...] = jnp.zeros_like(mean_ref)

    @pl.when(step == 0)
    def clear():
        total_ref[...] = jnp.zeros_like(total_ref)

    span = down_ref.shape[1]
    part = rows_ref[expert, :, pl.ds(pl.multiple_of(step * span, 128), span)]
    total_ref[...] += jnp.dot(part, down_ref[0], preferred_element_type=f32)

    @pl.when(step == pl.num_programs(1) - 1)
    def add():
        result = total_ref[...].astype(bf16).astype(f32)
        mean_ref[...] += result * shares_ref[expert]

    @pl.when((step == pl.num_programs(1) - 1) & (expert == experts - 1))
    def last():
        for peer in range(peers):
            outs[peer][...] = mean_ref[peer * slots : (peer + 1) * slots, :].astype(bf16)


def lower(pieces, places, expert_down, shares, peers, slots, steps):
    experts, depth, width = expert_down.shape
    rows = pieces[0].shape[1]
    return pl.pallas_call(
        functools.partial(lower_kernel, len(pieces), peers, slots),
        grid=(experts, steps),
        out_shape=[jax.ShapeDtypeStruct((slots, width), bf16)] * peers,
        in_specs=[scalars()]
        + [whole(piece.shape) for piece in pieces]
        + [pl.BlockSpec((1, depth // steps, width), lambda e, i: (e, i, 0)), whole(shares.shape)],
        out_specs=[whole((slots, width))] * peers,
        scratch_shapes=[
            pltpu.VMEM((experts, rows, depth), bf16),
            pltpu.VMEM((rows, width), f32),
            pltpu.VMEM((rows, width), f32),
        ],
        name="lower",
    )(places, *pieces, expert_down, shares)


def per_device(
    hidden,
    positions,
    ret_state,
    query_weight,
    key_weight,
    value_weight,
    gate_weight,
    head_gain,
    out_weight,
    mix_gain,
    ffn_gain,
    expert_gate,
    expert_up,
    expert_down,
    route_ids,
    route_weight,
):
    own_rows, slice_width = hidden.shape
    peers = lax.axis_size("ep")
    ranks = lax.axis_size("tp")
    depth = slice_width * ranks
    slab = query_weight.shape[0]
    width = query_weight.shape[1]
    heads_here = width // HEAD
    me = lax.axis_index("ep")
    rank = lax.axis_index("tp")
    level, core = rank // CORES, rank % CORES
    levels = ranks // CORES
    order = jnp.stack(
        [(level ^ k) * CORES + core for k in range(levels)]
        + [(level ^ k) * CORES + (1 - core) for k in range(levels)]
    ).astype(jnp.int32)

    local_experts = expert_gate.shape[0]
    experts = local_experts * peers
    group_size = experts // GROUPS
    capacity = 2 * ((own_rows // GROUPS + group_size - 1) // group_size)
    slots = local_experts * capacity
    if local_experts % group_size == 0:
        slots = slots // TOP
    homes = route_ids // local_experts
    near = route_ids % local_experts
    placing, shares = [], []
    for k in range(peers):
        here = homes == (me ^ k)
        goes = jnp.any(here, axis=1)
        slot = jnp.cumsum(goes.astype(jnp.int32)) - 1
        spot = (jnp.arange(slots, dtype=jnp.int32)[:, None] == slot[None, :]) & goes[None, :]
        spot = spot.astype(bf16)
        placing.append(spot)
        share = [
            jnp.sum(jnp.where(here & (near == number), route_weight, 0.0), axis=1)
            for number in range(local_experts)
        ]
        share = jnp.stack(share, axis=1)
        high = share.astype(bf16)
        rest = share - high.astype(f32)
        mid = rest.astype(bf16)
        low = (rest - mid.astype(f32)).astype(bf16)
        table = jnp.concatenate([high, mid, low], axis=1)
        table = jnp.pad(table, ((0, 0), (0, HEAD - table.shape[1])))
        shares.append(jnp.dot(spot, table, preferred_element_type=f32).astype(bf16))

    inverse = 1.0 / rope_base ** (jnp.arange(0, HEAD, 2, dtype=f32) / HEAD)
    angle = positions.astype(f32)[:, None] * inverse[None, :]
    cosine, sine = jnp.cos(angle), jnp.sin(angle)
    cosine = jnp.concatenate([cosine, cosine], axis=1)
    sine = jnp.concatenate([-sine, sine], axis=1)
    head_ids = rank * heads_here + jnp.arange(heads_here, dtype=jnp.int32)
    decay = jnp.exp(log_decay(head_ids))

    if ranks == CORES * peers:
        pieces = along_z(hidden)
        squares = sum(jnp.sum(jnp.square(p.astype(f32)), axis=1, keepdims=True) for p in pieces)
        squares = jnp.broadcast_to(squares, (own_rows, HEAD))
        squares = (squares + swap_cores(squares))[:, :1]
        mine = pick(pieces, level ^ me)
        came = [to_peer(pick(pieces, level ^ me ^ k), k) for k in range(1, peers)]
        half = jnp.concatenate([mine] + came, axis=0)
        parts = [half, swap_cores(half)]
        places = jnp.stack([core * slice_width, (1 - core) * slice_width]).astype(jnp.int32)
    else:
        full_rows = lax.all_gather(hidden, "tp", axis=1, tiled=True)
        squares = jnp.sum(jnp.square(full_rows.astype(f32)), axis=1, keepdims=True)
        columns = lax.all_to_all(full_rows, "ep", split_axis=1, concat_axis=0, tiled=True)
        columns = columns.reshape(peers, own_rows, slab)
        parts = [columns[me ^ jnp.arange(peers)].reshape(peers * own_rows, slab)]
        places = jnp.zeros((1,), jnp.int32)
    slab_gain = lax.dynamic_slice_in_dim(mix_gain, me * slab, slab, 0).reshape(1, slab)
    weights = (query_weight, key_weight, value_weight, gate_weight)
    partial = project(parts, places, slab_gain, weights, peers, own_rows)
    sums = [partial[0]] + [to_peer(partial[k], k) for k in range(1, peers)]

    mixed, next_state = retain(
        sums, squares, decay, cosine, sine, head_gain.reshape(1, width), ret_state, depth
    )

    lines = along_z(mixed)
    lines = jnp.stack(lines)
    other = swap_cores(lines)
    pieces = [lines[k] for k in range(levels)] + [other[k] for k in range(levels)]
    after, *packed = out_project(pieces, order * width, out_weight, hidden, placing, 4)

    packed = [jnp.concatenate([packed[k], shares[k]], axis=1) for k in range(peers)]
    arrived = [packed[0]] + [to_peer(packed[k], k) for k in range(1, peers)]
    arrived = jnp.concatenate(arrived, axis=0)
    table = arrived[:, slice_width : slice_width + 3 * local_experts].astype(f32)
    share_rows = jnp.sum(table.reshape(-1, 3, local_experts), axis=1).T[:, :, None]
    lines = jnp.stack(along_z(arrived[:, :slice_width]))
    other = swap_cores(lines)
    pieces = [lines[k] for k in range(levels)] + [other[k] for k in range(levels)]
    active = lift(pieces, order * slice_width, ffn_gain.reshape(1, depth), expert_gate, expert_up, 4)

    lines = jnp.stack(along_z(active))
    other = swap_cores(lines)
    pieces = [lines[k] for k in range(levels)] + [other[k] for k in range(levels)]
    back = lower(pieces, order * expert_gate.shape[2], expert_down, share_rows, peers, slots, 2)
    back = [back[0]] + [to_peer(back[k], k) for k in range(1, peers)]
    updated = after.astype(f32)
    for k in range(peers):
        updated = updated + lax.dot_general(
            placing[k], back[k], (((0,), (0,)), ((), ())), preferred_element_type=f32
        )
    return (updated.astype(bf16), next_state)


def solution(mesh):
    return jax.shard_map(
        per_device,
        mesh=mesh,
        in_specs=(
            P("ep", "tp"),
            P("ep"),
            P("ep", "tp", None, None),
            P("ep", "tp"),
            P("ep", "tp"),
            P("ep", "tp"),
            P("ep", "tp"),
            P("tp"),
            P(None, "tp"),
            P(),
            P(),
            P("ep", None, "tp"),
            P("ep", None, "tp"),
            P("ep", None, "tp"),
            P("ep", None),
            P("ep", None),
        ),
        out_specs=(P("ep", "tp"), P("ep", "tp", None, None)),
        check_vma=False,
    )
```

```python
import functools

import jax
import jax.numpy as jnp
from jax import lax
from jax.experimental import pallas as pl
from jax.experimental.pallas import tpu as pltpu
from jax.sharding import PartitionSpec as P

HEADS = 16
HEAD = 128
GROUPS = 4
TOP = 2
CORES = 2


epsilon = 1e-06
rope_base = 10000.0
f32 = jnp.float32
bf16 = jnp.bfloat16


def log_decay(head_ids):
    return jnp.log(1.0 - 2.0 ** (-5.0 - 5.0 * head_ids.astype(f32) / (HEADS - 1)))


def swap_cores(array):
    size = lax.axis_size("tp")
    return lax.ppermute(array, "tp", [(i, i ^ 1) for i in range(size)])


def along_z(array):
    size = lax.axis_size("tp")
    steps = range(1, size // CORES)
    return [array] + [
        lax.ppermute(array, "tp", [(i, i ^ (CORES * k)) for i in range(size)]) for k in steps
    ]


def to_peer(array, step):
    size = lax.axis_size("ep")
    return lax.ppermute(array, "ep", [(i, i ^ step) for i in range(size)])


def pick(pieces, index):
    chosen = pieces[0]
    for number in range(1, len(pieces)):
        chosen = jnp.where(index == number, pieces[number], chosen)
    return chosen


def whole(shape):
    rank = len(shape)
    return pl.BlockSpec(shape, lambda *_: (0,) * rank)


def near(array):
    return pltpu.with_memory_space_constraint(array, pltpu.VMEM)


def held():
    return pl.BlockSpec(memory_space=pltpu.VMEM)


def near_shape(shape, dtype):
    return pltpu.VMEM(shape, dtype)


def scalars():
    return pl.BlockSpec(memory_space=pltpu.SMEM)


def limit(mebibytes):
    return pltpu.CompilerParams(vmem_limit_bytes=mebibytes << 20)


def project_kernel(count, peers, rows, *refs):
    place_ref, gain_ref = refs[0], refs[1]
    parts = refs[2 : 2 + count]
    weights = refs[2 + count : 6 + count]
    outs = refs[6 + count :]
    width = weights[0].shape[1]
    totals = [None] * 4
    for number in range(count):
        part = parts[number]
        span = part.shape[1]
        start = pl.multiple_of(place_ref[number], 128)
        gain = gain_ref[:, pl.ds(start, span)]
        scaled = (part[...].astype(f32) * gain).astype(bf16)
        for which in range(4):
            block = weights[which][pl.ds(start, span), :]
            product = jnp.dot(scaled, block, preferred_element_type=f32)
            totals[which] = product if totals[which] is None else totals[which] + product
    for peer in range(peers):
        for which in range(4):
            rows_here = totals[which][peer * rows : (peer + 1) * rows, :]
            outs[peer][:, which * width : (which + 1) * width] = rows_here.astype(outs[peer].dtype)


def project(parts, places, gain, weights, peers, rows):
    width = weights[0].shape[1]
    out_shape = [near_shape((rows, 4 * width), f32)]
    out_shape += [near_shape((rows, 4 * width), bf16)] * (peers - 1)
    operands = [near(array) for array in (gain, *parts, *weights)]
    return pl.pallas_call(
        functools.partial(project_kernel, len(parts), peers, rows),
        out_shape=out_shape,
        in_specs=[scalars()] + [held()] * len(operands),
        out_specs=[held()] * peers,
        compiler_params=limit(8),
        name="project",
    )(places, *operands)


def retain_kernel(peers, heads, width_model, *refs):
    decay_ref, squares_ref, cos_ref, sin_ref, gain_ref = refs[:5]
    parts = refs[5 : 5 + peers]
    state_ref = refs[5 + peers]
    mixed_ref, next_ref = refs[6 + peers : 8 + peers]
    query_ref, key_ref, value_ref, gate_ref, read_ref = refs[8 + peers :]
    block = state_ref.shape[0]
    width = heads * HEAD

    @pl.when(pl.program_id(0) == 0)
    def first():
        factor = lax.rsqrt(squares_ref[...] * (1.0 / width_model) + epsilon)

        def total(which):
            cut = slice(which * width, (which + 1) * width)
            summed = parts[0][:, cut]
            for part in parts[1:]:
                summed = summed + part[:, cut].astype(f32)
            return (summed * factor).astype(bf16).astype(f32)

        query, key = total(0), total(1)
        for head in range(heads):
            cut = slice(head * HEAD, (head + 1) * HEAD)
            one = query[:, cut]
            query_ref[:, cut] = one * cos_ref[...] + pltpu.roll(one, HEAD // 2, 1) * sin_ref[...]
            two = key[:, cut]
            turned = two * cos_ref[...] + pltpu.roll(two, HEAD // 2, 1) * sin_ref[...]
            key_ref[:, cut] = turned * HEAD ** (-0.5)
        value_ref[...] = total(2)
        gate = total(3)
        gate_ref[...] = gate * jax.nn.sigmoid(gate) * gain_ref[...]

    start = pl.multiple_of(pl.program_id(0) * block, block)
    for head in range(heads):
        cut = slice(head * HEAD, (head + 1) * HEAD)
        query_columns = query_ref[pl.ds(start, block), cut].T
        key_columns = key_ref[pl.ds(start, block), cut].T
        value_rows = value_ref[pl.ds(start, block), cut]
        decay = decay_ref[head]
        for row in range(block):
            updated = (
                decay * state_ref[row, head]
                + key_columns[:, row : row + 1] * value_rows[row : row + 1, :]
            )
            next_ref[row, head] = updated
            read_ref[row : row + 1, :] = jnp.sum(
                query_columns[:, row : row + 1] * updated, axis=0, keepdims=True
            )
        read = read_ref[...]
        centered = read - jnp.mean(read, axis=-1, keepdims=True)
        spread = jnp.mean(centered * centered, axis=-1, keepdims=True)
        normal = centered * lax.rsqrt(spread + epsilon)
        mixed_ref[pl.ds(start, block), cut] = (normal * gate_ref[pl.ds(start, block), cut]).astype(bf16)


def retain(parts, squares, decay, cosine, sine, head_gain, ret_state, width_model):
    rows, heads = ret_state.shape[:2]
    width = heads * HEAD
    block = 8
    state_spec = pl.BlockSpec((block, heads, HEAD, HEAD), lambda i: (i, 0, 0, 0))
    operands = [near(array) for array in (squares, cosine, sine, head_gain, *parts)]
    return pl.pallas_call(
        functools.partial(retain_kernel, len(parts), heads, width_model),
        grid=(rows // block,),
        out_shape=[
            near_shape((rows, width), bf16),
            jax.ShapeDtypeStruct(ret_state.shape, f32),
        ],
        in_specs=[scalars()] + [held()] * len(operands) + [state_spec],
        out_specs=[held(), state_spec],
        scratch_shapes=[pltpu.VMEM((rows, width), f32)] * 4 + [pltpu.VMEM((block, HEAD), f32)],
        compiler_params=limit(10),
        name="retain",
    )(decay, *operands, ret_state)


def out_kernel(count, peers, *refs):
    place_ref = refs[0]
    pieces = refs[1 : 1 + count]
    weight_ref, hidden_ref = refs[1 + count : 3 + count]
    placing = refs[3 + count : 3 + count + peers]
    shares = refs[3 + count + peers : 3 + count + 2 * peers]
    after_ref = refs[3 + count + 2 * peers]
    outs = refs[4 + count + 2 * peers :]
    width = pieces[0].shape[1]
    total = hidden_ref[...].astype(f32)
    for number in range(count):
        block = weight_ref[pl.ds(pl.multiple_of(place_ref[number], 128), width), :]
        total = total + jnp.dot(pieces[number][...], block, preferred_element_type=f32)
    after = total.astype(bf16)
    after_ref[...] = after
    cut = after.shape[1]
    for peer in range(peers):
        sent = jnp.dot(placing[peer][...], after, preferred_element_type=f32)
        outs[peer][:, :cut] = sent.astype(bf16)
        outs[peer][:, cut:] = shares[peer][...]


def out_project(pieces, places, weight, hidden, placing, shares):
    rows, width = hidden.shape
    slots = placing[0].shape[0]
    peers = len(placing)
    operands = [near(array) for array in (*pieces, weight, hidden, *placing, *shares)]
    return pl.pallas_call(
        functools.partial(out_kernel, len(pieces), peers),
        out_shape=[near_shape((rows, width), bf16)]
        + [near_shape((slots, width + HEAD), bf16)] * peers,
        in_specs=[scalars()] + [held()] * len(operands),
        out_specs=[held()] * (1 + peers),
        compiler_params=limit(8),
        name="out_project",
    )(places, *operands)


def lift_kernel(count, depth, *refs):
    place_ref = refs[0]
    pieces = refs[1 : 1 + count]
    gain_ref, gate_ref, up_ref, active_ref = refs[1 + count :]
    width = pieces[0].shape[1]
    squares = None
    for piece in pieces:
        values = piece[...].astype(f32)
        here = jnp.sum(values * values, axis=-1, keepdims=True)
        squares = here if squares is None else squares + here
    factor = lax.rsqrt(squares * (1.0 / depth) + epsilon)
    experts = gate_ref.shape[0]
    gates, ups = [None] * experts, [None] * experts
    for number in range(count):
        start = pl.multiple_of(place_ref[number], 128)
        gain = gain_ref[:, pl.ds(start, width)]
        scaled = (pieces[number][...].astype(f32) * factor * gain).astype(bf16)
        for expert in range(experts):
            one = gate_ref[expert, pl.ds(start, width), :]
            two = up_ref[expert, pl.ds(start, width), :]
            gate = jnp.dot(scaled, one, preferred_element_type=f32)
            up = jnp.dot(scaled, two, preferred_element_type=f32)
            gates[expert] = gate if number == 0 else gates[expert] + gate
            ups[expert] = up if number == 0 else ups[expert] + up
    for expert in range(experts):
        gate = gates[expert]
        active_ref[expert] = (gate * jax.nn.sigmoid(gate) * ups[expert]).astype(bf16)


def lift(pieces, places, gain, expert_gate, expert_up):
    experts, depth, width = expert_gate.shape
    rows = pieces[0].shape[0]
    operands = [near(array) for array in (*pieces, gain, expert_gate, expert_up)]
    return pl.pallas_call(
        functools.partial(lift_kernel, len(pieces), depth),
        out_shape=near_shape((experts, rows, width), bf16),
        in_specs=[scalars()] + [held()] * len(operands),
        out_specs=held(),
        compiler_params=limit(8),
        name="lift",
    )(places, *operands)


def lower_kernel(count, peers, slots, *refs):
    place_ref = refs[0]
    pieces = refs[1 : 1 + count]
    down_ref = refs[1 + count]
    tables = refs[2 + count : 2 + count + peers]
    outs = refs[2 + count + peers : 2 + count + 2 * peers]
    mean_ref = refs[-1]
    experts, rows, width = pieces[0].shape
    totals = [None] * experts
    for number in range(count):
        start = pl.multiple_of(place_ref[number], 128)
        for expert in range(experts):
            block = down_ref[expert, pl.ds(start, width), :]
            product = jnp.dot(pieces[number][expert], block, preferred_element_type=f32)
            totals[expert] = product if number == 0 else totals[expert] + product
    for expert in range(experts):
        mean_ref[expert] = totals[expert].astype(bf16).astype(f32)
    cut = tables[0].shape[1] - HEAD
    for peer in range(peers):
        table = tables[peer][:, cut:].astype(f32)
        sent = None
        for expert in range(experts):
            share = (
                table[:, expert : expert + 1]
                + table[:, experts + expert : experts + expert + 1]
                + table[:, 2 * experts + expert : 2 * experts + expert + 1]
            )
            here = mean_ref[expert, peer * slots : (peer + 1) * slots, :] * share
            sent = here if sent is None else sent + here
        outs[peer][...] = sent.astype(bf16)


def lower(pieces, places, expert_down, tables):
    experts, depth, width = expert_down.shape
    rows = pieces[0].shape[1]
    peers, slots = len(tables), tables[0].shape[0]
    operands = [near(array) for array in (*pieces, expert_down, *tables)]
    return pl.pallas_call(
        functools.partial(lower_kernel, len(pieces), peers, slots),
        out_shape=[near_shape((slots, width), bf16)] * peers,
        in_specs=[scalars()] + [held()] * len(operands),
        out_specs=[held()] * peers,
        scratch_shapes=[pltpu.VMEM((experts, rows, width), f32)],
        compiler_params=limit(8),
        name="lower",
    )(places, *operands)


def finish_kernel(peers, *refs):
    after_ref = refs[0]
    placing = refs[1 : 1 + peers]
    back = refs[1 + peers : 1 + 2 * peers]
    updated_ref = refs[-1]
    total = after_ref[...].astype(f32)
    for peer in range(peers):
        total = total + lax.dot_general(
            placing[peer][...],
            back[peer][...],
            (((0,), (0,)), ((), ())),
            preferred_element_type=f32,
        )
    updated_ref[...] = total.astype(bf16)


def finish(after, placing, back):
    operands = [near(array) for array in (after, *placing, *back)]
    return pl.pallas_call(
        functools.partial(finish_kernel, len(placing)),
        out_shape=jax.ShapeDtypeStruct(after.shape, bf16),
        in_specs=[held()] * len(operands),
        out_specs=whole(after.shape),
        compiler_params=limit(4),
        name="finish",
    )(*operands)


def both_cores(array):
    lines = along_z(array)
    return lines + [swap_cores(line) for line in lines]


def per_device(
    hidden,
    positions,
    ret_state,
    query_weight,
    key_weight,
    value_weight,
    gate_weight,
    head_gain,
    out_weight,
    mix_gain,
    ffn_gain,
    expert_gate,
    expert_up,
    expert_down,
    route_ids,
    route_weight,
):
    own_rows, slice_width = hidden.shape
    peers = lax.axis_size("ep")
    ranks = lax.axis_size("tp")
    depth = slice_width * ranks
    slab = query_weight.shape[0]
    width = query_weight.shape[1]
    heads_here = width // HEAD
    me = lax.axis_index("ep")
    rank = lax.axis_index("tp")
    level, core = rank // CORES, rank % CORES
    levels = ranks // CORES
    order = jnp.stack(
        [(level ^ k) * CORES + core for k in range(levels)]
        + [(level ^ k) * CORES + (1 - core) for k in range(levels)]
    ).astype(jnp.int32)

    local_experts = expert_gate.shape[0]
    experts = local_experts * peers
    group_size = experts // GROUPS
    capacity = 2 * ((own_rows // GROUPS + group_size - 1) // group_size)
    slots = local_experts * capacity
    if local_experts % group_size == 0:
        slots = slots // TOP
    homes = route_ids // local_experts
    slot_of = route_ids % local_experts
    placing, shares = [], []
    for k in range(peers):
        here = homes == (me ^ k)
        goes = jnp.any(here, axis=1)
        slot = jnp.cumsum(goes.astype(jnp.int32)) - 1
        spot = (jnp.arange(slots, dtype=jnp.int32)[:, None] == slot[None, :]) & goes[None, :]
        spot = spot.astype(bf16)
        placing.append(spot)
        share = [
            jnp.sum(jnp.where(here & (slot_of == number), route_weight, 0.0), axis=1)
            for number in range(local_experts)
        ]
        share = jnp.stack(share, axis=1)
        high = share.astype(bf16)
        rest = share - high.astype(f32)
        mid = rest.astype(bf16)
        low = (rest - mid.astype(f32)).astype(bf16)
        table = jnp.concatenate([high, mid, low], axis=1)
        table = jnp.pad(table, ((0, 0), (0, HEAD - table.shape[1])))
        shares.append(jnp.dot(spot, table, preferred_element_type=f32).astype(bf16))

    inverse = 1.0 / rope_base ** (jnp.arange(0, HEAD, 2, dtype=f32) / HEAD)
    angle = positions.astype(f32)[:, None] * inverse[None, :]
    cosine, sine = jnp.cos(angle), jnp.sin(angle)
    cosine = jnp.concatenate([cosine, cosine], axis=1)
    sine = jnp.concatenate([-sine, sine], axis=1)
    head_ids = rank * heads_here + jnp.arange(heads_here, dtype=jnp.int32)
    decay = jnp.exp(log_decay(head_ids))

    if ranks == CORES * peers:
        pieces = along_z(hidden)
        squares = sum(jnp.sum(jnp.square(p.astype(f32)), axis=1, keepdims=True) for p in pieces)
        squares = jnp.broadcast_to(squares, (own_rows, HEAD))
        squares = (squares + swap_cores(squares))[:, :1]
        mine = pick(pieces, level ^ me)
        came = [to_peer(pick(pieces, level ^ me ^ k), k) for k in range(1, peers)]
        half = jnp.concatenate([mine] + came, axis=0)
        parts = [half, swap_cores(half)]
        places = jnp.stack([core * slice_width, (1 - core) * slice_width]).astype(jnp.int32)
    else:
        full_rows = lax.all_gather(hidden, "tp", axis=1, tiled=True)
        squares = jnp.sum(jnp.square(full_rows.astype(f32)), axis=1, keepdims=True)
        columns = lax.all_to_all(full_rows, "ep", split_axis=1, concat_axis=0, tiled=True)
        columns = columns.reshape(peers, own_rows, slab)
        parts = [columns[me ^ jnp.arange(peers)].reshape(peers * own_rows, slab)]
        places = jnp.zeros((1,), jnp.int32)
    slab_gain = lax.dynamic_slice_in_dim(mix_gain, me * slab, slab, 0).reshape(1, slab)
    weights = (query_weight, key_weight, value_weight, gate_weight)
    partial = project(parts, places, slab_gain, weights, peers, own_rows)
    sums = [partial[0]] + [to_peer(partial[k], k) for k in range(1, peers)]

    mixed, next_state = retain(
        sums, squares, decay, cosine, sine, head_gain.reshape(1, width), ret_state, depth
    )

    pieces = both_cores(mixed)
    after, *packed = out_project(pieces, order * width, out_weight, hidden, placing, shares)

    arrived = [packed[0]] + [to_peer(packed[k], k) for k in range(1, peers)]
    pieces = both_cores(jnp.concatenate([table[:, :slice_width] for table in arrived], axis=0))
    active = lift(pieces, order * slice_width, ffn_gain.reshape(1, depth), expert_gate, expert_up)

    pieces = both_cores(active)
    back = lower(pieces, order * expert_gate.shape[2], expert_down, arrived)
    back = [back[0]] + [to_peer(back[k], k) for k in range(1, peers)]
    return (finish(after, placing, back), next_state)


def solution(mesh):
    return jax.shard_map(
        per_device,
        mesh=mesh,
        in_specs=(
            P("ep", "tp"),
            P("ep"),
            P("ep", "tp", None, None),
            P("ep", "tp"),
            P("ep", "tp"),
            P("ep", "tp"),
            P("ep", "tp"),
            P("tp"),
            P(None, "tp"),
            P(),
            P(),
            P("ep", None, "tp"),
            P("ep", None, "tp"),
            P("ep", None, "tp"),
            P("ep", None),
            P("ep", None),
        ),
        out_specs=(P("ep", "tp"), P("ep", "tp", None, None)),
        check_vma=False,
    )
```

```python
import functools

import jax
import jax.numpy as jnp
from jax import lax
from jax.experimental import pallas as pl
from jax.experimental.pallas import tpu as pltpu
from jax.sharding import PartitionSpec as P

HEADS = 16
HEAD = 128
GROUPS = 4
TOP = 2
CORES = 2


epsilon = 1e-06
rope_base = 10000.0
f32 = jnp.float32
bf16 = jnp.bfloat16


def swap_cores(array):
    size = lax.axis_size("tp")
    return lax.ppermute(array, "tp", [(i, i ^ 1) for i in range(size)])


def along_z(array):
    size = lax.axis_size("tp")
    steps = range(1, size // CORES)
    return [array] + [
        lax.ppermute(array, "tp", [(i, i ^ (CORES * k)) for i in range(size)]) for k in steps
    ]


def to_peer(array, step):
    size = lax.axis_size("ep")
    return lax.ppermute(array, "ep", [(i, i ^ step) for i in range(size)])


def spots(count, width):
    level, core = lax.axis_index("tp") // CORES, lax.axis_index("tp") % CORES
    half = count // 2
    tables = [(level ^ k) * CORES + core for k in range(half)]
    tables += [(level ^ k) * CORES + (1 - core) for k in range(half)]
    return [pl.multiple_of(table * width, 128) for table in tables]


def near(array):
    return pltpu.with_memory_space_constraint(array, pltpu.VMEM)


def held():
    return pl.BlockSpec(memory_space=pltpu.VMEM)


def near_shape(shape, dtype):
    return pltpu.VMEM(shape, dtype)


def limit(mebibytes):
    return pltpu.CompilerParams(vmem_limit_bytes=mebibytes << 20)


def cost(microseconds):
    work = int(microseconds * 2.5e9)
    return pl.CostEstimate(flops=work, bytes_accessed=int(microseconds * 1.5e7), transcendentals=0)


def whole(shape):
    rank = len(shape)
    return pl.BlockSpec(shape, lambda *_: (0,) * rank)


def prepare_kernel(peers, experts, slots, ids_ref, share_ref, *outs):
    me = lax.axis_index("ep")
    rows = ids_ref.shape[1]
    ids = ids_ref[...]
    picks = [ids[number : number + 1, :] for number in range(TOP)]
    line = lax.broadcasted_iota(jnp.int32, (max(peers, 8), rows), 0)
    goes = None
    for pick in picks:
        hit = pick // experts == (line ^ me)
        goes = hit if goes is None else goes | hit
    row = lax.broadcasted_iota(jnp.int32, (rows, rows), 0)
    column = lax.broadcasted_iota(jnp.int32, (rows, rows), 1)
    before = (row < column).astype(f32).astype(bf16)
    counts = jnp.dot(goes.astype(f32).astype(bf16), before, preferred_element_type=f32)
    slot = jnp.where(goes, counts, -1.0)
    share = share_ref[...]
    line = lax.broadcasted_iota(jnp.int32, (HEAD, rows), 0)
    target = lax.broadcasted_iota(jnp.int32, (slots, rows), 0).astype(f32)
    for peer in range(peers):
        spot = (slot[peer : peer + 1, :] == target).astype(f32).astype(bf16)
        outs[peer][...] = spot
        table = jnp.zeros((HEAD, rows), f32)
        for expert in range(experts):
            number = (me ^ peer) * experts + expert
            weight = jnp.zeros((1, rows), f32)
            for pick in range(TOP):
                weight += jnp.where(picks[pick] == number, share[pick : pick + 1, :], 0.0)
            high = weight.astype(bf16).astype(f32)
            mid = (weight - high).astype(bf16).astype(f32)
            low = weight - high - mid
            table = jnp.where(line == expert, high, table)
            table = jnp.where(line == experts + expert, mid, table)
            table = jnp.where(line == 2 * experts + expert, low, table)
        moved = lax.dot_general(
            spot, table.astype(bf16), (((1,), (1,)), ((), ())), preferred_element_type=f32
        )
        outs[peers + peer][...] = moved.astype(bf16)


def prepare(route_ids, route_weight, peers, experts, slots):
    rows = route_ids.shape[0]
    outs = pl.pallas_call(
        functools.partial(prepare_kernel, peers, experts, slots),
        out_shape=[near_shape((slots, rows), bf16)] * peers
        + [near_shape((slots, HEAD), bf16)] * peers,
        in_specs=[held()] * 2,
        out_specs=[held()] * (2 * peers),
        compiler_params=limit(4),
        cost_estimate=cost(2),
        name="prepare",
    )(near(route_ids.T), near(route_weight.T))
    return outs[:peers], outs[peers:]


def sort_kernel(count, *refs):
    pieces = refs[:count]
    outs = refs[-1 - count : -1]
    squares_ref = refs[-1]
    level = lax.axis_index("tp") // CORES
    me = lax.axis_index("ep")
    values = [piece[...] for piece in pieces]
    for peer in range(count):
        wanted = level ^ me ^ peer
        chosen = values[0]
        for number in range(1, count):
            chosen = jnp.where(wanted == number, values[number], chosen)
        outs[peer][...] = chosen
    total = None
    for value in values:
        wide = value.astype(f32)
        here = jnp.sum(wide * wide, axis=-1, keepdims=True)
        total = here if total is None else total + here
    squares_ref[...] = jnp.broadcast_to(total, squares_ref.shape)


def sort_pieces(pieces, earlier):
    rows, width = pieces[0].shape
    count = len(pieces)
    outs = pl.pallas_call(
        functools.partial(sort_kernel, count),
        out_shape=[near_shape((rows, width), bf16)] * count + [near_shape((rows, HEAD), f32)],
        in_specs=[held()] * (count + len(earlier)),
        out_specs=[held()] * (count + 1),
        compiler_params=limit(4),
        cost_estimate=cost(1),
        name="sort",
    )(*[near(array) for array in (*pieces, *earlier)])
    return outs[:count], outs[count]


def project_kernel(count, peers, rows, *refs):
    gain_ref = refs[0]
    parts = refs[1 : 1 + count]
    weights = refs[1 + count : 5 + count]
    outs = refs[5 + count :]
    slab, width = weights[0].shape
    core = lax.axis_index("tp") % CORES
    base = lax.axis_index("ep") * slab
    totals = [None] * 4
    for number in range(count):
        part = parts[number]
        span = part.shape[1]
        place = (core ^ number) * span if count > 1 else 0
        start = pl.multiple_of(place, 128)
        gain = gain_ref[:, pl.ds(pl.multiple_of(base + place, 128), span)]
        scaled = (part[...].astype(f32) * gain).astype(bf16)
        for which in range(4):
            block = weights[which][pl.ds(start, span), :]
            product = jnp.dot(scaled, block, preferred_element_type=f32)
            totals[which] = product if totals[which] is None else totals[which] + product
    for peer in range(peers):
        for which in range(4):
            rows_here = totals[which][peer * rows : (peer + 1) * rows, :]
            outs[peer][:, which * width : (which + 1) * width] = rows_here.astype(outs[peer].dtype)


def project(parts, gain, weights, peers, rows):
    width = weights[0].shape[1]
    out_shape = [near_shape((rows, 4 * width), f32)]
    out_shape += [near_shape((rows, 4 * width), bf16)] * (peers - 1)
    operands = [near(array) for array in (gain, *parts, *weights)]
    return pl.pallas_call(
        functools.partial(project_kernel, len(parts), peers, rows),
        out_shape=out_shape,
        in_specs=[held()] * len(operands),
        out_specs=[held()] * peers,
        compiler_params=limit(8),
        cost_estimate=cost(2),
        name="project",
    )(*operands)


def decay_of(head, heads):
    number = (lax.axis_index("tp") * heads + head).astype(f32)
    power = jnp.full((1, HEAD), -5.0, f32) - number * (5.0 / (HEADS - 1))
    return 1.0 - jnp.exp2(power)


def read_kernel(peers, heads, width_model, *refs):
    squares, cos_ref, sin_ref, gain_ref = refs[0:2], refs[2], refs[3], refs[4]
    parts = refs[5 : 5 + peers]
    state_ref = refs[5 + peers]
    mixed_ref, key_ref, value_ref = refs[6 + peers : 9 + peers]
    query_ref, read_ref = refs[9 + peers :]
    rows, width = mixed_ref.shape
    mean = (squares[0][:, :1] + squares[1][:, :1]) * (1.0 / width_model)
    factor = lax.rsqrt(mean + epsilon)

    def total(which):
        cut = slice(which * width, (which + 1) * width)
        summed = parts[0][:, cut]
        for part in parts[1:]:
            summed = summed + part[:, cut].astype(f32)
        return (summed * factor).astype(bf16).astype(f32)

    query, key, value = total(0), total(1), total(2)
    value_ref[...] = value
    gate = total(3)
    gate = gate * jax.nn.sigmoid(gate) * gain_ref[...]
    own = []
    for head in range(heads):
        cut = slice(head * HEAD, (head + 1) * HEAD)
        one, two = query[:, cut], key[:, cut]
        one = one * cos_ref[...] + pltpu.roll(one, HEAD // 2, 1) * sin_ref[...]
        two = two * cos_ref[...] + pltpu.roll(two, HEAD // 2, 1) * sin_ref[...]
        two = two * HEAD ** (-0.5)
        query_ref[:, cut] = one
        key_ref[:, cut] = two
        own.append(jnp.sum(one * two, axis=-1, keepdims=True) * value[:, cut])
    block = 8

    def some(number, carry):
        start = pl.multiple_of(number * block, block)
        for head in range(heads):
            cut = slice(head * HEAD, (head + 1) * HEAD)
            columns = query_ref[pl.ds(start, block), cut].T
            found = [
                jnp.sum(columns[:, row : row + 1] * state_ref[start + row, head], axis=0, keepdims=True)
                for row in range(block)
            ]
            read_ref[pl.ds(start, block), cut] = jnp.concatenate(found, axis=0)
        return carry

    lax.fori_loop(0, rows // block, some, 0)
    for head in range(heads):
        cut = slice(head * HEAD, (head + 1) * HEAD)
        read = decay_of(head, heads) * read_ref[:, cut] + own[head]
        centered = read - jnp.mean(read, axis=-1, keepdims=True)
        spread = jnp.mean(centered * centered, axis=-1, keepdims=True)
        normal = centered * lax.rsqrt(spread + epsilon)
        mixed_ref[:, cut] = (normal * gate[:, cut]).astype(bf16)


def read_state(parts, squares, cosine, sine, head_gain, ret_state, width_model):
    rows, heads = ret_state.shape[:2]
    width = heads * HEAD
    operands = [near(a) for a in (*squares, cosine, sine, head_gain, *parts, ret_state)]
    return pl.pallas_call(
        functools.partial(read_kernel, len(parts), heads, width_model),
        out_shape=[
            near_shape((rows, width), bf16),
            near_shape((rows, width), f32),
            near_shape((rows, width), f32),
        ],
        in_specs=[held()] * len(operands),
        out_specs=[held()] * 3,
        scratch_shapes=[pltpu.VMEM((rows, width), f32)] * 2,
        compiler_params=limit(4),
        cost_estimate=cost(2),
        name="read_state",
    )(*operands)


def update_kernel(heads, key_ref, value_ref, state_ref, next_ref):
    block = next_ref.shape[0]
    start = pl.multiple_of(pl.program_id(0) * block, block)
    for head in range(heads):
        cut = slice(head * HEAD, (head + 1) * HEAD)
        columns = key_ref[pl.ds(start, block), cut].T
        values = value_ref[pl.ds(start, block), cut]
        decay = decay_of(head, heads)
        for row in range(block):
            next_ref[row, head] = (
                decay * state_ref[start + row, head]
                + columns[:, row : row + 1] * values[row : row + 1, :]
            )


def update_state(key, value, ret_state):
    rows, heads = ret_state.shape[:2]
    block = 8
    return pl.pallas_call(
        functools.partial(update_kernel, heads),
        grid=(rows // block,),
        out_shape=jax.ShapeDtypeStruct(ret_state.shape, f32),
        in_specs=[held()] * 3,
        out_specs=pl.BlockSpec((block, heads, HEAD, HEAD), lambda i: (i, 0, 0, 0)),
        compiler_params=limit(6),
        cost_estimate=cost(3),
        name="update_state",
    )(near(key), near(value), near(ret_state))


def out_kernel(count, peers, *refs):
    pieces = refs[:count]
    weight_ref, hidden_ref = refs[count : 2 + count]
    placing = refs[2 + count : 2 + count + peers]
    shares = refs[2 + count + peers : 2 + count + 2 * peers]
    after_ref = refs[2 + count + 2 * peers]
    outs = refs[3 + count + 2 * peers :]
    width = pieces[0].shape[1]
    places = spots(count, width)
    total = hidden_ref[...].astype(f32)
    for number in range(count):
        block = weight_ref[pl.ds(places[number], width), :]
        total = total + jnp.dot(pieces[number][...], block, preferred_element_type=f32)
    after = total.astype(bf16)
    after_ref[...] = after
    cut = after.shape[1]
    for peer in range(peers):
        sent = jnp.dot(placing[peer][...], after, preferred_element_type=f32)
        outs[peer][:, :cut] = sent.astype(bf16)
        outs[peer][:, cut:] = shares[peer][...]


def out_project(pieces, weight, hidden, placing, shares):
    rows, width = hidden.shape
    slots = placing[0].shape[0]
    peers = len(placing)
    operands = [near(array) for array in (*pieces, weight, hidden, *placing, *shares)]
    return pl.pallas_call(
        functools.partial(out_kernel, len(pieces), peers),
        out_shape=[near_shape((rows, width), bf16)]
        + [near_shape((slots, width + HEAD), bf16)] * peers,
        in_specs=[held()] * len(operands),
        out_specs=[held()] * (1 + peers),
        compiler_params=limit(8),
        cost_estimate=cost(2),
        name="out_project",
    )(*operands)


def lift_kernel(count, depth, *refs):
    pieces = refs[:count]
    gain_ref, gate_ref, up_ref, active_ref = refs[count:]
    width = pieces[0].shape[1]
    places = spots(count, width)
    squares = None
    for piece in pieces:
        values = piece[...].astype(f32)
        here = jnp.sum(values * values, axis=-1, keepdims=True)
        squares = here if squares is None else squares + here
    factor = lax.rsqrt(squares * (1.0 / depth) + epsilon)
    experts = gate_ref.shape[0]
    gates, ups = [None] * experts, [None] * experts
    for number in range(count):
        start = places[number]
        gain = gain_ref[:, pl.ds(start, width)]
        scaled = (pieces[number][...].astype(f32) * factor * gain).astype(bf16)
        for expert in range(experts):
            one = gate_ref[expert, pl.ds(start, width), :]
            two = up_ref[expert, pl.ds(start, width), :]
            gate = jnp.dot(scaled, one, preferred_element_type=f32)
            up = jnp.dot(scaled, two, preferred_element_type=f32)
            gates[expert] = gate if number == 0 else gates[expert] + gate
            ups[expert] = up if number == 0 else ups[expert] + up
    for expert in range(experts):
        gate = gates[expert]
        active_ref[expert] = (gate * jax.nn.sigmoid(gate) * ups[expert]).astype(bf16)


def lift(pieces, gain, expert_gate, expert_up):
    experts, depth, width = expert_gate.shape
    rows = pieces[0].shape[0]
    operands = [near(array) for array in (*pieces, gain, expert_gate, expert_up)]
    return pl.pallas_call(
        functools.partial(lift_kernel, len(pieces), depth),
        out_shape=near_shape((experts, rows, width), bf16),
        in_specs=[held()] * len(operands),
        out_specs=held(),
        compiler_params=limit(8),
        cost_estimate=cost(3),
        name="lift",
    )(*operands)


def lower_kernel(count, peers, slots, *refs):
    pieces = refs[:count]
    down_ref = refs[count]
    tables = refs[1 + count : 1 + count + peers]
    outs = refs[1 + count + peers : 1 + count + 2 * peers]
    mean_ref = refs[-1]
    experts, rows, width = pieces[0].shape
    places = spots(count, width)
    totals = [None] * experts
    for number in range(count):
        start = places[number]
        for expert in range(experts):
            block = down_ref[expert, pl.ds(start, width), :]
            product = jnp.dot(pieces[number][expert], block, preferred_element_type=f32)
            totals[expert] = product if number == 0 else totals[expert] + product
    for expert in range(experts):
        mean_ref[expert] = totals[expert].astype(bf16).astype(f32)
    cut = tables[0].shape[1] - HEAD
    for peer in range(peers):
        table = tables[peer][:, cut:].astype(f32)
        sent = None
        for expert in range(experts):
            share = (
                table[:, expert : expert + 1]
                + table[:, experts + expert : experts + expert + 1]
                + table[:, 2 * experts + expert : 2 * experts + expert + 1]
            )
            here = mean_ref[expert, peer * slots : (peer + 1) * slots, :] * share
            sent = here if sent is None else sent + here
        outs[peer][...] = sent.astype(bf16)


def lower(pieces, expert_down, tables):
    experts, depth, width = expert_down.shape
    rows = pieces[0].shape[1]
    peers, slots = len(tables), tables[0].shape[0]
    operands = [near(array) for array in (*pieces, expert_down, *tables)]
    return pl.pallas_call(
        functools.partial(lower_kernel, len(pieces), peers, slots),
        out_shape=[near_shape((slots, width), bf16)] * peers,
        in_specs=[held()] * len(operands),
        out_specs=[held()] * peers,
        scratch_shapes=[pltpu.VMEM((experts, rows, width), f32)],
        compiler_params=limit(8),
        cost_estimate=cost(2),
        name="lower",
    )(*operands)


def finish_kernel(peers, *refs):
    after_ref = refs[0]
    placing = refs[1 : 1 + peers]
    back = refs[1 + peers : 1 + 2 * peers]
    updated_ref = refs[-1]
    total = after_ref[...].astype(f32)
    for peer in range(peers):
        total = total + lax.dot_general(
            placing[peer][...],
            back[peer][...],
            (((0,), (0,)), ((), ())),
            preferred_element_type=f32,
        )
    updated_ref[...] = total.astype(bf16)


def finish(after, placing, back):
    operands = [near(array) for array in (after, *placing, *back)]
    return pl.pallas_call(
        functools.partial(finish_kernel, len(placing)),
        out_shape=jax.ShapeDtypeStruct(after.shape, bf16),
        in_specs=[held()] * len(operands),
        out_specs=whole(after.shape),
        compiler_params=limit(4),
        cost_estimate=cost(1),
        name="finish",
    )(*operands)


def both_cores(array):
    lines = along_z(array)
    return lines + [swap_cores(line) for line in lines]


def per_device(
    hidden,
    positions,
    ret_state,
    query_weight,
    key_weight,
    value_weight,
    gate_weight,
    head_gain,
    out_weight,
    mix_gain,
    ffn_gain,
    expert_gate,
    expert_up,
    expert_down,
    route_ids,
    route_weight,
):
    own_rows, slice_width = hidden.shape
    peers = lax.axis_size("ep")
    ranks = lax.axis_size("tp")
    depth = slice_width * ranks
    slab, width = query_weight.shape

    local_experts = expert_gate.shape[0]
    group_size = local_experts * peers // GROUPS
    capacity = 2 * ((own_rows // GROUPS + group_size - 1) // group_size)
    slots = local_experts * capacity
    if local_experts % group_size == 0:
        slots = slots // TOP
    placing, shares = prepare(route_ids, route_weight, peers, local_experts, slots)

    inverse = 1.0 / rope_base ** (jnp.arange(0, HEAD, 2, dtype=f32) / HEAD)
    angle = positions.astype(f32)[:, None] * inverse[None, :]
    cosine, sine = jnp.cos(angle), jnp.sin(angle)
    cosine = jnp.concatenate([cosine, cosine], axis=1)
    sine = jnp.concatenate([-sine, sine], axis=1)

    if ranks == CORES * peers:
        sorted_pieces, squares = sort_pieces(along_z(hidden), (shares[0], cosine, sine))
        squares = [squares, swap_cores(squares)]
        came = [to_peer(sorted_pieces[k], k) for k in range(1, peers)]
        half = jnp.concatenate([sorted_pieces[0]] + came, axis=0)
        parts = [half, swap_cores(half)]
    else:
        me = lax.axis_index("ep")
        full_rows = lax.all_gather(hidden, "tp", axis=1, tiled=True)
        squares = jnp.sum(jnp.square(full_rows.astype(f32)), axis=1, keepdims=True)
        squares = [squares, jnp.zeros_like(squares)]
        columns = lax.all_to_all(full_rows, "ep", split_axis=1, concat_axis=0, tiled=True)
        columns = columns.reshape(peers, own_rows, slab)
        parts = [columns[me ^ jnp.arange(peers)].reshape(peers * own_rows, slab)]
    weights = (query_weight, key_weight, value_weight, gate_weight)
    partial = project(parts, mix_gain.reshape(1, depth), weights, peers, own_rows)
    sums = [partial[0]] + [to_peer(partial[k], k) for k in range(1, peers)]

    mixed, key, value = read_state(
        sums, squares, cosine, sine, head_gain.reshape(1, width), ret_state, depth
    )
    next_state = update_state(key, value, ret_state)

    pieces = both_cores(mixed)
    after, *packed = out_project(pieces, out_weight, hidden, placing, shares)
    packed, next_state = lax.optimization_barrier((packed, next_state))

    arrived = [packed[0]] + [to_peer(packed[k], k) for k in range(1, peers)]
    pieces = both_cores(jnp.concatenate([table[:, :slice_width] for table in arrived], axis=0))
    active = lift(pieces, ffn_gain.reshape(1, depth), expert_gate, expert_up)

    pieces = both_cores(active)
    back = lower(pieces, expert_down, arrived)
    back = [back[0]] + [to_peer(back[k], k) for k in range(1, peers)]
    return (finish(after, placing, back), next_state)


def solution(mesh):
    return jax.shard_map(
        per_device,
        mesh=mesh,
        in_specs=(
            P("ep", "tp"),
            P("ep"),
            P("ep", "tp", None, None),
            P("ep", "tp"),
            P("ep", "tp"),
            P("ep", "tp"),
            P("ep", "tp"),
            P("tp"),
            P(None, "tp"),
            P(),
            P(),
            P("ep", None, "tp"),
            P("ep", None, "tp"),
            P("ep", None, "tp"),
            P("ep", None),
            P("ep", None),
        ),
        out_specs=(P("ep", "tp"), P("ep", "tp", None, None)),
        check_vma=False,
    )
```

```python
import functools

import jax
import jax.numpy as jnp
from jax import lax
from jax.experimental import pallas as pl
from jax.experimental.pallas import tpu as pltpu
from jax.sharding import PartitionSpec as P

HEADS = 16
HEAD = 128
GROUPS = 4
TOP = 2
CORES = 2


epsilon = 1e-06
rope_base = 10000.0
f32 = jnp.float32
bf16 = jnp.bfloat16


def swap_cores(array):
    size = lax.axis_size("tp")
    return lax.ppermute(array, "tp", [(i, i ^ 1) for i in range(size)])


def along_z(array):
    size = lax.axis_size("tp")
    found = [array]
    for k in range(1, size // CORES):
        found.append(lax.ppermute(array, "tp", [(i, i ^ (CORES * k)) for i in range(size)]))
    return found


def to_peers(arrays):
    size = lax.axis_size("ep")
    found = [arrays[0]]
    for k in range(1, size):
        found.append(lax.ppermute(arrays[k], "ep", [(i, i ^ k) for i in range(size)]))
    return found


def split_pieces(refs, levels):
    own, rest, other, others = refs
    rows = own.shape[-2]
    found = []
    for one, many in ((own, rest), (other, others)):
        found.append(one)
        found += [many.at[..., pl.ds(k * rows, rows), :] for k in range(levels - 1)]
    return found


def spots(count, width):
    level, core = lax.axis_index("tp") // CORES, lax.axis_index("tp") % CORES
    half = count // 2
    tables = [(level ^ k) * CORES + core for k in range(half)]
    tables += [(level ^ k) * CORES + (1 - core) for k in range(half)]
    return [pl.multiple_of(table * width, 128) for table in tables]


def near(array):
    return pltpu.with_memory_space_constraint(array, pltpu.VMEM)


def held():
    return pl.BlockSpec(memory_space=pltpu.VMEM)


def near_shape(shape, dtype):
    return pltpu.VMEM(shape, dtype)


def limit(mebibytes):
    return pltpu.CompilerParams(vmem_limit_bytes=mebibytes << 20)


def cost(microseconds):
    work = int(microseconds * 2.5e9)
    return pl.CostEstimate(flops=work, bytes_accessed=int(microseconds * 1.5e7), transcendentals=0)


def whole(shape):
    rank = len(shape)
    return pl.BlockSpec(shape, lambda *_: (0,) * rank)


def prepare_kernel(peers, experts, slots, ids_ref, share_ref, *outs):
    me = lax.axis_index("ep")
    rows = ids_ref.shape[1]
    ids = ids_ref[...]
    picks = [ids[number : number + 1, :] for number in range(TOP)]
    line = lax.broadcasted_iota(jnp.int32, (max(peers, 8), rows), 0)
    goes = None
    for pick in picks:
        hit = pick // experts == (line ^ me)
        goes = hit if goes is None else goes | hit
    row = lax.broadcasted_iota(jnp.int32, (rows, rows), 0)
    column = lax.broadcasted_iota(jnp.int32, (rows, rows), 1)
    before = (row < column).astype(f32).astype(bf16)
    counts = jnp.dot(goes.astype(f32).astype(bf16), before, preferred_element_type=f32)
    slot = jnp.where(goes, counts, -1.0)
    share = share_ref[...]
    line = lax.broadcasted_iota(jnp.int32, (HEAD, rows), 0)
    target = lax.broadcasted_iota(jnp.int32, (slots, rows), 0).astype(f32)
    for peer in range(peers):
        spot = (slot[peer : peer + 1, :] == target).astype(f32).astype(bf16)
        outs[peer][...] = spot
        table = jnp.zeros((HEAD, rows), f32)
        for expert in range(experts):
            number = (me ^ peer) * experts + expert
            weight = jnp.zeros((1, rows), f32)
            for pick in range(TOP):
                weight += jnp.where(picks[pick] == number, share[pick : pick + 1, :], 0.0)
            high = weight.astype(bf16).astype(f32)
            mid = (weight - high).astype(bf16).astype(f32)
            low = weight - high - mid
            table = jnp.where(line == expert, high, table)
            table = jnp.where(line == experts + expert, mid, table)
            table = jnp.where(line == 2 * experts + expert, low, table)
        moved = lax.dot_general(
            spot, table.astype(bf16), (((1,), (1,)), ((), ())), preferred_element_type=f32
        )
        outs[peers + peer][...] = moved.astype(bf16)


def prepare(route_ids, route_weight, peers, experts, slots):
    rows = route_ids.shape[0]
    outs = pl.pallas_call(
        functools.partial(prepare_kernel, peers, experts, slots),
        out_shape=[near_shape((slots, rows), bf16)] * peers
        + [near_shape((slots, HEAD), bf16)] * peers,
        in_specs=[held()] * 2,
        out_specs=[held()] * (2 * peers),
        compiler_params=limit(4),
        cost_estimate=cost(2),
        name="prepare",
    )(near(route_ids.T), near(route_weight.T))
    return outs[:peers], outs[peers:]


def sort_kernel(count, *refs):
    pieces = refs[:count]
    outs = refs[-1 - count : -1]
    squares_ref = refs[-1]
    level = lax.axis_index("tp") // CORES
    me = lax.axis_index("ep")
    values = [piece[...] for piece in pieces]
    for peer in range(count):
        wanted = level ^ me ^ peer
        chosen = values[0]
        for number in range(1, count):
            chosen = jnp.where(wanted == number, values[number], chosen)
        outs[peer][...] = chosen
    total = None
    for value in values:
        wide = value.astype(f32)
        here = jnp.sum(wide * wide, axis=-1, keepdims=True)
        total = here if total is None else total + here
    squares_ref[...] = jnp.broadcast_to(total, squares_ref.shape)


def sort_pieces(pieces, earlier):
    rows, width = pieces[0].shape
    count = len(pieces)
    outs = pl.pallas_call(
        functools.partial(sort_kernel, count),
        out_shape=[near_shape((rows, width), bf16)] * count + [near_shape((rows, HEAD), f32)],
        in_specs=[held()] * (count + len(earlier)),
        out_specs=[held()] * (count + 1),
        compiler_params=limit(4),
        cost_estimate=cost(1),
        name="sort",
    )(*[near(array) for array in (*pieces, *earlier)])
    return outs[:count], outs[count]


def project_kernel(count, peers, rows, *refs):
    gain_ref = refs[0]
    parts = refs[1 : 1 + count]
    weights = refs[1 + count : 5 + count]
    outs = refs[5 + count :]
    slab, width = weights[0].shape
    core = lax.axis_index("tp") % CORES
    base = lax.axis_index("ep") * slab
    totals = [None] * 4
    for number in range(count):
        part = parts[number]
        span = part.shape[1]
        place = (core ^ number) * span if count > 1 else 0
        start = pl.multiple_of(place, 128)
        gain = gain_ref[:, pl.ds(pl.multiple_of(base + place, 128), span)]
        scaled = (part[...].astype(f32) * gain).astype(bf16)
        for which in range(4):
            block = weights[which][pl.ds(start, span), :]
            product = jnp.dot(scaled, block, preferred_element_type=f32)
            totals[which] = product if totals[which] is None else totals[which] + product
    for peer in range(peers):
        for which in range(4):
            rows_here = totals[which][peer * rows : (peer + 1) * rows, :]
            outs[peer][:, which * width : (which + 1) * width] = rows_here.astype(outs[peer].dtype)


def project(parts, gain, weights, peers, rows):
    width = weights[0].shape[1]
    out_shape = [near_shape((rows, 4 * width), f32)]
    out_shape += [near_shape((rows, 4 * width), bf16)] * (peers - 1)
    operands = [near(array) for array in (gain, *parts, *weights)]
    return pl.pallas_call(
        functools.partial(project_kernel, len(parts), peers, rows),
        out_shape=out_shape,
        in_specs=[held()] * len(operands),
        out_specs=[held()] * peers,
        compiler_params=limit(8),
        cost_estimate=cost(2),
        name="project",
    )(*operands)


def blocks_of(block):
    row = lax.broadcasted_iota(jnp.int32, (block, block * HEAD), 0)
    lane = lax.broadcasted_iota(jnp.int32, (block, block * HEAD), 1)
    return (lane // HEAD == row).astype(f32)


def columns_times(rows, table):
    high = rows.astype(bf16).astype(f32)
    mid = (rows - high).astype(bf16).astype(f32)
    split = jnp.concatenate([high, mid, rows - high - mid], axis=0).astype(bf16)
    return lax.dot_general(split, table, (((0,), (0,)), ((), ())), preferred_element_type=f32)


def decay_of(head, heads):
    number = (lax.axis_index("tp") * heads + head).astype(f32)
    power = jnp.full((1, HEAD), -5.0, f32) - number * (5.0 / (HEADS - 1))
    return 1.0 - jnp.exp2(power)


def read_kernel(peers, heads, width_model, *refs):
    squares, cos_ref, sin_ref, gain_ref = refs[0:2], refs[2], refs[3], refs[4]
    parts = refs[5 : 5 + peers]
    state_ref = refs[5 + peers]
    mixed_ref, key_ref, value_ref = refs[6 + peers : 9 + peers]
    query_ref, read_ref = refs[9 + peers :]
    rows, width = mixed_ref.shape
    mean = (squares[0][:, :1] + squares[1][:, :1]) * (1.0 / width_model)
    factor = lax.rsqrt(mean + epsilon)

    def total(which):
        cut = slice(which * width, (which + 1) * width)
        summed = parts[0][:, cut]
        for part in parts[1:]:
            summed = summed + part[:, cut].astype(f32)
        return (summed * factor).astype(bf16).astype(f32)

    query, key, value = total(0), total(1), total(2)
    value_ref[...] = value
    gate = total(3)
    gate = gate * jax.nn.sigmoid(gate) * gain_ref[...]
    own = []
    for head in range(heads):
        cut = slice(head * HEAD, (head + 1) * HEAD)
        one, two = query[:, cut], key[:, cut]
        one = one * cos_ref[...] + pltpu.roll(one, HEAD // 2, 1) * sin_ref[...]
        two = two * cos_ref[...] + pltpu.roll(two, HEAD // 2, 1) * sin_ref[...]
        two = two * HEAD ** (-0.5)
        query_ref[:, cut] = one
        key_ref[:, cut] = two
        own.append(jnp.sum(one * two, axis=-1, keepdims=True) * value[:, cut])
    block = 8
    mask = blocks_of(block)
    ones = jnp.concatenate([mask] * 3, axis=0).astype(bf16)

    def some(number, carry):
        start = pl.multiple_of(number * block, block)
        for head in range(heads):
            cut = slice(head * HEAD, (head + 1) * HEAD)
            spread = columns_times(query_ref[pl.ds(start, block), cut], ones)
            found = [
                jnp.sum(
                    spread[:, row * HEAD : (row + 1) * HEAD] * state_ref[start + row, head],
                    axis=0,
                    keepdims=True,
                )
                for row in range(block)
            ]
            read_ref[pl.ds(start, block), cut] = jnp.concatenate(found, axis=0)
        return carry

    lax.fori_loop(0, rows // block, some, 0)
    for head in range(heads):
        cut = slice(head * HEAD, (head + 1) * HEAD)
        read = decay_of(head, heads) * read_ref[:, cut] + own[head]
        centered = read - jnp.mean(read, axis=-1, keepdims=True)
        spread = jnp.mean(centered * centered, axis=-1, keepdims=True)
        normal = centered * lax.rsqrt(spread + epsilon)
        mixed_ref[:, cut] = (normal * gate[:, cut]).astype(bf16)


def read_state(parts, squares, cosine, sine, head_gain, ret_state, width_model):
    rows, heads = ret_state.shape[:2]
    width = heads * HEAD
    operands = [near(a) for a in (*squares, cosine, sine, head_gain, *parts, ret_state)]
    return pl.pallas_call(
        functools.partial(read_kernel, len(parts), heads, width_model),
        out_shape=[
            near_shape((rows, width), bf16),
            near_shape((rows, width), f32),
            near_shape((rows, width), f32),
        ],
        in_specs=[held()] * len(operands),
        out_specs=[held()] * 3,
        scratch_shapes=[pltpu.VMEM((rows, width), f32)] * 2,
        compiler_params=limit(4),
        cost_estimate=cost(2),
        name="read_state",
    )(*operands)


def update_kernel(heads, first, *refs):
    key_ref, value_ref, state_ref, next_ref = *refs[:3], refs[-1]
    block = next_ref.shape[0]
    start = pl.multiple_of((pl.program_id(0) + first) * block, block)
    mask = blocks_of(block)
    for head in range(heads):
        cut = slice(head * HEAD, (head + 1) * HEAD)
        values = value_ref[pl.ds(start, block), cut]
        table = jnp.concatenate([values] * block, axis=1) * mask
        table = jnp.concatenate([table] * 3, axis=0).astype(bf16)
        outer = columns_times(key_ref[pl.ds(start, block), cut], table)
        decay = decay_of(head, heads)
        for row in range(block):
            next_ref[row, head] = (
                decay * state_ref[start + row, head] + outer[:, row * HEAD : (row + 1) * HEAD]
            )


def update_state(key, value, ret_state, first, last, so_far, after):
    _, heads = ret_state.shape[:2]
    block = 8
    operands = [near(key), near(value), near(ret_state)] + [near(array) for array in after]
    specs = [held()] * len(operands)
    aliases = {}
    if so_far is not None:
        aliases = {len(operands): 0}
        operands.append(so_far)
        specs.append(pl.BlockSpec(memory_space=pl.ANY))
    return pl.pallas_call(
        functools.partial(update_kernel, heads, first),
        grid=(last - first,),
        out_shape=jax.ShapeDtypeStruct(ret_state.shape, f32),
        in_specs=specs,
        out_specs=pl.BlockSpec((block, heads, HEAD, HEAD), lambda i: (i + first, 0, 0, 0)),
        input_output_aliases=aliases,
        compiler_params=limit(6),
        cost_estimate=cost(2),
        name="update_state",
    )(*operands)


def out_kernel(count, peers, *refs):
    pieces = split_pieces(refs[:4], count // CORES)
    weight_ref, hidden_ref = refs[4:6]
    placing = refs[6 : 6 + peers]
    shares = refs[6 + peers : 6 + 2 * peers]
    after_ref = refs[6 + 2 * peers]
    outs = refs[7 + 2 * peers :]
    width = pieces[0].shape[1]
    places = spots(count, width)
    total = hidden_ref[...].astype(f32)
    for number in range(count):
        block = weight_ref[pl.ds(places[number], width), :]
        total = total + jnp.dot(pieces[number][...], block, preferred_element_type=f32)
    after = total.astype(bf16)
    after_ref[...] = after
    cut = after.shape[1]
    for peer in range(peers):
        sent = jnp.dot(placing[peer][...], after, preferred_element_type=f32)
        outs[peer][:, :cut] = sent.astype(bf16)
        outs[peer][:, cut:] = shares[peer][...]


def out_project(pieces, weight, hidden, placing, shares):
    rows, width = hidden.shape
    slots = placing[0].shape[0]
    peers = len(placing)
    operands = [near(array) for array in (*pieces, weight, hidden, *placing, *shares)]
    return pl.pallas_call(
        functools.partial(out_kernel, weight.shape[0] // pieces[0].shape[1], peers),
        out_shape=[near_shape((rows, width), bf16)]
        + [near_shape((slots, width + HEAD), bf16)] * peers,
        in_specs=[held()] * len(operands),
        out_specs=[held()] * (1 + peers),
        compiler_params=limit(8),
        cost_estimate=cost(2),
        name="out_project",
    )(*operands)


def lift_kernel(count, depth, *refs):
    pieces = split_pieces(refs[:4], count // CORES)
    gain_ref, gate_ref, up_ref, active_ref = refs[4:]
    width = pieces[0].shape[1]
    places = spots(count, width)
    squares = None
    for piece in pieces:
        values = piece[...].astype(f32)
        here = jnp.sum(values * values, axis=-1, keepdims=True)
        squares = here if squares is None else squares + here
    factor = lax.rsqrt(squares * (1.0 / depth) + epsilon)
    experts = gate_ref.shape[0]
    gates, ups = [None] * experts, [None] * experts
    for number in range(count):
        start = places[number]
        gain = gain_ref[:, pl.ds(start, width)]
        scaled = (pieces[number][...].astype(f32) * factor * gain).astype(bf16)
        for expert in range(experts):
            one = gate_ref[expert, pl.ds(start, width), :]
            two = up_ref[expert, pl.ds(start, width), :]
            gate = jnp.dot(scaled, one, preferred_element_type=f32)
            up = jnp.dot(scaled, two, preferred_element_type=f32)
            gates[expert] = gate if number == 0 else gates[expert] + gate
            ups[expert] = up if number == 0 else ups[expert] + up
    for expert in range(experts):
        gate = gates[expert]
        active_ref[expert] = (gate * jax.nn.sigmoid(gate) * ups[expert]).astype(bf16)


def lift(pieces, gain, expert_gate, expert_up):
    experts, depth, width = expert_gate.shape
    rows = pieces[0].shape[0]
    operands = [near(array) for array in (*pieces, gain, expert_gate, expert_up)]
    return pl.pallas_call(
        functools.partial(lift_kernel, depth // pieces[0].shape[1], depth),
        out_shape=near_shape((experts, rows, width), bf16),
        in_specs=[held()] * len(operands),
        out_specs=held(),
        compiler_params=limit(8),
        cost_estimate=cost(3),
        name="lift",
    )(*operands)


def lower_kernel(count, peers, slots, *refs):
    pieces = split_pieces(refs[:4], count // CORES)
    down_ref = refs[4]
    tables = refs[5 : 5 + peers]
    outs = refs[5 + peers : 5 + 2 * peers]
    mean_ref = refs[-1]
    experts, _, width = pieces[0].shape
    places = spots(count, width)
    totals = [None] * experts
    for number in range(count):
        start = places[number]
        for expert in range(experts):
            block = down_ref[expert, pl.ds(start, width), :]
            product = jnp.dot(pieces[number][expert], block, preferred_element_type=f32)
            totals[expert] = product if number == 0 else totals[expert] + product
    for expert in range(experts):
        mean_ref[expert] = totals[expert].astype(bf16).astype(f32)
    cut = tables[0].shape[1] - HEAD
    for peer in range(peers):
        table = tables[peer][:, cut:].astype(f32)
        sent = None
        for expert in range(experts):
            share = (
                table[:, expert : expert + 1]
                + table[:, experts + expert : experts + expert + 1]
                + table[:, 2 * experts + expert : 2 * experts + expert + 1]
            )
            here = mean_ref[expert, peer * slots : (peer + 1) * slots, :] * share
            sent = here if sent is None else sent + here
        outs[peer][...] = sent.astype(bf16)


def lower(pieces, expert_down, tables):
    experts, depth, width = expert_down.shape
    rows = pieces[0].shape[1]
    peers, slots = len(tables), tables[0].shape[0]
    operands = [near(array) for array in (*pieces, expert_down, *tables)]
    return pl.pallas_call(
        functools.partial(lower_kernel, depth // pieces[0].shape[2], peers, slots),
        out_shape=[near_shape((slots, width), bf16)] * peers,
        in_specs=[held()] * len(operands),
        out_specs=[held()] * peers,
        scratch_shapes=[pltpu.VMEM((experts, rows, width), f32)],
        compiler_params=limit(8),
        cost_estimate=cost(2),
        name="lower",
    )(*operands)


def finish_kernel(peers, *refs):
    after_ref = refs[0]
    placing = refs[1 : 1 + peers]
    back = refs[1 + peers : 1 + 2 * peers]
    updated_ref = refs[-1]
    total = after_ref[...].astype(f32)
    for peer in range(peers):
        total = total + lax.dot_general(
            placing[peer][...],
            back[peer][...],
            (((0,), (0,)), ((), ())),
            preferred_element_type=f32,
        )
    updated_ref[...] = total.astype(bf16)


def finish(after, placing, back):
    operands = [near(array) for array in (after, *placing, *back)]
    return pl.pallas_call(
        functools.partial(finish_kernel, len(placing)),
        out_shape=jax.ShapeDtypeStruct(after.shape, bf16),
        in_specs=[held()] * len(operands),
        out_specs=whole(after.shape),
        compiler_params=limit(4),
        cost_estimate=cost(1),
        name="finish",
    )(*operands)


def shared(lines):
    rest = jnp.concatenate(lines[1:], axis=-2)
    return [lines[0], rest, swap_cores(lines[0]), swap_cores(rest)]


def layer(
    hidden,
    positions,
    ret_state,
    query_weight,
    key_weight,
    value_weight,
    gate_weight,
    head_gain,
    out_weight,
    mix_gain,
    ffn_gain,
    expert_gate,
    expert_up,
    expert_down,
    route_ids,
    route_weight,
):
    own_rows, slice_width = hidden.shape
    peers = lax.axis_size("ep")
    ranks = lax.axis_size("tp")
    depth = slice_width * ranks
    slab, width = query_weight.shape

    local_experts = expert_gate.shape[0]
    group_size = local_experts * peers // GROUPS
    capacity = 2 * ((own_rows // GROUPS + group_size - 1) // group_size)
    slots = local_experts * capacity
    if local_experts % group_size == 0:
        slots = slots // TOP
    placing, shares = prepare(route_ids, route_weight, peers, local_experts, slots)

    inverse = 1.0 / rope_base ** (jnp.arange(0, HEAD, 2, dtype=f32) / HEAD)
    angle = positions.astype(f32)[:, None] * inverse[None, :]
    cosine, sine = jnp.cos(angle), jnp.sin(angle)
    cosine = jnp.concatenate([cosine, cosine], axis=1)
    sine = jnp.concatenate([-sine, sine], axis=1)

    if ranks == CORES * peers:
        sorted_pieces, squares = sort_pieces(along_z(hidden), (shares[0], cosine, sine))
        squares = [squares, swap_cores(squares)]
        half = jnp.concatenate(to_peers(sorted_pieces), axis=0)
        parts = [half, swap_cores(half)]
    else:
        me = lax.axis_index("ep")
        full_rows = lax.all_gather(hidden, "tp", axis=1, tiled=True)
        squares = jnp.sum(jnp.square(full_rows.astype(f32)), axis=1, keepdims=True)
        squares = [squares, jnp.zeros_like(squares)]
        columns = lax.all_to_all(full_rows, "ep", split_axis=1, concat_axis=0, tiled=True)
        columns = columns.reshape(peers, own_rows, slab)
        parts = [columns[me ^ jnp.arange(peers)].reshape(peers * own_rows, slab)]
    weights = (query_weight, key_weight, value_weight, gate_weight)
    partial = project(parts, mix_gain.reshape(1, depth), weights, peers, own_rows)
    sums = to_peers(partial)

    mixed, key, value = read_state(
        sums, squares, cosine, sine, head_gain.reshape(1, width), ret_state, depth
    )
    blocks = own_rows // 8
    split = max(1, 2 * blocks // 5)
    next_state = update_state(key, value, ret_state, 0, split, None, ())

    lines, next_state = lax.optimization_barrier((along_z(mixed), next_state))
    pieces = shared(lines)
    after, *packed = out_project(pieces, out_weight, hidden, placing, shares)

    next_state = update_state(key, value, ret_state, split, blocks, next_state, (after,))
    arrived = to_peers(packed)
    arrived, next_state = lax.optimization_barrier((arrived, next_state))
    rows = jnp.concatenate([table[:, :slice_width] for table in arrived], axis=0)
    pieces = shared(along_z(rows))
    active = lift(pieces, ffn_gain.reshape(1, depth), expert_gate, expert_up)

    pieces = shared(along_z(active))
    back = lower(pieces, expert_down, arrived)
    back = to_peers(back)
    return (finish(after, placing, back), next_state)


def solution(mesh):
    return jax.shard_map(
        layer,
        mesh=mesh,
        in_specs=(
            P("ep", "tp"),
            P("ep"),
            P("ep", "tp", None, None),
            P("ep", "tp"),
            P("ep", "tp"),
            P("ep", "tp"),
            P("ep", "tp"),
            P("tp"),
            P(None, "tp"),
            P(),
            P(),
            P("ep", None, "tp"),
            P("ep", None, "tp"),
            P("ep", None, "tp"),
            P("ep", None),
            P("ep", None),
        ),
        out_specs=(P("ep", "tp"), P("ep", "tp", None, None)),
        check_vma=False,
    )
```

```python
import functools

import jax
import jax.numpy as jnp
from jax import lax
from jax.experimental import pallas as pl
from jax.experimental.pallas import tpu as pltpu
from jax.sharding import PartitionSpec as P

HEADS = 16
HEAD = 128
GROUPS = 4
TOP = 2
CORES = 2


epsilon = 1e-06
rope_base = 10000.0
f32 = jnp.float32
bf16 = jnp.bfloat16


def swap_cores(array):
    size = lax.axis_size("tp")
    return lax.ppermute(array, "tp", [(i, i ^ 1) for i in range(size)])


def along_z(array):
    size = lax.axis_size("tp")
    found = [array]
    for k in range(1, size // CORES):
        found.append(lax.ppermute(array, "tp", [(i, i ^ (CORES * k)) for i in range(size)]))
    return found


def to_peers(arrays):
    size = lax.axis_size("ep")
    found = [arrays[0]]
    for k in range(1, size):
        found.append(lax.ppermute(arrays[k], "ep", [(i, i ^ k) for i in range(size)]))
    return found


def split_pieces(refs, levels):
    own, rest, other, others = refs
    rows = own.shape[-2]
    found = []
    for one, many in ((own, rest), (other, others)):
        found.append(one)
        found += [many.at[..., pl.ds(k * rows, rows), :] for k in range(levels - 1)]
    return found


def spots(count, width):
    level, core = lax.axis_index("tp") // CORES, lax.axis_index("tp") % CORES
    half = count // 2
    tables = [(level ^ k) * CORES + core for k in range(half)]
    tables += [(level ^ k) * CORES + (1 - core) for k in range(half)]
    return [pl.multiple_of(table * width, 128) for table in tables]


def near(array):
    return pltpu.with_memory_space_constraint(array, pltpu.VMEM)


def held():
    return pl.BlockSpec(memory_space=pltpu.VMEM)


def near_shape(shape, dtype):
    return pltpu.VMEM(shape, dtype)


def limit(mebibytes):
    return pltpu.CompilerParams(vmem_limit_bytes=mebibytes << 20)


def cost(microseconds):
    work = int(microseconds * 2.5e9)
    return pl.CostEstimate(flops=work, bytes_accessed=int(microseconds * 1.5e7), transcendentals=0)


def whole(shape):
    rank = len(shape)
    return pl.BlockSpec(shape, lambda *_: (0,) * rank)


def prepare_kernel(peers, experts, slots, ids_ref, share_ref, *outs):
    me = lax.axis_index("ep")
    rows = ids_ref.shape[1]
    ids = ids_ref[...]
    picks = [ids[number : number + 1, :] for number in range(TOP)]
    line = lax.broadcasted_iota(jnp.int32, (max(peers, 8), rows), 0)
    goes = None
    for pick in picks:
        hit = pick // experts == (line ^ me)
        goes = hit if goes is None else goes | hit
    row = lax.broadcasted_iota(jnp.int32, (rows, rows), 0)
    column = lax.broadcasted_iota(jnp.int32, (rows, rows), 1)
    before = (row < column).astype(f32).astype(bf16)
    counts = jnp.dot(goes.astype(f32).astype(bf16), before, preferred_element_type=f32)
    slot = jnp.where(goes, counts, -1.0)
    share = share_ref[...]
    line = lax.broadcasted_iota(jnp.int32, (HEAD, rows), 0)
    target = lax.broadcasted_iota(jnp.int32, (slots, rows), 0).astype(f32)
    for peer in range(peers):
        spot = (slot[peer : peer + 1, :] == target).astype(f32).astype(bf16)
        outs[peer][...] = spot
        table = jnp.zeros((HEAD, rows), f32)
        for expert in range(experts):
            number = (me ^ peer) * experts + expert
            weight = jnp.zeros((1, rows), f32)
            for pick in range(TOP):
                weight += jnp.where(picks[pick] == number, share[pick : pick + 1, :], 0.0)
            high = weight.astype(bf16).astype(f32)
            mid = (weight - high).astype(bf16).astype(f32)
            low = weight - high - mid
            table = jnp.where(line == expert, high, table)
            table = jnp.where(line == experts + expert, mid, table)
            table = jnp.where(line == 2 * experts + expert, low, table)
        moved = lax.dot_general(
            spot, table.astype(bf16), (((1,), (1,)), ((), ())), preferred_element_type=f32
        )
        outs[peers + peer][...] = moved.astype(bf16)


def prepare(route_ids, route_weight, peers, experts, slots):
    rows = route_ids.shape[0]
    outs = pl.pallas_call(
        functools.partial(prepare_kernel, peers, experts, slots),
        out_shape=[near_shape((slots, rows), bf16)] * peers
        + [near_shape((slots, HEAD), bf16)] * peers,
        in_specs=[held()] * 2,
        out_specs=[held()] * (2 * peers),
        compiler_params=limit(4),
        cost_estimate=cost(2),
        name="prepare",
    )(near(route_ids.T), near(route_weight.T))
    return outs[:peers], outs[peers:]


def load_kernel(array_ref, out_ref):
    out_ref[...] = array_ref[...]


def load(array):
    return pl.pallas_call(
        load_kernel,
        out_shape=near_shape(array.shape, array.dtype),
        in_specs=[whole(array.shape)],
        out_specs=held(),
        compiler_params=limit(2),
        cost_estimate=cost(1),
        name="load",
    )(array)


def join_kernel(own_ref, other_ref, joined_ref):
    width = own_ref.shape[1]
    joined_ref[:, :width] = own_ref[...]
    joined_ref[:, width:] = other_ref[...]


def join(own, other):
    rows, width = own.shape
    return pl.pallas_call(
        join_kernel,
        out_shape=near_shape((rows, 2 * width), own.dtype),
        in_specs=[held()] * 2,
        out_specs=held(),
        compiler_params=limit(2),
        cost_estimate=cost(1),
        name="join",
    )(near(own), near(other))


def turns_of(peers):
    return [(peers - 1 - turn, turn) for turn in range(peers // CORES)]


def project_kernel(peers, rows, gain_ref, *refs):
    weights, outs, total_ref = refs[-5 - peers : -1 - peers], refs[-1 - peers : -1], refs[-1]
    slab, width = weights[0].shape
    me, rank = lax.axis_index("ep"), lax.axis_index("tp")
    level, core = rank // CORES, rank % CORES
    base = me * slab
    direct = len(refs) > 6 + peers
    halves = CORES if direct else 1
    span = slab // halves
    totals, squares = [None] * 4, None
    for half in range(halves):
        if direct:
            one = refs[0][:, pl.ds(pl.multiple_of((core ^ half) * span, 128), span)]
            two = refs[1][:, pl.ds(pl.multiple_of((1 - (core ^ half)) * span, 128), span)]
            values = jnp.concatenate([one.astype(f32), two.astype(f32)], axis=0)
        else:
            values = refs[0][...].astype(f32)
        here = jnp.sum(values * values, axis=-1, keepdims=True)
        squares = here if half == 0 else squares + here
        gain = gain_ref[:, pl.ds(pl.multiple_of(base + half * span, 128), span)]
        scaled = (values * gain).astype(bf16)
        for which in range(4):
            block = weights[which][half * span : (half + 1) * span, :]
            product = jnp.dot(scaled, block, preferred_element_type=f32)
            totals[which] = product if half == 0 else totals[which] + product
    for which in range(4):
        total_ref[:, which * width : (which + 1) * width] = totals[which]
    high = squares.astype(bf16).astype(f32)
    mid = (squares - high).astype(bf16).astype(f32)
    lane = lax.broadcasted_iota(jnp.int32, (squares.shape[0], HEAD), 1)
    table = jnp.where(lane == 0, high, jnp.where(lane == 1, mid, 0.0))
    total_ref[:, 4 * width :] = jnp.where(lane == 2, squares - high - mid, table)
    for peer in range(peers):
        place = peer
        if direct:
            wanted = level ^ me ^ peer
            place = 0
            for turn, pair in enumerate(turns_of(peers)):
                for side in range(CORES):
                    spot = turn + (side ^ core) * (peers // CORES)
                    place = jnp.where(wanted == pair[side], spot, place)
        chosen = total_ref[pl.ds(pl.multiple_of(place * rows, 8), rows), :]
        outs[peer][...] = chosen.astype(outs[peer].dtype)


def project(parts, gain, weights, peers, rows):
    width = 4 * weights[0].shape[1] + HEAD
    out_shape = [near_shape((rows, width), f32)]
    out_shape += [near_shape((rows, width), bf16)] * (peers - 1)
    operands = [near(array) for array in (gain, *parts, *weights)]
    return pl.pallas_call(
        functools.partial(project_kernel, peers, rows),
        out_shape=out_shape,
        in_specs=[held()] * len(operands),
        out_specs=[held()] * peers,
        scratch_shapes=[pltpu.VMEM((peers * rows, width), f32)],
        compiler_params=limit(8),
        cost_estimate=cost(2),
        name="project",
    )(*operands)


def blocks_of(block):
    row = lax.broadcasted_iota(jnp.int32, (block, block * HEAD), 0)
    lane = lax.broadcasted_iota(jnp.int32, (block, block * HEAD), 1)
    return (lane // HEAD == row).astype(f32)


def columns_times(rows, table):
    high = rows.astype(bf16).astype(f32)
    mid = (rows - high).astype(bf16).astype(f32)
    split = jnp.concatenate([high, mid, rows - high - mid], axis=0).astype(bf16)
    return lax.dot_general(split, table, (((0,), (0,)), ((), ())), preferred_element_type=f32)


def decay_of(head, heads):
    number = (lax.axis_index("tp") * heads + head).astype(f32)
    power = jnp.full((1, HEAD), -5.0, f32) - number * (5.0 / (HEADS - 1))
    return 1.0 - jnp.exp2(power)


def read_kernel(peers, heads, width_model, *refs):
    cos_ref, sin_ref, gain_ref = refs[:3]
    parts = refs[3 : 3 + peers]
    state_ref = refs[3 + peers]
    mixed_ref, key_ref, value_ref = refs[4 + peers : 7 + peers]
    query_ref, read_ref = refs[7 + peers :]
    rows, width = mixed_ref.shape
    squares = parts[0][:, 4 * width :]
    for part in parts[1:]:
        squares = squares + part[:, 4 * width :].astype(f32)
    mean = jnp.sum(squares, axis=-1, keepdims=True) * (1.0 / width_model)
    factor = lax.rsqrt(mean + epsilon)

    def total(which):
        cut = slice(which * width, (which + 1) * width)
        summed = parts[0][:, cut]
        for part in parts[1:]:
            summed = summed + part[:, cut].astype(f32)
        return (summed * factor).astype(bf16).astype(f32)

    query, key, value = total(0), total(1), total(2)
    value_ref[...] = value
    gate = total(3)
    gate = gate * jax.nn.sigmoid(gate) * gain_ref[...]
    own = []
    for head in range(heads):
        cut = slice(head * HEAD, (head + 1) * HEAD)
        one, two = query[:, cut], key[:, cut]
        one = one * cos_ref[...] + pltpu.roll(one, HEAD // 2, 1) * sin_ref[...]
        two = two * cos_ref[...] + pltpu.roll(two, HEAD // 2, 1) * sin_ref[...]
        two = two * HEAD ** (-0.5)
        query_ref[:, cut] = one
        key_ref[:, cut] = two
        own.append(jnp.sum(one * two, axis=-1, keepdims=True) * value[:, cut])
    block = 8
    mask = blocks_of(block)
    ones = jnp.concatenate([mask] * 3, axis=0).astype(bf16)

    def some(number, carry):
        start = pl.multiple_of(number * block, block)
        for head in range(heads):
            cut = slice(head * HEAD, (head + 1) * HEAD)
            spread = columns_times(query_ref[pl.ds(start, block), cut], ones)
            found = [
                jnp.sum(
                    spread[:, row * HEAD : (row + 1) * HEAD] * state_ref[start + row, head],
                    axis=0,
                    keepdims=True,
                )
                for row in range(block)
            ]
            read_ref[pl.ds(start, block), cut] = jnp.concatenate(found, axis=0)
        return carry

    lax.fori_loop(0, rows // block, some, 0)
    for head in range(heads):
        cut = slice(head * HEAD, (head + 1) * HEAD)
        read = decay_of(head, heads) * read_ref[:, cut] + own[head]
        centered = read - jnp.mean(read, axis=-1, keepdims=True)
        spread = jnp.mean(centered * centered, axis=-1, keepdims=True)
        normal = centered * lax.rsqrt(spread + epsilon)
        mixed_ref[:, cut] = (normal * gate[:, cut]).astype(bf16)


def read_state(parts, cosine, sine, head_gain, ret_state, width_model):
    rows, heads = ret_state.shape[:2]
    width = heads * HEAD
    operands = [near(a) for a in (cosine, sine, head_gain, *parts, ret_state)]
    return pl.pallas_call(
        functools.partial(read_kernel, len(parts), heads, width_model),
        out_shape=[
            near_shape((rows, width), bf16),
            near_shape((rows, width), f32),
            near_shape((rows, width), f32),
        ],
        in_specs=[held()] * len(operands),
        out_specs=[held()] * 3,
        scratch_shapes=[pltpu.VMEM((rows, width), f32)] * 2,
        compiler_params=limit(4),
        cost_estimate=cost(2),
        name="read_state",
    )(*operands)


def update_kernel(heads, first, *refs):
    key_ref, value_ref, state_ref, next_ref = *refs[:3], refs[-1]
    block = next_ref.shape[0]
    start = pl.multiple_of((pl.program_id(0) + first) * block, block)
    mask = blocks_of(block)
    for head in range(heads):
        cut = slice(head * HEAD, (head + 1) * HEAD)
        values = value_ref[pl.ds(start, block), cut]
        table = jnp.concatenate([values] * block, axis=1) * mask
        table = jnp.concatenate([table] * 3, axis=0).astype(bf16)
        outer = columns_times(key_ref[pl.ds(start, block), cut], table)
        decay = decay_of(head, heads)
        for row in range(block):
            next_ref[row, head] = (
                decay * state_ref[start + row, head] + outer[:, row * HEAD : (row + 1) * HEAD]
            )


def update_state(key, value, ret_state, first, last, so_far, after):
    _, heads = ret_state.shape[:2]
    block = 8
    operands = [near(key), near(value), near(ret_state)] + [near(array) for array in after]
    specs = [held()] * len(operands)
    aliases = {}
    if so_far is not None:
        aliases = {len(operands): 0}
        operands.append(so_far)
        specs.append(pl.BlockSpec(memory_space=pl.ANY))
    return pl.pallas_call(
        functools.partial(update_kernel, heads, first),
        grid=(last - first,),
        out_shape=jax.ShapeDtypeStruct(ret_state.shape, f32),
        in_specs=specs,
        out_specs=pl.BlockSpec((block, heads, HEAD, HEAD), lambda i: (i + first, 0, 0, 0)),
        input_output_aliases=aliases,
        compiler_params=limit(6),
        cost_estimate=cost(2),
        name="update_state",
    )(*operands)


def out_kernel(count, peers, *refs):
    pieces = split_pieces(refs[:4], count // CORES)
    weight_ref, hidden_ref = refs[4:6]
    placing = refs[6 : 6 + peers]
    shares = refs[6 + peers : 6 + 2 * peers]
    after_ref = refs[6 + 2 * peers]
    outs = refs[7 + 2 * peers :]
    width = pieces[0].shape[1]
    places = spots(count, width)
    total = hidden_ref[...].astype(f32)
    for number in range(count):
        block = weight_ref[pl.ds(places[number], width), :]
        total = total + jnp.dot(pieces[number][...], block, preferred_element_type=f32)
    after = total.astype(bf16)
    after_ref[...] = after
    cut = after.shape[1]
    for peer in range(peers):
        sent = jnp.dot(placing[peer][...], after, preferred_element_type=f32)
        outs[peer][:, :cut] = sent.astype(bf16)
        outs[peer][:, cut:] = shares[peer][...]


def out_project(pieces, weight, hidden, placing, shares):
    rows, width = hidden.shape
    slots = placing[0].shape[0]
    peers = len(placing)
    operands = [near(array) for array in (*pieces, weight, hidden, *placing, *shares)]
    return pl.pallas_call(
        functools.partial(out_kernel, weight.shape[0] // pieces[0].shape[1], peers),
        out_shape=[near_shape((rows, width), bf16)]
        + [near_shape((slots, width + HEAD), bf16)] * peers,
        in_specs=[held()] * len(operands),
        out_specs=[held()] * (1 + peers),
        compiler_params=limit(8),
        cost_estimate=cost(2),
        name="out_project",
    )(*operands)


def lift_kernel(count, depth, *refs):
    pieces = split_pieces(refs[:4], count // CORES)
    gain_ref, gate_ref, up_ref, active_ref = refs[4:]
    width = pieces[0].shape[1]
    places = spots(count, width)
    squares = None
    for piece in pieces:
        values = piece[...].astype(f32)
        here = jnp.sum(values * values, axis=-1, keepdims=True)
        squares = here if squares is None else squares + here
    factor = lax.rsqrt(squares * (1.0 / depth) + epsilon)
    experts = gate_ref.shape[0]
    gates, ups = [None] * experts, [None] * experts
    for number in range(count):
        start = places[number]
        gain = gain_ref[:, pl.ds(start, width)]
        scaled = (pieces[number][...].astype(f32) * factor * gain).astype(bf16)
        for expert in range(experts):
            one = gate_ref[expert, pl.ds(start, width), :]
            two = up_ref[expert, pl.ds(start, width), :]
            gate = jnp.dot(scaled, one, preferred_element_type=f32)
            up = jnp.dot(scaled, two, preferred_element_type=f32)
            gates[expert] = gate if number == 0 else gates[expert] + gate
            ups[expert] = up if number == 0 else ups[expert] + up
    for expert in range(experts):
        gate = gates[expert]
        active_ref[expert] = (gate * jax.nn.sigmoid(gate) * ups[expert]).astype(bf16)


def lift(pieces, gain, expert_gate, expert_up):
    experts, depth, width = expert_gate.shape
    rows = pieces[0].shape[0]
    operands = [near(array) for array in (*pieces, gain, expert_gate, expert_up)]
    return pl.pallas_call(
        functools.partial(lift_kernel, depth // pieces[0].shape[1], depth),
        out_shape=near_shape((experts, rows, width), bf16),
        in_specs=[held()] * len(operands),
        out_specs=held(),
        compiler_params=limit(8),
        cost_estimate=cost(3),
        name="lift",
    )(*operands)


def lower_kernel(count, peers, slots, *refs):
    pieces = split_pieces(refs[:4], count // CORES)
    down_ref = refs[4]
    tables = refs[5 : 5 + peers]
    outs = refs[5 + peers : 5 + 2 * peers]
    mean_ref = refs[-1]
    experts, _, width = pieces[0].shape
    places = spots(count, width)
    totals = [None] * experts
    for number in range(count):
        start = places[number]
        for expert in range(experts):
            block = down_ref[expert, pl.ds(start, width), :]
            product = jnp.dot(pieces[number][expert], block, preferred_element_type=f32)
            totals[expert] = product if number == 0 else totals[expert] + product
    for expert in range(experts):
        mean_ref[expert] = totals[expert].astype(bf16).astype(f32)
    cut = tables[0].shape[1] - HEAD
    for peer in range(peers):
        table = tables[peer][:, cut:].astype(f32)
        sent = None
        for expert in range(experts):
            share = (
                table[:, expert : expert + 1]
                + table[:, experts + expert : experts + expert + 1]
                + table[:, 2 * experts + expert : 2 * experts + expert + 1]
            )
            here = mean_ref[expert, peer * slots : (peer + 1) * slots, :] * share
            sent = here if sent is None else sent + here
        outs[peer][...] = sent.astype(bf16)


def lower(pieces, expert_down, tables):
    experts, depth, width = expert_down.shape
    rows = pieces[0].shape[1]
    peers, slots = len(tables), tables[0].shape[0]
    operands = [near(array) for array in (*pieces, expert_down, *tables)]
    return pl.pallas_call(
        functools.partial(lower_kernel, depth // pieces[0].shape[2], peers, slots),
        out_shape=[near_shape((slots, width), bf16)] * peers,
        in_specs=[held()] * len(operands),
        out_specs=[held()] * peers,
        scratch_shapes=[pltpu.VMEM((experts, rows, width), f32)],
        compiler_params=limit(8),
        cost_estimate=cost(2),
        name="lower",
    )(*operands)


def finish_kernel(peers, *refs):
    after_ref = refs[0]
    placing = refs[1 : 1 + peers]
    back = refs[1 + peers : 1 + 2 * peers]
    updated_ref = refs[-1]
    total = after_ref[...].astype(f32)
    for peer in range(peers):
        total = total + lax.dot_general(
            placing[peer][...],
            back[peer][...],
            (((0,), (0,)), ((), ())),
            preferred_element_type=f32,
        )
    updated_ref[...] = total.astype(bf16)


def finish(after, placing, back):
    operands = [near(array) for array in (after, *placing, *back)]
    return pl.pallas_call(
        functools.partial(finish_kernel, len(placing)),
        out_shape=jax.ShapeDtypeStruct(after.shape, bf16),
        in_specs=[held()] * len(operands),
        out_specs=whole(after.shape),
        compiler_params=limit(4),
        cost_estimate=cost(1),
        name="finish",
    )(*operands)


def shared(lines):
    rest = jnp.concatenate(lines[1:], axis=-2)
    return [lines[0], rest, swap_cores(lines[0]), swap_cores(rest)]


def layer(
    hidden,
    positions,
    ret_state,
    query_weight,
    key_weight,
    value_weight,
    gate_weight,
    head_gain,
    out_weight,
    mix_gain,
    ffn_gain,
    expert_gate,
    expert_up,
    expert_down,
    route_ids,
    route_weight,
):
    own_rows, slice_width = hidden.shape
    peers = lax.axis_size("ep")
    ranks = lax.axis_size("tp")
    depth = slice_width * ranks
    slab, width = query_weight.shape

    local_experts = expert_gate.shape[0]
    group_size = local_experts * peers // GROUPS
    capacity = 2 * ((own_rows // GROUPS + group_size - 1) // group_size)
    slots = local_experts * capacity
    if local_experts % group_size == 0:
        slots = slots // TOP
    direct = ranks == CORES * peers
    if direct:
        joined = join(load(hidden), swap_cores(hidden))
        positions, route_ids, route_weight, joined = lax.optimization_barrier(
            (positions, route_ids, route_weight, joined)
        )
    placing, shares = prepare(route_ids, route_weight, peers, local_experts, slots)

    inverse = 1.0 / rope_base ** (jnp.arange(0, HEAD, 2, dtype=f32) / HEAD)
    angle = positions.astype(f32)[:, None] * inverse[None, :]
    cosine, sine = jnp.cos(angle), jnp.sin(angle)
    cosine = jnp.concatenate([cosine, cosine], axis=1)
    sine = jnp.concatenate([-sine, sine], axis=1)

    if direct:
        came = []
        for pair in turns_of(peers):
            route = [
                ((e * peers + z) * CORES + side, (z * peers + (e ^ pair[side])) * CORES + side)
                for e in range(peers)
                for z in range(peers)
                for side in range(CORES)
            ]
            came.append(lax.ppermute(joined, ("ep", "tp"), route))
        came, placing, shares, cosine, sine = lax.optimization_barrier(
            (came, placing, shares, cosine, sine)
        )
        came = jnp.concatenate(came, axis=0)
        parts = [came, swap_cores(came)]
    else:
        me = lax.axis_index("ep")
        full_rows = lax.all_gather(hidden, "tp", axis=1, tiled=True)
        columns = lax.all_to_all(full_rows, "ep", split_axis=1, concat_axis=0, tiled=True)
        columns = columns.reshape(peers, own_rows, slab)
        parts = [columns[me ^ jnp.arange(peers)].reshape(peers * own_rows, slab)]
    weights = (query_weight, key_weight, value_weight, gate_weight)
    partial = project(parts, mix_gain.reshape(1, depth), weights, peers, own_rows)
    sums = to_peers(partial)

    mixed, key, value = read_state(
        sums, cosine, sine, head_gain.reshape(1, width), ret_state, depth
    )
    blocks = own_rows // 8
    split = max(1, 2 * blocks // 5)
    next_state = update_state(key, value, ret_state, 0, split, None, ())

    lines, next_state = lax.optimization_barrier((along_z(mixed), next_state))
    pieces = shared(lines)
    after, *packed = out_project(pieces, out_weight, hidden, placing, shares)

    next_state = update_state(key, value, ret_state, split, blocks, next_state, (after,))
    arrived = to_peers(packed)
    arrived, next_state = lax.optimization_barrier((arrived, next_state))
    rows = jnp.concatenate([table[:, :slice_width] for table in arrived], axis=0)
    pieces = shared(along_z(rows))
    active = lift(pieces, ffn_gain.reshape(1, depth), expert_gate, expert_up)

    pieces = shared(along_z(active))
    back = lower(pieces, expert_down, arrived)
    back = to_peers(back)
    return (finish(after, placing, back), next_state)


def solution(mesh):
    return jax.shard_map(
        layer,
        mesh=mesh,
        in_specs=(
            P("ep", "tp"),
            P("ep"),
            P("ep", "tp", None, None),
            P("ep", "tp"),
            P("ep", "tp"),
            P("ep", "tp"),
            P("ep", "tp"),
            P("tp"),
            P(None, "tp"),
            P(),
            P(),
            P("ep", None, "tp"),
            P("ep", None, "tp"),
            P("ep", None, "tp"),
            P("ep", None),
            P("ep", None),
        ),
        out_specs=(P("ep", "tp"), P("ep", "tp", None, None)),
        check_vma=False,
    )
```

```python
import functools

import jax
import jax.numpy as jnp
from jax import lax
from jax.experimental import pallas as pl
from jax.experimental.pallas import tpu as pltpu
from jax.sharding import PartitionSpec as P

HEADS = 16
HEAD = 128
GROUPS = 4
TOP = 2
CORES = 2


epsilon = 1e-06
rope_base = 10000.0
f32 = jnp.float32
bf16 = jnp.bfloat16


def swap_cores(array):
    size = lax.axis_size("tp")
    return lax.ppermute(array, "tp", [(i, i ^ 1) for i in range(size)])


def along_z(array):
    size = lax.axis_size("tp")
    found = [array]
    for k in range(1, size // CORES):
        found.append(lax.ppermute(array, "tp", [(i, i ^ (CORES * k)) for i in range(size)]))
    return found


def to_peers(arrays):
    size = lax.axis_size("ep")
    found = [arrays[0]]
    for k in range(1, size):
        found.append(lax.ppermute(arrays[k], "ep", [(i, i ^ k) for i in range(size)]))
    return found


def split_pieces(refs, levels):
    own, rest, other, others = refs
    rows = own.shape[-2]
    found = []
    for one, many in ((own, rest), (other, others)):
        found.append(one)
        found += [many.at[..., pl.ds(k * rows, rows), :] for k in range(levels - 1)]
    return found


def spots(count, width):
    level, core = lax.axis_index("tp") // CORES, lax.axis_index("tp") % CORES
    half = count // 2
    tables = [(level ^ k) * CORES + core for k in range(half)]
    tables += [(level ^ k) * CORES + (1 - core) for k in range(half)]
    return [pl.multiple_of(table * width, 128) for table in tables]


def near(array):
    return pltpu.with_memory_space_constraint(array, pltpu.VMEM)


def held():
    return pl.BlockSpec(memory_space=pltpu.VMEM)


def near_shape(shape, dtype):
    return pltpu.VMEM(shape, dtype)


def limit(mebibytes):
    return pltpu.CompilerParams(vmem_limit_bytes=mebibytes << 20)


def cost(microseconds):
    work = int(microseconds * 2.5e9)
    return pl.CostEstimate(flops=work, bytes_accessed=int(microseconds * 1.5e7), transcendentals=0)


def whole(shape):
    rank = len(shape)
    return pl.BlockSpec(shape, lambda *_: (0,) * rank)


def prepare_kernel(peers, experts, slots, ids_ref, share_ref, *outs):
    me = lax.axis_index("ep")
    rows = ids_ref.shape[1]
    ids = ids_ref[...]
    picks = [ids[number : number + 1, :] for number in range(TOP)]
    line = lax.broadcasted_iota(jnp.int32, (max(peers, 8), rows), 0)
    goes = None
    for pick in picks:
        hit = pick // experts == (line ^ me)
        goes = hit if goes is None else goes | hit
    row = lax.broadcasted_iota(jnp.int32, (rows, rows), 0)
    column = lax.broadcasted_iota(jnp.int32, (rows, rows), 1)
    before = (row < column).astype(f32).astype(bf16)
    counts = jnp.dot(goes.astype(f32).astype(bf16), before, preferred_element_type=f32)
    slot = jnp.where(goes, counts, -1.0)
    share = share_ref[...]
    line = lax.broadcasted_iota(jnp.int32, (HEAD, rows), 0)
    target = lax.broadcasted_iota(jnp.int32, (slots, rows), 0).astype(f32)
    for peer in range(peers):
        spot = (slot[peer : peer + 1, :] == target).astype(f32).astype(bf16)
        outs[peer][...] = spot
        table = jnp.zeros((HEAD, rows), f32)
        for expert in range(experts):
            number = (me ^ peer) * experts + expert
            weight = jnp.zeros((1, rows), f32)
            for pick in range(TOP):
                weight += jnp.where(picks[pick] == number, share[pick : pick + 1, :], 0.0)
            high = weight.astype(bf16).astype(f32)
            mid = (weight - high).astype(bf16).astype(f32)
            low = weight - high - mid
            table = jnp.where(line == expert, high, table)
            table = jnp.where(line == experts + expert, mid, table)
            table = jnp.where(line == 2 * experts + expert, low, table)
        moved = lax.dot_general(
            spot, table.astype(bf16), (((1,), (1,)), ((), ())), preferred_element_type=f32
        )
        outs[peers + peer][...] = moved.astype(bf16)


def prepare(route_ids, route_weight, peers, experts, slots):
    rows = route_ids.shape[0]
    outs = pl.pallas_call(
        functools.partial(prepare_kernel, peers, experts, slots),
        out_shape=[near_shape((slots, rows), bf16)] * peers
        + [near_shape((slots, HEAD), bf16)] * peers,
        in_specs=[held()] * 2,
        out_specs=[held()] * (2 * peers),
        compiler_params=limit(4),
        cost_estimate=cost(2),
        name="prepare",
    )(near(route_ids.T), near(route_weight.T))
    return outs[:peers], outs[peers:]


def load_kernel(array_ref, out_ref):
    out_ref[...] = array_ref[...]


def load(array):
    return pl.pallas_call(
        load_kernel,
        out_shape=near_shape(array.shape, array.dtype),
        in_specs=[whole(array.shape)],
        out_specs=held(),
        compiler_params=limit(2),
        cost_estimate=cost(1),
        name="load",
    )(array)


def join_kernel(own_ref, other_ref, joined_ref):
    width = own_ref.shape[1]
    joined_ref[:, :width] = own_ref[...]
    joined_ref[:, width:] = other_ref[...]


def join(own, other):
    rows, width = own.shape
    return pl.pallas_call(
        join_kernel,
        out_shape=near_shape((rows, 2 * width), own.dtype),
        in_specs=[held()] * 2,
        out_specs=held(),
        compiler_params=limit(2),
        cost_estimate=cost(1),
        name="join",
    )(near(own), near(other))


def turns_of(peers):
    return [(peers - 1 - turn, turn) for turn in reversed(range(peers // CORES))]


def project_kernel(peers, rows, gain_ref, *refs):
    weights, outs, total_ref = refs[-5 - peers : -1 - peers], refs[-1 - peers : -1], refs[-1]
    slab, width = weights[0].shape
    me, rank = lax.axis_index("ep"), lax.axis_index("tp")
    level, core = rank // CORES, rank % CORES
    base = me * slab
    direct = len(refs) > 6 + peers
    halves = CORES if direct else 1
    span = slab // halves
    totals, squares = [None] * 4, None
    for half in range(halves):
        if direct:
            one = refs[0][:, pl.ds(pl.multiple_of((core ^ half) * span, 128), span)]
            two = refs[1][:, pl.ds(pl.multiple_of((1 - (core ^ half)) * span, 128), span)]
            values = jnp.concatenate([one.astype(f32), two.astype(f32)], axis=0)
        else:
            values = refs[0][...].astype(f32)
        here = jnp.sum(values * values, axis=-1, keepdims=True)
        squares = here if half == 0 else squares + here
        gain = gain_ref[:, pl.ds(pl.multiple_of(base + half * span, 128), span)]
        scaled = (values * gain).astype(bf16)
        for which in range(4):
            block = weights[which][half * span : (half + 1) * span, :]
            product = jnp.dot(scaled, block, preferred_element_type=f32)
            totals[which] = product if half == 0 else totals[which] + product
    for which in range(4):
        total_ref[:, which * width : (which + 1) * width] = totals[which]
    high = squares.astype(bf16).astype(f32)
    mid = (squares - high).astype(bf16).astype(f32)
    lane = lax.broadcasted_iota(jnp.int32, (squares.shape[0], HEAD), 1)
    table = jnp.where(lane == 0, high, jnp.where(lane == 1, mid, 0.0))
    total_ref[:, 4 * width :] = jnp.where(lane == 2, squares - high - mid, table)
    for peer in range(peers):
        place = peer
        if direct:
            wanted = level ^ me ^ peer
            place = 0
            for turn, pair in enumerate(turns_of(peers)):
                for side in range(CORES):
                    spot = turn + (side ^ core) * (peers // CORES)
                    place = jnp.where(wanted == pair[side], spot, place)
        chosen = total_ref[pl.ds(pl.multiple_of(place * rows, 8), rows), :]
        outs[peer][...] = chosen.astype(outs[peer].dtype)


def project(parts, gain, weights, peers, rows):
    width = 4 * weights[0].shape[1] + HEAD
    out_shape = [near_shape((rows, width), f32)]
    out_shape += [near_shape((rows, width), bf16)] * (peers - 1)
    operands = [near(array) for array in (gain, *parts, *weights)]
    return pl.pallas_call(
        functools.partial(project_kernel, peers, rows),
        out_shape=out_shape,
        in_specs=[held()] * len(operands),
        out_specs=[held()] * peers,
        scratch_shapes=[pltpu.VMEM((peers * rows, width), f32)],
        compiler_params=limit(8),
        cost_estimate=cost(2),
        name="project",
    )(*operands)


def blocks_of(block):
    row = lax.broadcasted_iota(jnp.int32, (block, block * HEAD), 0)
    lane = lax.broadcasted_iota(jnp.int32, (block, block * HEAD), 1)
    return (lane // HEAD == row).astype(f32)


def split_of(rows):
    high = rows.astype(bf16).astype(f32)
    mid = (rows - high).astype(bf16).astype(f32)
    return jnp.concatenate([high, mid, rows - high - mid], axis=0).astype(bf16)


def columns_times(rows, table):
    split = split_of(rows)
    return lax.dot_general(split, table, (((0,), (0,)), ((), ())), preferred_element_type=f32)


def decay_of(head, heads):
    number = (lax.axis_index("tp") * heads + head).astype(f32)
    power = jnp.full((1, HEAD), -5.0, f32) - number * (5.0 / (HEADS - 1))
    return 1.0 - jnp.exp2(power)


def read_kernel(peers, heads, width_model, *refs):
    cos_ref, sin_ref, gain_ref = refs[:3]
    parts = refs[3 : 3 + peers]
    state_ref = refs[3 + peers]
    mixed_ref, key_ref, value_ref = refs[4 + peers : 7 + peers]
    query_ref, read_ref = refs[7 + peers :]
    rows, width = mixed_ref.shape
    squares = parts[0][:, 4 * width :]
    for part in parts[1:]:
        squares = squares + part[:, 4 * width :].astype(f32)
    mean = jnp.sum(squares, axis=-1, keepdims=True) * (1.0 / width_model)
    factor = lax.rsqrt(mean + epsilon)

    def total(which):
        cut = slice(which * width, (which + 1) * width)
        summed = parts[0][:, cut]
        for part in parts[1:]:
            summed = summed + part[:, cut].astype(f32)
        return (summed * factor).astype(bf16).astype(f32)

    query, key, value = total(0), total(1), total(2)
    value_ref[...] = value
    gate = total(3)
    gate = gate * jax.nn.sigmoid(gate) * gain_ref[...]
    own = []
    for head in range(heads):
        cut = slice(head * HEAD, (head + 1) * HEAD)
        one, two = query[:, cut], key[:, cut]
        one = one * cos_ref[...] + pltpu.roll(one, HEAD // 2, 1) * sin_ref[...]
        two = two * cos_ref[...] + pltpu.roll(two, HEAD // 2, 1) * sin_ref[...]
        two = two * HEAD ** (-0.5)
        query_ref[:, cut] = one
        key_ref[:, cut] = two
        own.append(jnp.sum(one * two, axis=-1, keepdims=True) * value[:, cut])
    block = 8
    line = lax.broadcasted_iota(jnp.int32, (block, HEAD), 0)

    def some(number, carry):
        start = pl.multiple_of(number * block, block)
        for head in range(heads):
            cut = slice(head * HEAD, (head + 1) * HEAD)
            split = split_of(query_ref[pl.ds(start, block), cut])
            split = jnp.concatenate([split, split], axis=1)
            found = jnp.zeros((block, HEAD), f32)
            for row in range(block):
                state = state_ref[start + row, head]
                high = state.astype(bf16)
                low = (state - high.astype(f32)).astype(bf16)
                both = jnp.concatenate([high, low], axis=0)
                part = jnp.dot(split, both, preferred_element_type=f32)
                part = part[:block] + part[block : 2 * block] + part[2 * block :]
                found = jnp.where(line == row, part, found)
            read_ref[pl.ds(start, block), cut] = found
        return carry

    lax.fori_loop(0, rows // block, some, 0, unroll=True)
    for head in range(heads):
        cut = slice(head * HEAD, (head + 1) * HEAD)
        read = decay_of(head, heads) * read_ref[:, cut] + own[head]
        centered = read - jnp.mean(read, axis=-1, keepdims=True)
        spread = jnp.mean(centered * centered, axis=-1, keepdims=True)
        normal = centered * lax.rsqrt(spread + epsilon)
        mixed_ref[:, cut] = (normal * gate[:, cut]).astype(bf16)


def read_state(parts, cosine, sine, head_gain, ret_state, width_model):
    rows, heads = ret_state.shape[:2]
    width = heads * HEAD
    operands = [near(a) for a in (cosine, sine, head_gain, *parts, ret_state)]
    return pl.pallas_call(
        functools.partial(read_kernel, len(parts), heads, width_model),
        out_shape=[
            near_shape((rows, width), bf16),
            near_shape((rows, width), f32),
            near_shape((rows, width), f32),
        ],
        in_specs=[held()] * len(operands),
        out_specs=[held()] * 3,
        scratch_shapes=[pltpu.VMEM((rows, width), f32)] * 2,
        compiler_params=limit(4),
        cost_estimate=cost(2),
        name="read_state",
    )(*operands)


def update_kernel(heads, first, *refs):
    key_ref, value_ref, state_ref, next_ref = *refs[:3], refs[-1]
    block = next_ref.shape[0]
    start = pl.multiple_of((pl.program_id(0) + first) * block, block)
    mask = blocks_of(block)
    for head in range(heads):
        cut = slice(head * HEAD, (head + 1) * HEAD)
        values = value_ref[pl.ds(start, block), cut]
        table = jnp.concatenate([values] * block, axis=1) * mask
        table = jnp.concatenate([table] * 3, axis=0).astype(bf16)
        outer = columns_times(key_ref[pl.ds(start, block), cut], table)
        decay = decay_of(head, heads)
        for row in range(block):
            next_ref[row, head] = (
                decay * state_ref[start + row, head] + outer[:, row * HEAD : (row + 1) * HEAD]
            )


def update_state(key, value, ret_state, first, last, so_far, after):
    _, heads = ret_state.shape[:2]
    block = 8
    operands = [near(key), near(value), near(ret_state)] + [near(array) for array in after]
    specs = [held()] * len(operands)
    aliases = {}
    if so_far is not None:
        aliases = {len(operands): 0}
        operands.append(so_far)
        specs.append(pl.BlockSpec(memory_space=pl.ANY))
    return pl.pallas_call(
        functools.partial(update_kernel, heads, first),
        grid=(last - first,),
        out_shape=jax.ShapeDtypeStruct(ret_state.shape, f32),
        in_specs=specs,
        out_specs=pl.BlockSpec((block, heads, HEAD, HEAD), lambda i: (i + first, 0, 0, 0)),
        input_output_aliases=aliases,
        compiler_params=limit(6),
        cost_estimate=cost(2),
        name="update_state",
    )(*operands)


def out_kernel(count, peers, *refs):
    pieces = split_pieces(refs[:4], count // CORES)
    weight_ref, hidden_ref = refs[4:6]
    placing = refs[6 : 6 + peers]
    shares = refs[6 + peers : 6 + 2 * peers]
    after_ref = refs[6 + 2 * peers]
    outs = refs[7 + 2 * peers :]
    width = pieces[0].shape[1]
    places = spots(count, width)
    total = hidden_ref[...].astype(f32)
    for number in range(count):
        block = weight_ref[pl.ds(places[number], width), :]
        total = total + jnp.dot(pieces[number][...], block, preferred_element_type=f32)
    after = total.astype(bf16)
    after_ref[...] = after
    cut = after.shape[1]
    for peer in range(peers):
        sent = jnp.dot(placing[peer][...], after, preferred_element_type=f32)
        outs[peer][:, :cut] = sent.astype(bf16)
        outs[peer][:, cut:] = shares[peer][...]


def out_project(pieces, weight, hidden, placing, shares):
    rows, width = hidden.shape
    slots = placing[0].shape[0]
    peers = len(placing)
    operands = [near(array) for array in (*pieces, weight, hidden, *placing, *shares)]
    return pl.pallas_call(
        functools.partial(out_kernel, weight.shape[0] // pieces[0].shape[1], peers),
        out_shape=[near_shape((rows, width), bf16)]
        + [near_shape((slots, width + HEAD), bf16)] * peers,
        in_specs=[held()] * len(operands),
        out_specs=[held()] * (1 + peers),
        compiler_params=limit(8),
        cost_estimate=cost(2),
        name="out_project",
    )(*operands)


def lift_kernel(count, depth, *refs):
    pieces = split_pieces(refs[:4], count // CORES)
    gain_ref, gate_ref, up_ref, active_ref = refs[4:]
    width = pieces[0].shape[1]
    places = spots(count, width)
    squares = None
    for piece in pieces:
        values = piece[...].astype(f32)
        here = jnp.sum(values * values, axis=-1, keepdims=True)
        squares = here if squares is None else squares + here
    factor = lax.rsqrt(squares * (1.0 / depth) + epsilon)
    experts = gate_ref.shape[0]
    gates, ups = [None] * experts, [None] * experts
    for number in range(count):
        start = places[number]
        gain = gain_ref[:, pl.ds(start, width)]
        scaled = (pieces[number][...].astype(f32) * factor * gain).astype(bf16)
        for expert in range(experts):
            one = gate_ref[expert, pl.ds(start, width), :]
            two = up_ref[expert, pl.ds(start, width), :]
            gate = jnp.dot(scaled, one, preferred_element_type=f32)
            up = jnp.dot(scaled, two, preferred_element_type=f32)
            gates[expert] = gate if number == 0 else gates[expert] + gate
            ups[expert] = up if number == 0 else ups[expert] + up
    for expert in range(experts):
        gate = gates[expert]
        active_ref[expert] = (gate * jax.nn.sigmoid(gate) * ups[expert]).astype(bf16)


def lift(pieces, gain, expert_gate, expert_up):
    experts, depth, width = expert_gate.shape
    rows = pieces[0].shape[0]
    operands = [near(array) for array in (*pieces, gain, expert_gate, expert_up)]
    return pl.pallas_call(
        functools.partial(lift_kernel, depth // pieces[0].shape[1], depth),
        out_shape=near_shape((experts, rows, width), bf16),
        in_specs=[held()] * len(operands),
        out_specs=held(),
        compiler_params=limit(8),
        cost_estimate=cost(3),
        name="lift",
    )(*operands)


def lower_kernel(count, peers, slots, *refs):
    pieces = split_pieces(refs[:4], count // CORES)
    down_ref = refs[4]
    tables = refs[5 : 5 + peers]
    outs = refs[5 + peers : 5 + 2 * peers]
    mean_ref = refs[-1]
    experts, _, width = pieces[0].shape
    places = spots(count, width)
    totals = [None] * experts
    for number in range(count):
        start = places[number]
        for expert in range(experts):
            block = down_ref[expert, pl.ds(start, width), :]
            product = jnp.dot(pieces[number][expert], block, preferred_element_type=f32)
            totals[expert] = product if number == 0 else totals[expert] + product
    for expert in range(experts):
        mean_ref[expert] = totals[expert].astype(bf16).astype(f32)
    cut = tables[0].shape[1] - HEAD
    for peer in range(peers):
        table = tables[peer][:, cut:].astype(f32)
        sent = None
        for expert in range(experts):
            share = (
                table[:, expert : expert + 1]
                + table[:, experts + expert : experts + expert + 1]
                + table[:, 2 * experts + expert : 2 * experts + expert + 1]
            )
            here = mean_ref[expert, peer * slots : (peer + 1) * slots, :] * share
            sent = here if sent is None else sent + here
        outs[peer][...] = sent.astype(bf16)


def lower(pieces, expert_down, tables):
    experts, depth, width = expert_down.shape
    rows = pieces[0].shape[1]
    peers, slots = len(tables), tables[0].shape[0]
    operands = [near(array) for array in (*pieces, expert_down, *tables)]
    return pl.pallas_call(
        functools.partial(lower_kernel, depth // pieces[0].shape[2], peers, slots),
        out_shape=[near_shape((slots, width), bf16)] * peers,
        in_specs=[held()] * len(operands),
        out_specs=[held()] * peers,
        scratch_shapes=[pltpu.VMEM((experts, rows, width), f32)],
        compiler_params=limit(8),
        cost_estimate=cost(2),
        name="lower",
    )(*operands)


def finish_kernel(peers, *refs):
    after_ref = refs[0]
    placing = refs[1 : 1 + peers]
    back = refs[1 + peers : 1 + 2 * peers]
    updated_ref = refs[-1]
    total = after_ref[...].astype(f32)
    for peer in range(peers):
        total = total + lax.dot_general(
            placing[peer][...],
            back[peer][...],
            (((0,), (0,)), ((), ())),
            preferred_element_type=f32,
        )
    updated_ref[...] = total.astype(bf16)


def finish(after, placing, back):
    operands = [near(array) for array in (after, *placing, *back)]
    return pl.pallas_call(
        functools.partial(finish_kernel, len(placing)),
        out_shape=jax.ShapeDtypeStruct(after.shape, bf16),
        in_specs=[held()] * len(operands),
        out_specs=whole(after.shape),
        compiler_params=limit(4),
        cost_estimate=cost(1),
        name="finish",
    )(*operands)


def shared(lines):
    rest = jnp.concatenate(lines[1:], axis=-2)
    return [lines[0], rest, swap_cores(lines[0]), swap_cores(rest)]


def layer(
    hidden,
    positions,
    ret_state,
    query_weight,
    key_weight,
    value_weight,
    gate_weight,
    head_gain,
    out_weight,
    mix_gain,
    ffn_gain,
    expert_gate,
    expert_up,
    expert_down,
    route_ids,
    route_weight,
):
    own_rows, slice_width = hidden.shape
    peers = lax.axis_size("ep")
    ranks = lax.axis_size("tp")
    depth = slice_width * ranks
    slab, width = query_weight.shape

    local_experts = expert_gate.shape[0]
    group_size = local_experts * peers // GROUPS
    capacity = 2 * ((own_rows // GROUPS + group_size - 1) // group_size)
    slots = local_experts * capacity
    if local_experts % group_size == 0:
        slots = slots // TOP
    direct = ranks == CORES * peers
    if direct:
        joined = join(load(hidden), swap_cores(hidden))
        positions, route_ids, route_weight, joined = lax.optimization_barrier(
            (positions, route_ids, route_weight, joined)
        )
    placing, shares = prepare(route_ids, route_weight, peers, local_experts, slots)

    inverse = 1.0 / rope_base ** (jnp.arange(0, HEAD, 2, dtype=f32) / HEAD)
    angle = positions.astype(f32)[:, None] * inverse[None, :]
    cosine, sine = jnp.cos(angle), jnp.sin(angle)
    cosine = jnp.concatenate([cosine, cosine], axis=1)
    sine = jnp.concatenate([-sine, sine], axis=1)

    if direct:
        came = []
        for pair in turns_of(peers):
            route = [
                ((e * peers + z) * CORES + side, (z * peers + (e ^ pair[side])) * CORES + side)
                for e in range(peers)
                for z in range(peers)
                for side in range(CORES)
            ]
            came.append(lax.ppermute(joined, ("ep", "tp"), route))
        came, placing, shares, cosine, sine = lax.optimization_barrier(
            (came, placing, shares, cosine, sine)
        )
        came = jnp.concatenate(came, axis=0)
        parts = [came, swap_cores(came)]
    else:
        me = lax.axis_index("ep")
        full_rows = lax.all_gather(hidden, "tp", axis=1, tiled=True)
        columns = lax.all_to_all(full_rows, "ep", split_axis=1, concat_axis=0, tiled=True)
        columns = columns.reshape(peers, own_rows, slab)
        parts = [columns[me ^ jnp.arange(peers)].reshape(peers * own_rows, slab)]
    weights = (query_weight, key_weight, value_weight, gate_weight)
    partial = project(parts, mix_gain.reshape(1, depth), weights, peers, own_rows)
    sums = to_peers(partial)

    mixed, key, value = read_state(
        sums, cosine, sine, head_gain.reshape(1, width), ret_state, depth
    )
    blocks = own_rows // 8
    split = max(1, 2 * blocks // 5)
    next_state = update_state(key, value, ret_state, 0, split, None, ())

    lines, next_state = lax.optimization_barrier((along_z(mixed), next_state))
    pieces = shared(lines)
    after, *packed = out_project(pieces, out_weight, hidden, placing, shares)

    next_state = update_state(key, value, ret_state, split, blocks, next_state, (after,))
    arrived = to_peers(packed)
    arrived, next_state = lax.optimization_barrier((arrived, next_state))
    rows = jnp.concatenate([table[:, :slice_width] for table in arrived], axis=0)
    pieces = shared(along_z(rows))
    active = lift(pieces, ffn_gain.reshape(1, depth), expert_gate, expert_up)

    pieces = shared(along_z(active))
    back = lower(pieces, expert_down, arrived)
    back = to_peers(back)
    return (finish(after, placing, back), next_state)


def solution(mesh):
    return jax.shard_map(
        layer,
        mesh=mesh,
        in_specs=(
            P("ep", "tp"),
            P("ep"),
            P("ep", "tp", None, None),
            P("ep", "tp"),
            P("ep", "tp"),
            P("ep", "tp"),
            P("ep", "tp"),
            P("tp"),
            P(None, "tp"),
            P(),
            P(),
            P("ep", None, "tp"),
            P("ep", None, "tp"),
            P("ep", None, "tp"),
            P("ep", None),
            P("ep", None),
        ),
        out_specs=(P("ep", "tp"), P("ep", "tp", None, None)),
        check_vma=False,
    )
```

```python
import functools

import jax
import jax.numpy as jnp
from jax import lax
from jax.experimental import pallas as pl
from jax.experimental.pallas import tpu as pltpu
from jax.sharding import PartitionSpec as P

HEADS = 16
HEAD = 128
GROUPS = 4
TOP = 2
CORES = 2


epsilon = 1e-06
rope_base = 10000.0
f32 = jnp.float32
bf16 = jnp.bfloat16


def swap_cores(array):
    size = lax.axis_size("tp")
    return lax.ppermute(array, "tp", [(i, i ^ 1) for i in range(size)])


def along_z(array):
    size = lax.axis_size("tp")
    found = [array]
    for k in range(1, size // CORES):
        found.append(lax.ppermute(array, "tp", [(i, i ^ (CORES * k)) for i in range(size)]))
    return found


def to_peers(arrays):
    size = lax.axis_size("ep")
    found = [arrays[0]]
    for k in range(1, size):
        found.append(lax.ppermute(arrays[k], "ep", [(i, i ^ k) for i in range(size)]))
    return found


def pieces_of(one, many, levels):
    rows = one.shape[-2]
    return [one] + [many.at[..., pl.ds(k * rows, rows), :] for k in range(levels - 1)]


def call(kernel, outs, operands, microseconds, scratch=()):
    specs = [held()] * len(outs)
    return pl.pallas_call(
        kernel,
        out_shape=outs,
        in_specs=[held()] * len(operands),
        out_specs=specs,
        scratch_shapes=list(scratch),
        compiler_params=limit(6),
        cost_estimate=cost(microseconds),
    )(*[near(array) for array in operands])


def spots(count, width):
    level, core = lax.axis_index("tp") // CORES, lax.axis_index("tp") % CORES
    half = count // 2
    tables = [(level ^ k) * CORES + core for k in range(half)]
    tables += [(level ^ k) * CORES + (1 - core) for k in range(half)]
    return [pl.multiple_of(table * width, 128) for table in tables]


def near(array):
    return pltpu.with_memory_space_constraint(array, pltpu.VMEM)


def held():
    return pl.BlockSpec(memory_space=pltpu.VMEM)


def near_shape(shape, dtype):
    return pltpu.VMEM(shape, dtype)


def limit(mebibytes):
    return pltpu.CompilerParams(vmem_limit_bytes=mebibytes << 20)


def cost(microseconds):
    work = int(microseconds * 2.5e9)
    return pl.CostEstimate(flops=work, bytes_accessed=int(microseconds * 1.5e7), transcendentals=0)


def whole(shape):
    rank = len(shape)
    return pl.BlockSpec(shape, lambda *_: (0,) * rank)


def prepare_kernel(peers, experts, slots, ids_ref, share_ref, *outs):
    me = lax.axis_index("ep")
    rows = ids_ref.shape[1]
    ids = ids_ref[...]
    picks = [ids[number : number + 1, :] for number in range(TOP)]
    line = lax.broadcasted_iota(jnp.int32, (max(peers, 8), rows), 0)
    goes = None
    for pick in picks:
        hit = pick // experts == (line ^ me)
        goes = hit if goes is None else goes | hit
    row = lax.broadcasted_iota(jnp.int32, (rows, rows), 0)
    column = lax.broadcasted_iota(jnp.int32, (rows, rows), 1)
    before = (row < column).astype(f32).astype(bf16)
    counts = jnp.dot(goes.astype(f32).astype(bf16), before, preferred_element_type=f32)
    slot = jnp.where(goes, counts, -1.0)
    share = share_ref[...]
    line = lax.broadcasted_iota(jnp.int32, (HEAD, rows), 0)
    target = lax.broadcasted_iota(jnp.int32, (slots, rows), 0).astype(f32)
    for peer in range(peers):
        spot = (slot[peer : peer + 1, :] == target).astype(f32).astype(bf16)
        outs[peer][...] = spot
        table = jnp.zeros((HEAD, rows), f32)
        for expert in range(experts):
            number = (me ^ peer) * experts + expert
            weight = jnp.zeros((1, rows), f32)
            for pick in range(TOP):
                weight += jnp.where(picks[pick] == number, share[pick : pick + 1, :], 0.0)
            high = weight.astype(bf16).astype(f32)
            mid = (weight - high).astype(bf16).astype(f32)
            low = weight - high - mid
            table = jnp.where(line == expert, high, table)
            table = jnp.where(line == experts + expert, mid, table)
            table = jnp.where(line == 2 * experts + expert, low, table)
        moved = lax.dot_general(
            spot, table.astype(bf16), (((1,), (1,)), ((), ())), preferred_element_type=f32
        )
        outs[peers + peer][...] = moved.astype(bf16)


def prepare(route_ids, route_weight, peers, experts, slots):
    rows = route_ids.shape[0]
    outs = pl.pallas_call(
        functools.partial(prepare_kernel, peers, experts, slots),
        out_shape=[near_shape((slots, rows), bf16)] * peers
        + [near_shape((slots, HEAD), bf16)] * peers,
        in_specs=[held()] * 2,
        out_specs=[held()] * (2 * peers),
        compiler_params=limit(4),
        cost_estimate=cost(2),
        name="prepare",
    )(near(route_ids.T), near(route_weight.T))
    return outs[:peers], outs[peers:]


def load_kernel(array_ref, out_ref):
    out_ref[...] = array_ref[...]


def load(array):
    return pl.pallas_call(
        load_kernel,
        out_shape=near_shape(array.shape, array.dtype),
        in_specs=[whole(array.shape)],
        out_specs=held(),
        compiler_params=limit(2),
        cost_estimate=cost(1),
        name="load",
    )(array)


def join_kernel(own_ref, other_ref, joined_ref):
    width = own_ref.shape[1]
    joined_ref[:, :width] = own_ref[...]
    joined_ref[:, width:] = other_ref[...]


def join(own, other):
    rows, width = own.shape
    return pl.pallas_call(
        join_kernel,
        out_shape=near_shape((rows, 2 * width), own.dtype),
        in_specs=[held()] * 2,
        out_specs=held(),
        compiler_params=limit(2),
        cost_estimate=cost(1),
        name="join",
    )(near(own), near(other))


def turns_of(peers):
    return [(peers - 1 - turn, turn) for turn in reversed(range(peers // CORES))]


def project_kernel(peers, rows, gain_ref, *refs):
    weights, outs, total_ref = refs[-5 - peers : -1 - peers], refs[-1 - peers : -1], refs[-1]
    slab, width = weights[0].shape
    me, rank = lax.axis_index("ep"), lax.axis_index("tp")
    level, core = rank // CORES, rank % CORES
    base = me * slab
    direct = len(refs) > 6 + peers
    halves = CORES if direct else 1
    span = slab // halves
    totals, squares = [None] * 4, None
    for half in range(halves):
        if direct:
            one = refs[0][:, pl.ds(pl.multiple_of((core ^ half) * span, 128), span)]
            two = refs[1][:, pl.ds(pl.multiple_of((1 - (core ^ half)) * span, 128), span)]
            values = jnp.concatenate([one.astype(f32), two.astype(f32)], axis=0)
        else:
            values = refs[0][...].astype(f32)
        here = jnp.sum(values * values, axis=-1, keepdims=True)
        squares = here if half == 0 else squares + here
        gain = gain_ref[:, pl.ds(pl.multiple_of(base + half * span, 128), span)]
        scaled = (values * gain).astype(bf16)
        for which in range(4):
            block = weights[which][half * span : (half + 1) * span, :]
            product = jnp.dot(scaled, block, preferred_element_type=f32)
            totals[which] = product if half == 0 else totals[which] + product
    for which in range(4):
        total_ref[:, which * width : (which + 1) * width] = totals[which]
    high = squares.astype(bf16).astype(f32)
    mid = (squares - high).astype(bf16).astype(f32)
    lane = lax.broadcasted_iota(jnp.int32, (squares.shape[0], HEAD), 1)
    table = jnp.where(lane == 0, high, jnp.where(lane == 1, mid, 0.0))
    total_ref[:, 4 * width :] = jnp.where(lane == 2, squares - high - mid, table)
    for peer in range(peers):
        place = peer
        if direct:
            wanted = level ^ me ^ peer
            place = 0
            for turn, pair in enumerate(turns_of(peers)):
                for side in range(CORES):
                    spot = turn + (side ^ core) * (peers // CORES)
                    place = jnp.where(wanted == pair[side], spot, place)
        chosen = total_ref[pl.ds(pl.multiple_of(place * rows, 8), rows), :]
        outs[peer][...] = chosen.astype(outs[peer].dtype)


def project(parts, gain, weights, peers, rows):
    width = 4 * weights[0].shape[1] + HEAD
    out_shape = [near_shape((rows, width), f32)]
    out_shape += [near_shape((rows, width), bf16)] * (peers - 1)
    operands = [near(array) for array in (gain, *parts, *weights)]
    return pl.pallas_call(
        functools.partial(project_kernel, peers, rows),
        out_shape=out_shape,
        in_specs=[held()] * len(operands),
        out_specs=[held()] * peers,
        scratch_shapes=[pltpu.VMEM((peers * rows, width), f32)],
        compiler_params=limit(8),
        cost_estimate=cost(2),
        name="project",
    )(*operands)


def blocks_of(block):
    row = lax.broadcasted_iota(jnp.int32, (block, block * HEAD), 0)
    lane = lax.broadcasted_iota(jnp.int32, (block, block * HEAD), 1)
    return (lane // HEAD == row).astype(f32)


def split_of(rows):
    high = rows.astype(bf16).astype(f32)
    mid = (rows - high).astype(bf16).astype(f32)
    return jnp.concatenate([high, mid, rows - high - mid], axis=0).astype(bf16)


def columns_times(rows, table):
    split = split_of(rows)
    return lax.dot_general(split, table, (((0,), (0,)), ((), ())), preferred_element_type=f32)


def decay_of(head, heads):
    number = (lax.axis_index("tp") * heads + head).astype(f32)
    power = jnp.full((1, HEAD), -5.0, f32) - number * (5.0 / (HEADS - 1))
    return 1.0 - jnp.exp2(power)


def read_kernel(peers, heads, width_model, *refs):
    cos_ref, sin_ref, gain_ref = refs[:3]
    parts = refs[3 : 3 + peers]
    state_ref = refs[3 + peers]
    mixed_ref, key_ref, value_ref = refs[4 + peers : 7 + peers]
    query_ref, read_ref = refs[7 + peers :]
    rows, width = mixed_ref.shape
    squares = parts[0][:, 4 * width :]
    for part in parts[1:]:
        squares = squares + part[:, 4 * width :].astype(f32)
    mean = jnp.sum(squares, axis=-1, keepdims=True) * (1.0 / width_model)
    factor = lax.rsqrt(mean + epsilon)

    def total(which):
        cut = slice(which * width, (which + 1) * width)
        summed = parts[0][:, cut]
        for part in parts[1:]:
            summed = summed + part[:, cut].astype(f32)
        return (summed * factor).astype(bf16).astype(f32)

    query, key, value = total(0), total(1), total(2)
    value_ref[...] = value
    gate = total(3)
    gate = gate * jax.nn.sigmoid(gate) * gain_ref[...]
    own = []
    for head in range(heads):
        cut = slice(head * HEAD, (head + 1) * HEAD)
        one, two = query[:, cut], key[:, cut]
        one = one * cos_ref[...] + pltpu.roll(one, HEAD // 2, 1) * sin_ref[...]
        two = two * cos_ref[...] + pltpu.roll(two, HEAD // 2, 1) * sin_ref[...]
        two = two * HEAD ** (-0.5)
        query_ref[:, cut] = one
        key_ref[:, cut] = two
        own.append(jnp.sum(one * two, axis=-1, keepdims=True) * value[:, cut])
    block = 8
    line = lax.broadcasted_iota(jnp.int32, (block, HEAD), 0)

    def some(number, carry):
        start = pl.multiple_of(number * block, block)
        for head in range(heads):
            cut = slice(head * HEAD, (head + 1) * HEAD)
            split = split_of(query_ref[pl.ds(start, block), cut])
            split = jnp.concatenate([split, split], axis=1)
            found = jnp.zeros((block, HEAD), f32)
            for row in range(block):
                state = state_ref[start + row, head]
                high = state.astype(bf16)
                low = (state - high.astype(f32)).astype(bf16)
                both = jnp.concatenate([high, low], axis=0)
                part = jnp.dot(split, both, preferred_element_type=f32)
                part = part[:block] + part[block : 2 * block] + part[2 * block :]
                found = jnp.where(line == row, part, found)
            read_ref[pl.ds(start, block), cut] = found
        return carry

    lax.fori_loop(0, rows // block, some, 0, unroll=True)
    for head in range(heads):
        cut = slice(head * HEAD, (head + 1) * HEAD)
        read = decay_of(head, heads) * read_ref[:, cut] + own[head]
        centered = read - jnp.mean(read, axis=-1, keepdims=True)
        spread = jnp.mean(centered * centered, axis=-1, keepdims=True)
        normal = centered * lax.rsqrt(spread + epsilon)
        mixed_ref[:, cut] = (normal * gate[:, cut]).astype(bf16)


def read_state(parts, cosine, sine, head_gain, ret_state, width_model):
    rows, heads = ret_state.shape[:2]
    width = heads * HEAD
    operands = [near(a) for a in (cosine, sine, head_gain, *parts, ret_state)]
    return pl.pallas_call(
        functools.partial(read_kernel, len(parts), heads, width_model),
        out_shape=[
            near_shape((rows, width), bf16),
            near_shape((rows, width), f32),
            near_shape((rows, width), f32),
        ],
        in_specs=[held()] * len(operands),
        out_specs=[held()] * 3,
        scratch_shapes=[pltpu.VMEM((rows, width), f32)] * 2,
        compiler_params=limit(4),
        cost_estimate=cost(2),
        name="read_state",
    )(*operands)


def update_kernel(heads, first, *refs):
    key_ref, value_ref, state_ref, next_ref = *refs[:3], refs[-1]
    block = next_ref.shape[0]
    start = pl.multiple_of((pl.program_id(0) + first) * block, block)
    mask = blocks_of(block)
    for head in range(heads):
        cut = slice(head * HEAD, (head + 1) * HEAD)
        values = value_ref[pl.ds(start, block), cut]
        table = jnp.concatenate([values] * block, axis=1) * mask
        table = jnp.concatenate([table] * 3, axis=0).astype(bf16)
        outer = columns_times(key_ref[pl.ds(start, block), cut], table)
        decay = decay_of(head, heads)
        for row in range(block):
            next_ref[row, head] = (
                decay * state_ref[start + row, head] + outer[:, row * HEAD : (row + 1) * HEAD]
            )


def update_state(key, value, ret_state, first, last, so_far, after):
    _, heads = ret_state.shape[:2]
    block = 8
    operands = [near(key), near(value), near(ret_state)] + [near(array) for array in after]
    specs = [held()] * len(operands)
    aliases = {}
    if so_far is not None:
        aliases = {len(operands): 0}
        operands.append(so_far)
        specs.append(pl.BlockSpec(memory_space=pl.ANY))
    return pl.pallas_call(
        functools.partial(update_kernel, heads, first),
        grid=(last - first,),
        out_shape=jax.ShapeDtypeStruct(ret_state.shape, f32),
        in_specs=specs,
        out_specs=pl.BlockSpec((block, heads, HEAD, HEAD), lambda i: (i + first, 0, 0, 0)),
        input_output_aliases=aliases,
        compiler_params=limit(6),
        cost_estimate=cost(2),
        name="update_state",
    )(*operands)


def out_sum(pieces, places, weight_ref, total):
    width = pieces[0].shape[1]
    for piece, place in zip(pieces, places):
        block = weight_ref[pl.ds(place, width), :]
        total = total + jnp.dot(piece[...], block, preferred_element_type=f32)
    return total


def out_first(levels, own, rest, weight_ref, hidden_ref, total_ref):
    places = spots(CORES * levels, own.shape[1])[:levels]
    total = hidden_ref[...].astype(f32)
    total_ref[...] = out_sum(pieces_of(own, rest, levels), places, weight_ref, total)


def out_last(levels, peers, other, others, weight_ref, total_ref, *refs):
    placing, shares = refs[:peers], refs[peers : 2 * peers]
    after_ref, outs = refs[2 * peers], refs[2 * peers + 1 :]
    places = spots(CORES * levels, other.shape[1])[levels:]
    pieces = pieces_of(other, others, levels)
    after = out_sum(pieces, places, weight_ref, total_ref[...]).astype(bf16)
    after_ref[...] = after
    cut = after.shape[1]
    for peer in range(peers):
        sent = jnp.dot(placing[peer][...], after, preferred_element_type=f32)
        outs[peer][:, :cut] = sent.astype(bf16)
        outs[peer][:, cut:] = shares[peer][...]


def out_project(pieces, weight, hidden, placing, shares):
    own, rest, other, others = pieces
    rows, width = hidden.shape
    slots, peers = placing[0].shape[0], len(placing)
    levels = 1 + rest.shape[0] // rows
    (total,) = call(
        functools.partial(out_first, levels),
        [near_shape((rows, width), f32)],
        (own, rest, weight, hidden),
        1,
    )
    return call(
        functools.partial(out_last, levels, peers),
        [near_shape((rows, width), bf16)] + [near_shape((slots, width + HEAD), bf16)] * peers,
        (other, others, weight, total, *placing, *shares),
        2,
    )


def lift_sum(pieces, places, gain_ref, gate_ref, up_ref, squares, gates, ups):
    width = pieces[0].shape[1]
    for piece, place in zip(pieces, places):
        values = piece[...].astype(f32)
        squares = squares + jnp.sum(values * values, axis=-1, keepdims=True)
        scaled = (values * gain_ref[:, pl.ds(place, width)]).astype(bf16)
        for expert in range(gate_ref.shape[0]):
            one = gate_ref[expert, pl.ds(place, width), :]
            two = up_ref[expert, pl.ds(place, width), :]
            gates[expert] = gates[expert] + jnp.dot(scaled, one, preferred_element_type=f32)
            ups[expert] = ups[expert] + jnp.dot(scaled, two, preferred_element_type=f32)
    return squares, gates, ups


def lift_first(levels, own, rest, gain_ref, gate_ref, up_ref, gates_ref, ups_ref, squares_ref):
    experts, rows, width = gates_ref.shape
    places = spots(CORES * levels, own.shape[1])[:levels]
    zeros = [jnp.zeros((rows, width), f32)] * experts
    squares, gates, ups = lift_sum(
        pieces_of(own, rest, levels),
        places,
        gain_ref,
        gate_ref,
        up_ref,
        jnp.zeros((rows, 1), f32),
        list(zeros),
        list(zeros),
    )
    squares_ref[...] = jnp.broadcast_to(squares, squares_ref.shape)
    for expert in range(experts):
        gates_ref[expert] = gates[expert]
        ups_ref[expert] = ups[expert]


def lift_last(
    levels, depth, other, others, gain_ref, gate_ref, up_ref, gates_ref, ups_ref, squares_ref, active_ref
):
    experts = gates_ref.shape[0]
    places = spots(CORES * levels, other.shape[1])[levels:]
    squares, gates, ups = lift_sum(
        pieces_of(other, others, levels),
        places,
        gain_ref,
        gate_ref,
        up_ref,
        squares_ref[:, :1],
        [gates_ref[expert] for expert in range(experts)],
        [ups_ref[expert] for expert in range(experts)],
    )
    factor = lax.rsqrt(squares * (1.0 / depth) + epsilon)
    for expert in range(experts):
        gate = gates[expert] * factor
        active_ref[expert] = (gate * jax.nn.sigmoid(gate) * (ups[expert] * factor)).astype(bf16)


def lift(pieces, gain, expert_gate, expert_up):
    own, rest, other, others = pieces
    experts, depth, width = expert_gate.shape
    rows = own.shape[0]
    levels = 1 + rest.shape[0] // rows
    sums = call(
        functools.partial(lift_first, levels),
        [near_shape((experts, rows, width), f32)] * 2 + [near_shape((rows, HEAD), f32)],
        (own, rest, gain, expert_gate, expert_up),
        2,
    )
    (active,) = call(
        functools.partial(lift_last, levels, depth),
        [near_shape((experts, rows, width), bf16)],
        (other, others, gain, expert_gate, expert_up, *sums),
        2,
    )
    return active


def lower_sum(pieces, places, down_ref, totals):
    width = pieces[0].shape[-1]
    for piece, place in zip(pieces, places):
        for expert in range(down_ref.shape[0]):
            block = down_ref[expert, pl.ds(place, width), :]
            product = jnp.dot(piece[expert], block, preferred_element_type=f32)
            totals[expert] = product if totals[expert] is None else totals[expert] + product
    return totals


def lower_first(levels, own, rest, down_ref, totals_ref):
    experts = down_ref.shape[0]
    places = spots(CORES * levels, own.shape[2])[:levels]
    totals = lower_sum(pieces_of(own, rest, levels), places, down_ref, [None] * experts)
    for expert in range(experts):
        totals_ref[expert] = totals[expert]


def lower_last(levels, peers, other, others, down_ref, totals_ref, *refs):
    tables, outs, mean_ref = refs[:peers], refs[peers : 2 * peers], refs[-1]
    experts, _ = totals_ref.shape[:2]
    slots = tables[0].shape[0]
    places = spots(CORES * levels, other.shape[2])[levels:]
    totals = [totals_ref[expert] for expert in range(experts)]
    totals = lower_sum(pieces_of(other, others, levels), places, down_ref, totals)
    for expert in range(experts):
        mean_ref[expert] = totals[expert].astype(bf16).astype(f32)
    cut = tables[0].shape[1] - HEAD
    for peer in range(peers):
        table = tables[peer][:, cut:].astype(f32)
        sent = None
        for expert in range(experts):
            share = (
                table[:, expert : expert + 1]
                + table[:, experts + expert : experts + expert + 1]
                + table[:, 2 * experts + expert : 2 * experts + expert + 1]
            )
            here = mean_ref[expert, peer * slots : (peer + 1) * slots, :] * share
            sent = here if sent is None else sent + here
        outs[peer][...] = sent.astype(bf16)


def lower(pieces, expert_down, tables):
    own, rest, other, others = pieces
    experts, _, width = expert_down.shape
    rows = own.shape[1]
    levels = 1 + rest.shape[1] // rows
    peers, slots = len(tables), tables[0].shape[0]
    (totals,) = call(
        functools.partial(lower_first, levels),
        [near_shape((experts, rows, width), f32)],
        (own, rest, expert_down),
        1,
    )
    return call(
        functools.partial(lower_last, levels, peers),
        [near_shape((slots, width), bf16)] * peers,
        (other, others, expert_down, totals, *tables),
        2,
        [pltpu.VMEM((experts, rows, width), f32)],
    )


def finish_kernel(peers, *refs):
    after_ref = refs[0]
    placing = refs[1 : 1 + peers]
    back = refs[1 + peers : 1 + 2 * peers]
    updated_ref = refs[-1]
    total = after_ref[...].astype(f32)
    for peer in range(peers):
        total = total + lax.dot_general(
            placing[peer][...],
            back[peer][...],
            (((0,), (0,)), ((), ())),
            preferred_element_type=f32,
        )
    updated_ref[...] = total.astype(bf16)


def finish(after, placing, back):
    operands = [near(array) for array in (after, *placing, *back)]
    return pl.pallas_call(
        functools.partial(finish_kernel, len(placing)),
        out_shape=jax.ShapeDtypeStruct(after.shape, bf16),
        in_specs=[held()] * len(operands),
        out_specs=whole(after.shape),
        compiler_params=limit(4),
        cost_estimate=cost(1),
        name="finish",
    )(*operands)


def shared(lines):
    rest = jnp.concatenate(lines[1:], axis=-2)
    return [lines[0], rest, swap_cores(lines[0]), swap_cores(rest)]


def layer(
    hidden,
    positions,
    ret_state,
    query_weight,
    key_weight,
    value_weight,
    gate_weight,
    head_gain,
    out_weight,
    mix_gain,
    ffn_gain,
    expert_gate,
    expert_up,
    expert_down,
    route_ids,
    route_weight,
):
    own_rows, slice_width = hidden.shape
    peers = lax.axis_size("ep")
    ranks = lax.axis_size("tp")
    depth = slice_width * ranks
    slab, width = query_weight.shape

    local_experts = expert_gate.shape[0]
    group_size = local_experts * peers // GROUPS
    capacity = 2 * ((own_rows // GROUPS + group_size - 1) // group_size)
    slots = local_experts * capacity
    if local_experts % group_size == 0:
        slots = slots // TOP
    direct = ranks == CORES * peers
    if direct:
        joined = join(load(hidden), swap_cores(hidden))
        positions, route_ids, route_weight, joined = lax.optimization_barrier(
            (positions, route_ids, route_weight, joined)
        )
    placing, shares = prepare(route_ids, route_weight, peers, local_experts, slots)

    inverse = 1.0 / rope_base ** (jnp.arange(0, HEAD, 2, dtype=f32) / HEAD)
    angle = positions.astype(f32)[:, None] * inverse[None, :]
    cosine, sine = jnp.cos(angle), jnp.sin(angle)
    cosine = jnp.concatenate([cosine, cosine], axis=1)
    sine = jnp.concatenate([-sine, sine], axis=1)

    if direct:
        came = []
        for pair in turns_of(peers):
            route = [
                ((e * peers + z) * CORES + side, (z * peers + (e ^ pair[side])) * CORES + side)
                for e in range(peers)
                for z in range(peers)
                for side in range(CORES)
            ]
            came.append(lax.ppermute(joined, ("ep", "tp"), route))
        came, placing, shares, cosine, sine = lax.optimization_barrier(
            (came, placing, shares, cosine, sine)
        )
        came = jnp.concatenate(came, axis=0)
        parts = [came, swap_cores(came)]
    else:
        me = lax.axis_index("ep")
        full_rows = lax.all_gather(hidden, "tp", axis=1, tiled=True)
        columns = lax.all_to_all(full_rows, "ep", split_axis=1, concat_axis=0, tiled=True)
        columns = columns.reshape(peers, own_rows, slab)
        parts = [columns[me ^ jnp.arange(peers)].reshape(peers * own_rows, slab)]
    weights = (query_weight, key_weight, value_weight, gate_weight)
    partial = project(parts, mix_gain.reshape(1, depth), weights, peers, own_rows)
    sums = to_peers(partial)

    mixed, key, value = read_state(
        sums, cosine, sine, head_gain.reshape(1, width), ret_state, depth
    )
    blocks = own_rows // 8
    split = max(1, 2 * blocks // 5)
    next_state = update_state(key, value, ret_state, 0, split, None, ())

    lines, next_state = lax.optimization_barrier((along_z(mixed), next_state))
    pieces = shared(lines)
    after, *packed = out_project(pieces, out_weight, hidden, placing, shares)

    next_state = update_state(key, value, ret_state, split, blocks, next_state, (after,))
    arrived = to_peers(packed)
    arrived, next_state = lax.optimization_barrier((arrived, next_state))
    rows = jnp.concatenate([table[:, :slice_width] for table in arrived], axis=0)
    pieces = shared(along_z(rows))
    active = lift(pieces, ffn_gain.reshape(1, depth), expert_gate, expert_up)

    pieces = shared(along_z(active))
    back = lower(pieces, expert_down, arrived)
    back = to_peers(back)
    return (finish(after, placing, back), next_state)


def solution(mesh):
    return jax.shard_map(
        layer,
        mesh=mesh,
        in_specs=(
            P("ep", "tp"),
            P("ep"),
            P("ep", "tp", None, None),
            P("ep", "tp"),
            P("ep", "tp"),
            P("ep", "tp"),
            P("ep", "tp"),
            P("tp"),
            P(None, "tp"),
            P(),
            P(),
            P("ep", None, "tp"),
            P("ep", None, "tp"),
            P("ep", None, "tp"),
            P("ep", None),
            P("ep", None),
        ),
        out_specs=(P("ep", "tp"), P("ep", "tp", None, None)),
        check_vma=False,
    )
```

```python
import functools

import jax
import jax.numpy as jnp
from jax import lax
from jax.experimental import pallas as pl
from jax.experimental.pallas import tpu as pltpu
from jax.sharding import PartitionSpec as P

HEADS = 16
HEAD = 128
GROUPS = 4
TOP = 2
CORES = 2


epsilon = 1e-06
rope_base = 10000.0
f32 = jnp.float32
bf16 = jnp.bfloat16


def swap_cores(array):
    size = lax.axis_size("tp")
    return lax.ppermute(array, "tp", [(i, i ^ 1) for i in range(size)])


def along_z(array):
    size = lax.axis_size("tp")
    found = [array]
    for k in range(1, size // CORES):
        found.append(lax.ppermute(array, "tp", [(i, i ^ (CORES * k)) for i in range(size)]))
    return found


def to_peers(arrays):
    size = lax.axis_size("ep")
    found = [arrays[0]]
    for k in range(1, size):
        found.append(lax.ppermute(arrays[k], "ep", [(i, i ^ k) for i in range(size)]))
    return found


def parts_of(many, levels):
    rows = many.shape[-2] // (levels - 1)
    return [many.at[..., pl.ds(k * rows, rows), :] for k in range(levels - 1)]


def call(kernel, outs, operands, microseconds, scratch=()):
    specs = [held()] * len(outs)
    return pl.pallas_call(
        kernel,
        out_shape=outs,
        in_specs=[held()] * len(operands),
        out_specs=specs,
        scratch_shapes=list(scratch),
        compiler_params=limit(6),
        cost_estimate=cost(microseconds),
    )(*[near(array) for array in operands])


def spots(count, width):
    level, core = lax.axis_index("tp") // CORES, lax.axis_index("tp") % CORES
    half = count // 2
    tables = [(level ^ k) * CORES + core for k in range(half)]
    tables += [(level ^ k) * CORES + (1 - core) for k in range(half)]
    return [pl.multiple_of(table * width, 128) for table in tables]


def near(array):
    return pltpu.with_memory_space_constraint(array, pltpu.VMEM)


def held():
    return pl.BlockSpec(memory_space=pltpu.VMEM)


def near_shape(shape, dtype):
    return pltpu.VMEM(shape, dtype)


def limit(mebibytes):
    return pltpu.CompilerParams(vmem_limit_bytes=mebibytes << 20)


def cost(microseconds):
    work = int(microseconds * 2.5e9)
    return pl.CostEstimate(flops=work, bytes_accessed=int(microseconds * 1.5e7), transcendentals=0)


def whole(shape):
    rank = len(shape)
    return pl.BlockSpec(shape, lambda *_: (0,) * rank)


def prepare_kernel(peers, experts, slots, ids_ref, share_ref, *outs):
    me = lax.axis_index("ep")
    rows = ids_ref.shape[1]
    ids = ids_ref[...]
    picks = [ids[number : number + 1, :] for number in range(TOP)]
    line = lax.broadcasted_iota(jnp.int32, (max(peers, 8), rows), 0)
    goes = None
    for pick in picks:
        hit = pick // experts == (line ^ me)
        goes = hit if goes is None else goes | hit
    row = lax.broadcasted_iota(jnp.int32, (rows, rows), 0)
    column = lax.broadcasted_iota(jnp.int32, (rows, rows), 1)
    before = (row < column).astype(f32).astype(bf16)
    counts = jnp.dot(goes.astype(f32).astype(bf16), before, preferred_element_type=f32)
    slot = jnp.where(goes, counts, -1.0)
    share = share_ref[...]
    line = lax.broadcasted_iota(jnp.int32, (HEAD, rows), 0)
    target = lax.broadcasted_iota(jnp.int32, (slots, rows), 0).astype(f32)
    for peer in range(peers):
        spot = (slot[peer : peer + 1, :] == target).astype(f32).astype(bf16)
        outs[peer][...] = spot
        table = jnp.zeros((HEAD, rows), f32)
        for expert in range(experts):
            number = (me ^ peer) * experts + expert
            weight = jnp.zeros((1, rows), f32)
            for pick in range(TOP):
                weight += jnp.where(picks[pick] == number, share[pick : pick + 1, :], 0.0)
            high = weight.astype(bf16).astype(f32)
            mid = (weight - high).astype(bf16).astype(f32)
            low = weight - high - mid
            table = jnp.where(line == expert, high, table)
            table = jnp.where(line == experts + expert, mid, table)
            table = jnp.where(line == 2 * experts + expert, low, table)
        moved = lax.dot_general(
            spot, table.astype(bf16), (((1,), (1,)), ((), ())), preferred_element_type=f32
        )
        outs[peers + peer][...] = moved.astype(bf16)


def prepare(route_ids, route_weight, peers, experts, slots):
    rows = route_ids.shape[0]
    outs = pl.pallas_call(
        functools.partial(prepare_kernel, peers, experts, slots),
        out_shape=[near_shape((slots, rows), bf16)] * peers
        + [near_shape((slots, HEAD), bf16)] * peers,
        in_specs=[held()] * 2,
        out_specs=[held()] * (2 * peers),
        compiler_params=limit(4),
        cost_estimate=cost(2),
        name="prepare",
    )(near(route_ids.T), near(route_weight.T))
    return outs[:peers], outs[peers:]


def load_kernel(array_ref, out_ref):
    out_ref[...] = array_ref[...]


def load(array):
    return pl.pallas_call(
        load_kernel,
        out_shape=near_shape(array.shape, array.dtype),
        in_specs=[whole(array.shape)],
        out_specs=held(),
        compiler_params=limit(2),
        cost_estimate=cost(1),
        name="load",
    )(array)


def join_kernel(own_ref, other_ref, joined_ref):
    width = own_ref.shape[1]
    joined_ref[:, :width] = own_ref[...]
    joined_ref[:, width:] = other_ref[...]


def join(own, other):
    rows, width = own.shape
    return pl.pallas_call(
        join_kernel,
        out_shape=near_shape((rows, 2 * width), own.dtype),
        in_specs=[held()] * 2,
        out_specs=held(),
        compiler_params=limit(2),
        cost_estimate=cost(1),
        name="join",
    )(near(own), near(other))


def turns_of(peers):
    return [(peers - 1 - turn, turn) for turn in reversed(range(peers // CORES))]


def project_kernel(peers, rows, gain_ref, *refs):
    weights, outs, total_ref = refs[-5 - peers : -1 - peers], refs[-1 - peers : -1], refs[-1]
    slab, width = weights[0].shape
    me, rank = lax.axis_index("ep"), lax.axis_index("tp")
    level, core = rank // CORES, rank % CORES
    base = me * slab
    direct = len(refs) > 6 + peers
    halves = CORES if direct else 1
    span = slab // halves
    totals, squares = [None] * 4, None
    for half in range(halves):
        if direct:
            one = refs[0][:, pl.ds(pl.multiple_of((core ^ half) * span, 128), span)]
            two = refs[1][:, pl.ds(pl.multiple_of((1 - (core ^ half)) * span, 128), span)]
            values = jnp.concatenate([one.astype(f32), two.astype(f32)], axis=0)
        else:
            values = refs[0][...].astype(f32)
        here = jnp.sum(values * values, axis=-1, keepdims=True)
        squares = here if half == 0 else squares + here
        gain = gain_ref[:, pl.ds(pl.multiple_of(base + half * span, 128), span)]
        scaled = (values * gain).astype(bf16)
        for which in range(4):
            block = weights[which][half * span : (half + 1) * span, :]
            product = jnp.dot(scaled, block, preferred_element_type=f32)
            totals[which] = product if half == 0 else totals[which] + product
    for which in range(4):
        total_ref[:, which * width : (which + 1) * width] = totals[which]
    high = squares.astype(bf16).astype(f32)
    mid = (squares - high).astype(bf16).astype(f32)
    lane = lax.broadcasted_iota(jnp.int32, (squares.shape[0], HEAD), 1)
    table = jnp.where(lane == 0, high, jnp.where(lane == 1, mid, 0.0))
    total_ref[:, 4 * width :] = jnp.where(lane == 2, squares - high - mid, table)
    for peer in range(peers):
        place = peer
        if direct:
            wanted = level ^ me ^ peer
            place = 0
            for turn, pair in enumerate(turns_of(peers)):
                for side in range(CORES):
                    spot = turn + (side ^ core) * (peers // CORES)
                    place = jnp.where(wanted == pair[side], spot, place)
        chosen = total_ref[pl.ds(pl.multiple_of(place * rows, 8), rows), :]
        outs[peer][...] = chosen.astype(outs[peer].dtype)


def project(parts, gain, weights, peers, rows):
    width = 4 * weights[0].shape[1] + HEAD
    out_shape = [near_shape((rows, width), f32)]
    out_shape += [near_shape((rows, width), bf16)] * (peers - 1)
    operands = [near(array) for array in (gain, *parts, *weights)]
    return pl.pallas_call(
        functools.partial(project_kernel, peers, rows),
        out_shape=out_shape,
        in_specs=[held()] * len(operands),
        out_specs=[held()] * peers,
        scratch_shapes=[pltpu.VMEM((peers * rows, width), f32)],
        compiler_params=limit(8),
        cost_estimate=cost(2),
        name="project",
    )(*operands)


def blocks_of(block):
    row = lax.broadcasted_iota(jnp.int32, (block, block * HEAD), 0)
    lane = lax.broadcasted_iota(jnp.int32, (block, block * HEAD), 1)
    return (lane // HEAD == row).astype(f32)


def split_of(rows):
    high = rows.astype(bf16).astype(f32)
    mid = (rows - high).astype(bf16).astype(f32)
    return jnp.concatenate([high, mid, rows - high - mid], axis=0).astype(bf16)


def columns_times(rows, table):
    split = split_of(rows)
    return lax.dot_general(split, table, (((0,), (0,)), ((), ())), preferred_element_type=f32)


def decay_of(head, heads):
    number = (lax.axis_index("tp") * heads + head).astype(f32)
    power = jnp.full((1, HEAD), -5.0, f32) - number * (5.0 / (HEADS - 1))
    return 1.0 - jnp.exp2(power)


def read_kernel(peers, heads, width_model, *refs):
    cos_ref, sin_ref, gain_ref = refs[:3]
    parts = refs[3 : 3 + peers]
    state_ref = refs[3 + peers]
    mixed_ref, key_ref, value_ref = refs[4 + peers : 7 + peers]
    query_ref, read_ref = refs[7 + peers :]
    rows, width = mixed_ref.shape
    squares = parts[0][:, 4 * width :]
    for part in parts[1:]:
        squares = squares + part[:, 4 * width :].astype(f32)
    mean = jnp.sum(squares, axis=-1, keepdims=True) * (1.0 / width_model)
    factor = lax.rsqrt(mean + epsilon)

    def total(which):
        cut = slice(which * width, (which + 1) * width)
        summed = parts[0][:, cut]
        for part in parts[1:]:
            summed = summed + part[:, cut].astype(f32)
        return (summed * factor).astype(bf16).astype(f32)

    query, key, value = total(0), total(1), total(2)
    value_ref[...] = value
    gate = total(3)
    gate = gate * jax.nn.sigmoid(gate) * gain_ref[...]
    own = []
    for head in range(heads):
        cut = slice(head * HEAD, (head + 1) * HEAD)
        one, two = query[:, cut], key[:, cut]
        one = one * cos_ref[...] + pltpu.roll(one, HEAD // 2, 1) * sin_ref[...]
        two = two * cos_ref[...] + pltpu.roll(two, HEAD // 2, 1) * sin_ref[...]
        two = two * HEAD ** (-0.5)
        query_ref[:, cut] = one
        key_ref[:, cut] = two
        own.append(jnp.sum(one * two, axis=-1, keepdims=True) * value[:, cut])
    block = 8
    line = lax.broadcasted_iota(jnp.int32, (block, HEAD), 0)

    def some(number, carry):
        start = pl.multiple_of(number * block, block)
        for head in range(heads):
            cut = slice(head * HEAD, (head + 1) * HEAD)
            split = split_of(query_ref[pl.ds(start, block), cut])
            split = jnp.concatenate([split, split], axis=1)
            found = jnp.zeros((block, HEAD), f32)
            for row in range(block):
                state = state_ref[start + row, head]
                high = state.astype(bf16)
                low = (state - high.astype(f32)).astype(bf16)
                both = jnp.concatenate([high, low], axis=0)
                part = jnp.dot(split, both, preferred_element_type=f32)
                part = part[:block] + part[block : 2 * block] + part[2 * block :]
                found = jnp.where(line == row, part, found)
            read_ref[pl.ds(start, block), cut] = found
        return carry

    lax.fori_loop(0, rows // block, some, 0, unroll=True)
    for head in range(heads):
        cut = slice(head * HEAD, (head + 1) * HEAD)
        read = decay_of(head, heads) * read_ref[:, cut] + own[head]
        centered = read - jnp.mean(read, axis=-1, keepdims=True)
        spread = jnp.mean(centered * centered, axis=-1, keepdims=True)
        normal = centered * lax.rsqrt(spread + epsilon)
        mixed_ref[:, cut] = (normal * gate[:, cut]).astype(bf16)


def read_state(parts, cosine, sine, head_gain, ret_state, width_model):
    rows, heads = ret_state.shape[:2]
    width = heads * HEAD
    operands = [near(a) for a in (cosine, sine, head_gain, *parts, ret_state)]
    return pl.pallas_call(
        functools.partial(read_kernel, len(parts), heads, width_model),
        out_shape=[
            near_shape((rows, width), bf16),
            near_shape((rows, width), f32),
            near_shape((rows, width), f32),
        ],
        in_specs=[held()] * len(operands),
        out_specs=[held()] * 3,
        scratch_shapes=[pltpu.VMEM((rows, width), f32)] * 2,
        compiler_params=limit(4),
        cost_estimate=cost(2),
        name="read_state",
    )(*operands)


def update_kernel(heads, first, *refs):
    key_ref, value_ref, state_ref, next_ref = *refs[:3], refs[-1]
    block = next_ref.shape[0]
    start = pl.multiple_of((pl.program_id(0) + first) * block, block)
    mask = blocks_of(block)
    for head in range(heads):
        cut = slice(head * HEAD, (head + 1) * HEAD)
        values = value_ref[pl.ds(start, block), cut]
        table = jnp.concatenate([values] * block, axis=1) * mask
        table = jnp.concatenate([table] * 3, axis=0).astype(bf16)
        outer = columns_times(key_ref[pl.ds(start, block), cut], table)
        decay = decay_of(head, heads)
        for row in range(block):
            next_ref[row, head] = (
                decay * state_ref[start + row, head] + outer[:, row * HEAD : (row + 1) * HEAD]
            )


def update_state(key, value, ret_state, first, last, so_far, after):
    _, heads = ret_state.shape[:2]
    block = 8
    operands = [near(key), near(value), near(ret_state)] + [near(array) for array in after]
    specs = [held()] * len(operands)
    aliases = {}
    if so_far is not None:
        aliases = {len(operands): 0}
        operands.append(so_far)
        specs.append(pl.BlockSpec(memory_space=pl.ANY))
    return pl.pallas_call(
        functools.partial(update_kernel, heads, first),
        grid=(last - first,),
        out_shape=jax.ShapeDtypeStruct(ret_state.shape, f32),
        in_specs=specs,
        out_specs=pl.BlockSpec((block, heads, HEAD, HEAD), lambda i: (i + first, 0, 0, 0)),
        input_output_aliases=aliases,
        compiler_params=limit(6),
        cost_estimate=cost(2),
        name="update_state",
    )(*operands)


def out_sum(pieces, places, weight_ref, total):
    width = pieces[0].shape[1]
    for piece, place in zip(pieces, places):
        block = weight_ref[pl.ds(place, width), :]
        total = total + jnp.dot(piece[...], block, preferred_element_type=f32)
    return total


def out_first(levels, own, rest, other, weight_ref, hidden_ref, total_ref):
    places = spots(CORES * levels, own.shape[1])[: levels + 1]
    total = hidden_ref[...].astype(f32)
    total_ref[...] = out_sum([own, *parts_of(rest, levels), other], places, weight_ref, total)


def out_last(levels, peers, others, weight_ref, total_ref, *refs):
    placing, shares = refs[:peers], refs[peers : 2 * peers]
    after_ref, outs = refs[2 * peers], refs[2 * peers + 1 :]
    places = spots(CORES * levels, others.shape[1])[levels + 1 :]
    pieces = parts_of(others, levels)
    after = out_sum(pieces, places, weight_ref, total_ref[...]).astype(bf16)
    after_ref[...] = after
    cut = after.shape[1]
    for peer in range(peers):
        sent = jnp.dot(placing[peer][...], after, preferred_element_type=f32)
        outs[peer][:, :cut] = sent.astype(bf16)
        outs[peer][:, cut:] = shares[peer][...]


def out_project(pieces, weight, hidden, placing, shares):
    own, rest, other, others = pieces
    rows, width = hidden.shape
    slots, peers = placing[0].shape[0], len(placing)
    levels = 1 + rest.shape[0] // rows
    (total,) = call(
        functools.partial(out_first, levels),
        [near_shape((rows, width), f32)],
        (own, rest, other, weight, hidden),
        1,
    )
    return call(
        functools.partial(out_last, levels, peers),
        [near_shape((rows, width), bf16)] + [near_shape((slots, width + HEAD), bf16)] * peers,
        (others, weight, total, *placing, *shares),
        2,
    )


def lift_sum(pieces, places, gain_ref, gate_ref, up_ref, squares, gates, ups):
    width = pieces[0].shape[1]
    for piece, place in zip(pieces, places):
        values = piece[...].astype(f32)
        squares = squares + jnp.sum(values * values, axis=-1, keepdims=True)
        scaled = (values * gain_ref[:, pl.ds(place, width)]).astype(bf16)
        for expert in range(gate_ref.shape[0]):
            one = gate_ref[expert, pl.ds(place, width), :]
            two = up_ref[expert, pl.ds(place, width), :]
            gates[expert] = gates[expert] + jnp.dot(scaled, one, preferred_element_type=f32)
            ups[expert] = ups[expert] + jnp.dot(scaled, two, preferred_element_type=f32)
    return squares, gates, ups


def lift_first(levels, own, rest, other, gain_ref, gate_ref, up_ref, gates_ref, ups_ref, squares_ref):
    experts, rows, width = gates_ref.shape
    places = spots(CORES * levels, own.shape[1])[: levels + 1]
    zeros = [jnp.zeros((rows, width), f32)] * experts
    squares, gates, ups = lift_sum(
        [own, *parts_of(rest, levels), other],
        places,
        gain_ref,
        gate_ref,
        up_ref,
        jnp.zeros((rows, 1), f32),
        list(zeros),
        list(zeros),
    )
    squares_ref[...] = jnp.broadcast_to(squares, squares_ref.shape)
    for expert in range(experts):
        gates_ref[expert] = gates[expert]
        ups_ref[expert] = ups[expert]


def lift_last(
    levels, depth, others, gain_ref, gate_ref, up_ref, gates_ref, ups_ref, squares_ref, active_ref
):
    experts = gates_ref.shape[0]
    places = spots(CORES * levels, others.shape[1])[levels + 1 :]
    squares, gates, ups = lift_sum(
        parts_of(others, levels),
        places,
        gain_ref,
        gate_ref,
        up_ref,
        squares_ref[:, :1],
        [gates_ref[expert] for expert in range(experts)],
        [ups_ref[expert] for expert in range(experts)],
    )
    factor = lax.rsqrt(squares * (1.0 / depth) + epsilon)
    for expert in range(experts):
        gate = gates[expert] * factor
        active_ref[expert] = (gate * jax.nn.sigmoid(gate) * (ups[expert] * factor)).astype(bf16)


def lift(pieces, gain, expert_gate, expert_up):
    own, rest, other, others = pieces
    experts, depth, width = expert_gate.shape
    rows = own.shape[0]
    levels = 1 + rest.shape[0] // rows
    sums = call(
        functools.partial(lift_first, levels),
        [near_shape((experts, rows, width), f32)] * 2 + [near_shape((rows, HEAD), f32)],
        (own, rest, other, gain, expert_gate, expert_up),
        2,
    )
    (active,) = call(
        functools.partial(lift_last, levels, depth),
        [near_shape((experts, rows, width), bf16)],
        (others, gain, expert_gate, expert_up, *sums),
        2,
    )
    return active


def lower_sum(pieces, places, down_ref, totals):
    width = pieces[0].shape[-1]
    for piece, place in zip(pieces, places):
        for expert in range(down_ref.shape[0]):
            block = down_ref[expert, pl.ds(place, width), :]
            product = jnp.dot(piece[expert], block, preferred_element_type=f32)
            totals[expert] = product if totals[expert] is None else totals[expert] + product
    return totals


def lower_first(levels, own, rest, other, down_ref, totals_ref):
    experts = down_ref.shape[0]
    places = spots(CORES * levels, own.shape[2])[: levels + 1]
    totals = lower_sum([own, *parts_of(rest, levels), other], places, down_ref, [None] * experts)
    for expert in range(experts):
        totals_ref[expert] = totals[expert]


def lower_last(levels, peers, others, down_ref, totals_ref, *refs):
    tables, outs, mean_ref = refs[:peers], refs[peers : 2 * peers], refs[-1]
    experts, _ = totals_ref.shape[:2]
    slots = tables[0].shape[0]
    places = spots(CORES * levels, others.shape[2])[levels + 1 :]
    totals = [totals_ref[expert] for expert in range(experts)]
    totals = lower_sum(parts_of(others, levels), places, down_ref, totals)
    for expert in range(experts):
        mean_ref[expert] = totals[expert].astype(bf16).astype(f32)
    cut = tables[0].shape[1] - HEAD
    for peer in range(peers):
        table = tables[peer][:, cut:].astype(f32)
        sent = None
        for expert in range(experts):
            share = (
                table[:, expert : expert + 1]
                + table[:, experts + expert : experts + expert + 1]
                + table[:, 2 * experts + expert : 2 * experts + expert + 1]
            )
            here = mean_ref[expert, peer * slots : (peer + 1) * slots, :] * share
            sent = here if sent is None else sent + here
        outs[peer][...] = sent.astype(bf16)


def lower(pieces, expert_down, tables):
    own, rest, other, others = pieces
    experts, _, width = expert_down.shape
    rows = own.shape[1]
    levels = 1 + rest.shape[1] // rows
    peers, slots = len(tables), tables[0].shape[0]
    (totals,) = call(
        functools.partial(lower_first, levels),
        [near_shape((experts, rows, width), f32)],
        (own, rest, other, expert_down),
        1,
    )
    return call(
        functools.partial(lower_last, levels, peers),
        [near_shape((slots, width), bf16)] * peers,
        (others, expert_down, totals, *tables),
        2,
        [pltpu.VMEM((experts, rows, width), f32)],
    )


def finish_kernel(peers, *refs):
    after_ref = refs[0]
    placing = refs[1 : 1 + peers]
    back = refs[1 + peers : 1 + 2 * peers]
    updated_ref = refs[-1]
    total = after_ref[...].astype(f32)
    for peer in range(peers):
        total = total + lax.dot_general(
            placing[peer][...],
            back[peer][...],
            (((0,), (0,)), ((), ())),
            preferred_element_type=f32,
        )
    updated_ref[...] = total.astype(bf16)


def finish(after, placing, back):
    operands = [near(array) for array in (after, *placing, *back)]
    return pl.pallas_call(
        functools.partial(finish_kernel, len(placing)),
        out_shape=jax.ShapeDtypeStruct(after.shape, bf16),
        in_specs=[held()] * len(operands),
        out_specs=whole(after.shape),
        compiler_params=limit(4),
        cost_estimate=cost(1),
        name="finish",
    )(*operands)


def shared(piece, lines):
    rest = jnp.concatenate(lines[1:], axis=-2)
    return [piece, rest, swap_cores(piece), swap_cores(rest)]


def layer(
    hidden,
    positions,
    ret_state,
    query_weight,
    key_weight,
    value_weight,
    gate_weight,
    head_gain,
    out_weight,
    mix_gain,
    ffn_gain,
    expert_gate,
    expert_up,
    expert_down,
    route_ids,
    route_weight,
):
    own_rows, slice_width = hidden.shape
    peers = lax.axis_size("ep")
    ranks = lax.axis_size("tp")
    depth = slice_width * ranks
    slab, width = query_weight.shape

    local_experts = expert_gate.shape[0]
    group_size = local_experts * peers // GROUPS
    capacity = 2 * ((own_rows // GROUPS + group_size - 1) // group_size)
    slots = local_experts * capacity
    if local_experts % group_size == 0:
        slots = slots // TOP
    direct = ranks == CORES * peers
    if direct:
        joined = join(load(hidden), swap_cores(hidden))
        positions, route_ids, route_weight, joined = lax.optimization_barrier(
            (positions, route_ids, route_weight, joined)
        )
    placing, shares = prepare(route_ids, route_weight, peers, local_experts, slots)

    inverse = 1.0 / rope_base ** (jnp.arange(0, HEAD, 2, dtype=f32) / HEAD)
    angle = positions.astype(f32)[:, None] * inverse[None, :]
    cosine, sine = jnp.cos(angle), jnp.sin(angle)
    cosine = jnp.concatenate([cosine, cosine], axis=1)
    sine = jnp.concatenate([-sine, sine], axis=1)

    if direct:
        came = []
        for pair in turns_of(peers):
            route = [
                ((e * peers + z) * CORES + side, (z * peers + (e ^ pair[side])) * CORES + side)
                for e in range(peers)
                for z in range(peers)
                for side in range(CORES)
            ]
            came.append(lax.ppermute(joined, ("ep", "tp"), route))
        came, placing, shares, cosine, sine = lax.optimization_barrier(
            (came, placing, shares, cosine, sine)
        )
        came = jnp.concatenate(came, axis=0)
        parts = [came, swap_cores(came)]
    else:
        me = lax.axis_index("ep")
        full_rows = lax.all_gather(hidden, "tp", axis=1, tiled=True)
        columns = lax.all_to_all(full_rows, "ep", split_axis=1, concat_axis=0, tiled=True)
        columns = columns.reshape(peers, own_rows, slab)
        parts = [columns[me ^ jnp.arange(peers)].reshape(peers * own_rows, slab)]
    weights = (query_weight, key_weight, value_weight, gate_weight)
    partial = project(parts, mix_gain.reshape(1, depth), weights, peers, own_rows)
    sums = to_peers(partial)

    mixed, key, value = read_state(
        sums, cosine, sine, head_gain.reshape(1, width), ret_state, depth
    )
    blocks = own_rows // 8
    split = max(1, 2 * blocks // 5)
    next_state = update_state(key, value, ret_state, 0, split, None, ())

    lines, next_state = lax.optimization_barrier((along_z(mixed), next_state))
    pieces = shared(mixed, lines)
    after, *packed = out_project(pieces, out_weight, hidden, placing, shares)

    next_state = update_state(key, value, ret_state, split, blocks, next_state, (after,))
    arrived = to_peers(packed)
    arrived, next_state = lax.optimization_barrier((arrived, next_state))
    rows = jnp.concatenate([table[:, :slice_width] for table in arrived], axis=0)
    pieces = shared(rows, along_z(rows))
    active = lift(pieces, ffn_gain.reshape(1, depth), expert_gate, expert_up)

    pieces = shared(active, along_z(active))
    back = lower(pieces, expert_down, arrived)
    back = to_peers(back)
    return (finish(after, placing, back), next_state)


def solution(mesh):
    return jax.shard_map(
        layer,
        mesh=mesh,
        in_specs=(
            P("ep", "tp"),
            P("ep"),
            P("ep", "tp", None, None),
            P("ep", "tp"),
            P("ep", "tp"),
            P("ep", "tp"),
            P("ep", "tp"),
            P("tp"),
            P(None, "tp"),
            P(),
            P(),
            P("ep", None, "tp"),
            P("ep", None, "tp"),
            P("ep", None, "tp"),
            P("ep", None),
            P("ep", None),
        ),
        out_specs=(P("ep", "tp"), P("ep", "tp", None, None)),
        check_vma=False,
    )
```
